128 devices in a mesh: fs: 16 (over z, y), tp: 8 (over x, core).
Axes of the slice: x: 4, y: 4, z: 4, core: 2. Of those that a mesh axis runs over, the one named last changes fastest.
Arguments:
- tokens: bfloat16 [16384, 2048], P('fs'), may hold values from -6 to 6
- w_gate_side: bfloat16 [2048, 1024], P('fs', 'tp'), may hold values from -0.125 to 0.125
- w_value_side: bfloat16 [2048, 1024], P('fs', 'tp'), may hold values from -0.125 to 0.125
- spatial_gain: float32 [1024], P('tp'), may hold values from 0.1 to 1.9
- w_spatial: bfloat16 [16, 128, 128], P('tp'), may hold values from -0.5 to 0.5
- spatial_bias: float32 [16, 128], P('tp'), may hold values from 0.1 to 1.9
- w_mixer_out: bfloat16 [1024, 2048], P('tp', 'fs'), may hold values from -0.1875 to 0.1875
- first_gain: float32 [2048], replicated, may hold values from 0.1 to 1.9
- w_ff_gate: bfloat16 [2048, 5632], P('fs', 'tp'), may hold values from -0.125 to 0.125
- w_ff_up: bfloat16 [2048, 5632], P('fs', 'tp'), may hold values from -0.125 to 0.125
- conv_gate_taps: float32 [3, 5632], P(None, 'tp'), may hold values from -3.5 to 3.5
- conv_up_taps: float32 [3, 5632], P(None, 'tp'), may hold values from -3.5 to 3.5
- w_ff_down: bfloat16 [5632, 2048], P('tp', 'fs'), may hold values from -0.078125 to 0.078125
- second_gain: float32 [2048], replicated, may hold values from 0.1 to 1.9
Outputs:
- layer_out: bfloat16 [16384, 2048], P('fs', 'tp')
The draws below stay inside these ranges and needn't reach their ends.
All inputs are finite; a program needn't handle non-finite values.
Results may differ from the reference program's by a relative error of at most 0.015.
Values may be sent and summed in bfloat16 or wider, within the bound.
A program may use at most 64 MiB of HBM per device.

```python
import jax
import jax.numpy as jnp
from jax import lax

D = 2048
GROUPS = 16
GROUP_DIM = 64
SG_WIDTH = 1024
FF = 5632
SPAN = 128
SEQ = 256
TOKENS = 16384
N_TP = 8


def steps_of(stream_key, shape, split, least, high):
    def one(axis_at, blocks):
        steps = jax.random.uniform(jax.random.fold_in(jax.random.fold_in(stream_key, 6), axis_at), (blocks,), jnp.float32, least / len(split), high / len(split))
        return jnp.repeat(jnp.exp(steps), shape[axis_at] // blocks).reshape((-1,) + (1,) * (len(shape) - axis_at - 1))

    level = one(*split[0])
    for cut in split[1:]:
        level = level * one(*cut)
    return level


def noise(key, shape, scale, limit, shards=(), kind=jnp.bfloat16):
    level = steps_of(key, shape, shards, -0.22, 0.18) if shards else 1.0
    values = jax.random.normal(key, shape, jnp.float32) * scale * level
    return jnp.minimum(jnp.maximum(values, -limit), limit).astype(kind)


def setup_inputs(seed: int = 0) -> dict:
    key_of = jax.random.split(jax.random.key(seed), 15)
    tokens = noise(key_of[0], (TOKENS, D), 1.0, 6.0, ((0, 16),))
    w_gate_side = noise(key_of[1], (D, SG_WIDTH), D ** -0.5, 0.125, ((0, 16), (1, 8)))
    w_value_side = noise(key_of[2], (D, SG_WIDTH), D ** -0.5, 0.125, ((0, 16), (1, 8)))
    spatial_gain = jnp.clip(1.0 + 0.18 * jax.random.normal(key_of[3], (SG_WIDTH,), jnp.float32), 0.1, 1.9)
    w_spatial = noise(key_of[4], (GROUPS, SPAN, SPAN), SPAN ** -0.5, 0.5, ((0, 8),))
    spatial_bias = jnp.clip(1.0 + 0.18 * jax.random.normal(key_of[5], (GROUPS, SPAN), jnp.float32), 0.1, 1.9)
    w_mixer_out = noise(key_of[6], (SG_WIDTH, D), SG_WIDTH ** -0.5, 0.1875, ((0, 8), (1, 16)))
    first_gain = jnp.clip(1.0 + 0.18 * jax.random.normal(key_of[7], (D,), jnp.float32), 0.1, 1.9)
    w_ff_gate = noise(key_of[8], (D, FF), D ** -0.5, 0.125, ((0, 16), (1, 8)))
    w_ff_up = noise(key_of[9], (D, FF), D ** -0.5, 0.125, ((0, 16), (1, 8)))
    conv_gate_taps = noise(key_of[10], (3, FF), 3 ** -0.5, 3.5, ((1, 8),), jnp.float32)
    conv_up_taps = noise(key_of[11], (3, FF), 3 ** -0.5, 3.5, ((1, 8),), jnp.float32)
    w_ff_down = noise(key_of[12], (FF, D), FF ** -0.5, 0.078125, ((0, 8), (1, 16)))
    second_gain = jnp.clip(1.0 + 0.18 * jax.random.normal(key_of[13], (D,), jnp.float32), 0.1, 1.9)
    return {"tokens": tokens, "w_gate_side": w_gate_side, "w_value_side": w_value_side, "spatial_gain": spatial_gain, "w_spatial": w_spatial, "spatial_bias": spatial_bias, "w_mixer_out": w_mixer_out, "first_gain": first_gain, "w_ff_gate": w_ff_gate, "w_ff_up": w_ff_up, "conv_gate_taps": conv_gate_taps, "conv_up_taps": conv_up_taps, "w_ff_down": w_ff_down, "second_gain": second_gain}


residual_scale = 2.0 ** 0.25
norm_eps = 1e-05

def row_norm(values, gain):
    width = values.shape[-1]
    mean = lax.optimization_barrier(jnp.sum(values, axis=-1, keepdims=True)) / width
    square = lax.optimization_barrier(jnp.sum(values * values, axis=-1, keepdims=True)) / width
    spread = square - mean * mean
    return (values - mean) * lax.rsqrt(spread + norm_eps) * gain

def causal_taps(pre, taps):
    count = pre.shape[0] // SEQ
    blocks = pre.reshape(count, SEQ, pre.shape[1])
    padded = jnp.pad(blocks, ((0, 0), (2, 0), (0, 0)))
    result = padded[:, 0:SEQ] * taps[0] + padded[:, 1:SEQ + 1] * taps[1] + padded[:, 2:] * taps[2]
    return result.reshape(pre.shape)

def range_sum(left, right, parts):
    width = left.shape[1] // parts
    total = jnp.zeros((left.shape[0], right.shape[1]), jnp.float32)
    for index in range(parts):
        term = jnp.dot(left[:, index * width:(index + 1) * width], right[index * width:(index + 1) * width], preferred_element_type=jnp.float32)
        total = total + term.astype(jnp.bfloat16).astype(jnp.float32)
    return total

def reference(tokens, w_gate_side, w_value_side, spatial_gain, w_spatial, spatial_bias, w_mixer_out, first_gain, w_ff_gate, w_ff_up, conv_gate_taps, conv_up_taps, w_ff_down, second_gain):
    gate_act = jax.nn.gelu(jnp.dot(tokens, w_gate_side, preferred_element_type=jnp.float32))
    value_act = jax.nn.gelu(jnp.dot(tokens, w_value_side, preferred_element_type=jnp.float32))
    value_norm = row_norm(value_act, spatial_gain).astype(jnp.bfloat16)
    blocks = value_norm.reshape(TOKENS // SPAN, SPAN, GROUPS, GROUP_DIM).astype(jnp.float32)
    lower = jnp.tril(jnp.ones((SPAN, SPAN), jnp.float32))
    causal_w = w_spatial.astype(jnp.float32) * lower
    mixed = jnp.einsum('gts,nsgc->ntgc', causal_w, blocks) + spatial_bias.T[None, :, :, None]
    spatial_out = (gate_act * mixed.reshape(TOKENS, SG_WIDTH)).astype(jnp.bfloat16)
    mixer_sum = range_sum(spatial_out, w_mixer_out, N_TP)
    first_normed = row_norm(residual_scale * tokens.astype(jnp.float32) + mixer_sum, first_gain).astype(jnp.bfloat16)
    ff_gate = causal_taps(jnp.dot(first_normed, w_ff_gate, preferred_element_type=jnp.float32), conv_gate_taps)
    ff_up = causal_taps(jnp.dot(first_normed, w_ff_up, preferred_element_type=jnp.float32), conv_up_taps)
    ff_hidden = (jax.nn.silu(ff_gate) * ff_up).astype(jnp.bfloat16)
    ff_sum = range_sum(ff_hidden, w_ff_down, N_TP)
    layer_out = row_norm(residual_scale * first_normed.astype(jnp.float32) + ff_sum, second_gain)
    return layer_out.astype(jnp.bfloat16)
```

```python
import jax
import jax.numpy as jnp
from jax import lax
from jax.experimental import pallas as pl
from jax.experimental.pallas import tpu as pltpu
from jax.sharding import Mesh
from jax.sharding import PartitionSpec as P

ROWS = 1024
D = 2048
SG_WIDTH = 1024
SEQ = 256
FS = ("z", "y")
TP = ("x", "c")
SCALE = 2.0**0.25
EPS = 1e-05
F32 = jnp.float32
BF16 = jnp.bfloat16
MESH = pl.DeviceIdType.MESH


def mul(i, n):
    return pl.multiple_of(i, n)


def dot(a, b):
    return jnp.dot(a, b, preferred_element_type=F32)


ORDER = ((1, 0), (3, 0), (0, 1), (2, 0), (1, 3), (3, 3), (2, 1))
LAST = ((0, 3), (1, 1), (3, 1), (2, 3), (0, 2), (1, 2), (3, 2), (2, 2))


class PlaneGather:
    def __init__(self, block, pos, send_sem, recv_sem, flip=0):
        self.block, self.pos = block, pos
        self.send_sem, self.recv_sem = send_sem, recv_sem
        self.flip = flip

    def axes(self, half):
        return ("y", "z") if half == 0 else ("z", "y")

    def ref(self, half, d):
        a1, a2 = self.axes(half)
        at = {
            a1: lax.rem(self.pos[a1] + 4 - d[0], 4),
            a2: lax.rem(self.pos[a2] + 4 - d[1], 4),
        }
        return self.block(half, at["z"] * 4 + at["y"])

    def copy(self, half, target, source, axis, step):
        ref = self.ref(half, source)
        i = target[0] * 4 + target[1]
        return pltpu.make_async_remote_copy(
            src_ref=ref,
            dst_ref=ref,
            send_sem=self.send_sem.at[half, i],
            recv_sem=self.recv_sem.at[half, i],
            device_id={axis: lax.rem(self.pos[axis] + 4 + step, 4)},
            device_id_type=MESH,
        )

    def route(self, half, target):
        a1, a2 = self.axes(half)
        d1, d2 = target
        if d2 == 0:
            if d1 == 2:
                plus = (half + self.flip) % 2 == 0
                return ((1, 0), a1, 1) if plus else ((3, 0), a1, -1)
            return ((0, 0), a1, 1 if d1 == 1 else -1)
        if d2 == 2:
            return ((d1, 1), a2, 1) if d1 % 2 == 0 else ((d1, 3), a2, -1)
        return ((d1, 0), a2, 1 if d2 == 1 else -1)

    def send(self, half, target):
        source, axis, step = self.route(half, target)
        self.copy(half, target, source, axis, step).start()

    def after(self, half, source):
        for target in ((1, 0), (3, 0), (2, 0)):
            if self.route(half, target)[0] == source:
                self.send(half, target)
        for d1 in range(4):
            for d2 in (1, 3, 2):
                if self.route(half, (d1, d2))[0] == source:
                    self.send(half, (d1, d2))

    def own(self):
        for half in (0, 1):
            self.after(half, (0, 0))

    def arrived(self, half, d):
        i = d[0] * 4 + d[1]
        ref = self.ref(half, d)
        pltpu.make_async_remote_copy(
            src_ref=ref,
            dst_ref=ref,
            send_sem=self.send_sem.at[half, i],
            recv_sem=self.recv_sem.at[half, i],
            device_id={"y": lax.rem(self.pos["y"] + 1, 4)},
            device_id_type=MESH,
        ).wait_recv()

    def step(self, *which):
        for k in which:
            for half in (0, 1):
                self.arrived(half, ORDER[k])
                self.after(half, ORDER[k])

    def rest(self):
        for d in LAST:
            for half in (0, 1):
                self.arrived(half, d)

    def sent(self):
        for half in (0, 1):
            for d1 in range(4):
                for d2 in range(4):
                    if d1 or d2:
                        source, axis, step = self.route(half, (d1, d2))
                        self.copy(half, (d1, d2), source, axis, step).wait_send()


class RingGather:
    def __init__(self, block, x, send_sem, recv_sem):
        self.block, self.x = block, x
        self.send_sem, self.recv_sem = send_sem, recv_sem

    def copy(self, back, part, slot, step):
        ref = self.block(lax.rem(self.x + 4 - back, 4), part)
        return pltpu.make_async_remote_copy(
            src_ref=ref,
            dst_ref=ref,
            send_sem=self.send_sem.at[slot],
            recv_sem=self.recv_sem.at[slot],
            device_id={"x": lax.rem(self.x + 4 + step, 4)},
            device_id_type=MESH,
        )

    def sends(self):
        return ((0, 0, 0, 1), (0, 1, 1, -1), (0, 1, 2, 1), (0, 0, 3, -1), (1, 0, 4, 1), (3, 1, 5, -1))

    def own(self):
        for c in self.sends()[:4]:
            self.copy(*c).start()

    def forward(self):
        self.copy(1, 0, 0, 1).wait_recv()
        self.copy(*self.sends()[4]).start()
        self.copy(3, 1, 1, 1).wait_recv()
        self.copy(*self.sends()[5]).start()

    def rest(self):
        self.copy(1, 1, 2, 1).wait_recv()
        self.copy(3, 0, 3, 1).wait_recv()
        self.copy(2, 0, 4, 1).wait_recv()
        self.copy(2, 1, 5, 1).wait_recv()

    def sent(self):
        for c in self.sends():
            self.copy(*c).wait_send()


class Stats:
    def __init__(self, ref, x, c, send_sem, recv_sem):
        self.ref, self.x, self.c = ref, x, c
        self.send_sem, self.recv_sem = send_sem, recv_sem

    def copies(self):
        out = []
        for k in (4, 5, 2, 6, 3, 7, 1):
            dx, dc = k // 2, k % 2
            out.append(
                pltpu.make_async_remote_copy(
                    src_ref=self.ref.at[0],
                    dst_ref=self.ref.at[k],
                    send_sem=self.send_sem.at[k],
                    recv_sem=self.recv_sem.at[k],
                    device_id={"x": lax.rem(self.x + dx, 4), "c": lax.rem(self.c + dc, 2)},
                    device_id_type=MESH,
                )
            )
        return out

    def start(self):
        for c in self.copies():
            c.start()

    def total(self):
        for c in self.copies():
            c.wait_recv()
        total = self.ref[0]
        for k in range(1, 8):
            total = total + self.ref[k]
        return total

    def sent(self):
        for c in self.copies():
            c.wait_send()


def spread(row):
    return jnp.broadcast_to(row, (128, 128)).T


def kernel(
    tok_h, gv_h, mo_h, in1_h, in2_h, wd_h, gain, wsp, bias, g1, taps, g2,
    out,
    tok, gv, mo, in1, in2, wd, ga, va, st1, st2, tot, so,
    msend, mrecv, mown, fn, hid, dsend, drecv, xs, xr2, xr1, acc,
    lsem, psend, precv, rsend, rrecv, ssend, srecv, dss, drs, xss, xrs,
):
    z, y = lax.axis_index("z"), lax.axis_index("y")
    x, c = lax.axis_index("x"), lax.axis_index("c")
    pos = {"z": z, "y": y}
    f = z * 4 + y
    j = x * 2 + c
    sib = {"c": 1 - c}

    gv_block = lambda half, b: gv.at[pl.ds(mul(b * 128 + half * 64, 64), 64), :]
    in1_block = lambda half, b: in1.at[pl.ds(mul(b * 128 + half * 64, 64), 64), :]
    in2_block = lambda half, b: in2.at[pl.ds(mul(b * 128 + half * 64, 64), 64), :]
    mo_block = lambda half, b: mo.at[
        pl.ds(mul(x * 128 + half * 64, 64), 64), pl.ds(mul(b * 128, 128), 128)
    ]
    wd_block = lambda half, b: wd.at[pl.ds(half * 352, 352), pl.ds(mul(b * 128, 128), 128)]
    g_gv = PlaneGather(gv_block, pos, psend.at[0], precv.at[0], 0)
    g_mo = PlaneGather(mo_block, pos, psend.at[1], precv.at[1], 1)
    g_in1 = PlaneGather(in1_block, pos, psend.at[2], precv.at[2], 0)
    g_in2 = PlaneGather(in2_block, pos, psend.at[3], precv.at[3], 1)
    g_wd = PlaneGather(wd_block, pos, psend.at[4], precv.at[4], 0)
    r_mo = RingGather(
        lambda b, part: mo.at[pl.ds(mul(b * 128 + part * 64, 64), 64), :], x, rsend.at[0], rrecv.at[0]
    )
    r_so = RingGather(
        lambda b, part: so.at[pl.ds(part * 512, 512), pl.ds(mul(b * 128, 128), 128)],
        x, rsend.at[1], rrecv.at[1],
    )
    s1 = Stats(st1, x, c, ssend.at[0], srecv.at[0])
    s2 = Stats(st2, x, c, ssend.at[1], srecv.at[1])

    loads = [
        pltpu.make_async_copy(gv_h, gv.at[pl.ds(mul(f * 128, 128), 128), :], lsem.at[0]),
        pltpu.make_async_copy(
            mo_h, mo.at[pl.ds(mul(x * 128, 128), 128), pl.ds(mul(f * 128, 128), 128)], lsem.at[1]
        ),
        pltpu.make_async_copy(in1_h, in1.at[pl.ds(mul(f * 128, 128), 128), :], lsem.at[2]),
        pltpu.make_async_copy(in2_h, in2.at[pl.ds(mul(f * 128, 128), 128), :], lsem.at[3]),
        pltpu.make_async_copy(
            wd_h, wd.at[pl.ds(0, 704), pl.ds(mul(f * 128, 128), 128)], lsem.at[4]
        ),
        pltpu.make_async_copy(tok_h, tok, lsem.at[5]),
    ]
    for l in loads:
        l.start()

    barrier = pltpu.get_barrier_semaphore()
    peers = [{a: lax.rem(pos[a] + s, 4)} for a in ("y", "z") for s in (1, 3)]
    peers += [
        {"x": lax.rem(x + k // 2, 4), "c": lax.rem(c + k % 2, 2)} for k in range(1, 8)
    ]
    for p in peers:
        pl.semaphore_signal(barrier, inc=1, device_id=p, device_id_type=MESH)
    wd[704:768, :] = jnp.zeros((64, D), BF16)
    loads[0].wait()
    pl.semaphore_wait(barrier, len(peers))

    g_gv.own()
    loads[1].wait()
    g_mo.own()
    g_gv.step(0, 1)
    loads[2].wait()
    g_mo.step(0, 1)
    g_gv.step(2, 3)
    g_mo.step(2, 3)
    g_in1.own()
    g_gv.step(4, 5, 6)
    g_mo.step(4, 5, 6)
    g_gv.rest()
    loads[5].wait()

    @pl.loop(0, 4)
    def _(i):
        r = pl.ds(mul(i * 256, 256), 256)
        pre = dot(tok[r, :], gv[...])
        act = jax.nn.gelu(pre)
        ga[r, :] = act[:, :128]
        va[r, :] = act[:, 128:]
        for h in range(2):
            v = act[h * 128 : h * 128 + 128, 128:].T
            st1[0, pl.ds(i * 2 + h, 1), :] = jnp.sum(v, axis=0, keepdims=True)
            st1[0, pl.ds(i * 2 + h + 8, 1), :] = jnp.sum(v * v, axis=0, keepdims=True)

    s1.start()
    g_mo.rest()
    r_mo.own()
    g_in1.step(0, 1)
    loads[3].wait()
    g_in2.own()
    tot[...] = s1.total()

    lane = lax.broadcasted_iota(jnp.int32, (128, 128), 1)
    low = lax.broadcasted_iota(jnp.int32, (128, 128), 0) >= lane
    w0 = jnp.where(low, wsp[0], jnp.zeros((128, 128), BF16))
    w1 = jnp.where(low, wsp[1], jnp.zeros((128, 128), BF16))

    @pl.loop(0, 8)
    def _(n):
        r = pl.ds(mul(n * 128, 128), 128)
        mean = spread(tot[pl.ds(n, 1), :] * (1.0 / SG_WIDTH))
        square = spread(tot[pl.ds(n + 8, 1), :] * (1.0 / SG_WIDTH))
        inv = lax.rsqrt(square - mean * mean + EPS)
        vn = ((va[r, :] - mean) * inv * gain[...]).astype(BF16)
        mixed = jnp.where(lane < 64, dot(w0, vn), dot(w1, vn)) + bias[...]
        so[r, pl.ds(mul(x * 128, 128), 128)] = (ga[r, :] * mixed).astype(BF16)

    r_so.own()
    g_in1.step(2, 3)
    g_in1.step(4, 5, 6)
    loads[4].wait()
    g_in2.step(0, 1)
    r_mo.forward()
    r_so.forward()
    g_in2.step(2, 3)
    g_wd.own()
    g_in2.step(4, 5, 6)
    r_mo.rest()
    r_so.rest()

    theirs = (1 - c) * 512
    mine = c * 512

    def mix_copy(k):
        return pltpu.make_async_remote_copy(
            src_ref=msend.at[pl.ds(k * 256, 256), :],
            dst_ref=mrecv.at[pl.ds(k * 256, 256), :],
            send_sem=dss.at[k], recv_sem=drs.at[k], device_id=sib, device_id_type=MESH,
        )

    def fn_copy(k, base):
        ref = fn.at[pl.ds(mul(base + k * 256, 256), 256), :]
        return pltpu.make_async_remote_copy(
            src_ref=ref, dst_ref=ref,
            send_sem=dss.at[2 + k], recv_sem=drs.at[2 + k], device_id=sib, device_id_type=MESH,
        )

    for k in range(2):
        @pl.loop(0, 4)
        def _(i):
            cols = pl.ds(mul(i * 512, 512), 512)
            p = dot(so[pl.ds(mul(theirs + k * 256, 256), 256), :], mo[:, cols])
            msend[k * 256 : k * 256 + 256, cols] = p.astype(BF16)

        mix_copy(k).start()
    for k in range(2):
        @pl.loop(0, 4)
        def _(i):
            cols = pl.ds(mul(i * 512, 512), 512)
            mown[k * 256 : k * 256 + 256, cols] = dot(
                so[pl.ds(mul(mine + k * 256, 256), 256), :], mo[:, cols]
            )

    g_wd.step(0, 1)
    for k in range(2):
        mix_copy(k).wait_recv()

        @pl.loop(0, 8)
        def _(i):
            r = pl.ds(mul(k * 256 + i * 32, 32), 32)
            g = pl.ds(mul(mine + k * 256 + i * 32, 32), 32)
            v = SCALE * tok[g, :].astype(F32) + (mown[r, :] + mrecv[r, :].astype(F32))
            mean = jnp.sum(v, axis=1, keepdims=True) * (1.0 / D)
            square = jnp.sum(v * v, axis=1, keepdims=True) * (1.0 / D)
            inv = lax.rsqrt(square - mean * mean + EPS)
            fn[g, :] = ((v - mean) * inv * g1[...]).astype(BF16)

        fn_copy(k, mine).start()

    g_in1.rest()
    g_wd.step(2, 3)

    row = lax.broadcasted_iota(jnp.int32, (SEQ, 256), 0)
    lane2 = lax.broadcasted_iota(jnp.int32, (SEQ, 128), 1)

    def conv(p, t):
        n = p.shape[1]
        p1 = jnp.where(row[:, :n] >= 1, pltpu.roll(p, 1, 0), 0.0)
        p2 = jnp.where(row[:, :n] >= 2, pltpu.roll(p, 2, 0), 0.0)
        return p2 * t[0:1, :] + p1 * t[1:2, :] + p * t[2:3, :]

    def hidden(seq, buf, at, tile):
        r = pl.ds(mul(seq * SEQ, SEQ), SEQ)
        p = dot(fn[r, :], buf[:, pl.ds(mul(at * 256, 256), 256)])
        q = conv(p, taps[:, pl.ds(mul(tile * 256, 256), 256)])
        hid[r, pl.ds(mul(tile * 128, 128), 128)] = (
            jax.nn.silu(q[:, :128]) * q[:, 128:]
        ).astype(BF16)

    def hidden_last(seq):
        r = pl.ds(mul(seq * SEQ, SEQ), SEQ)
        p = dot(fn[r, :], in2[:, 512:640])
        q = conv(p, taps[:, 1280:1408])
        h = jax.nn.silu(q) * pltpu.roll(q, 64, 1)
        hid[r, 640:768] = jnp.where(lane2 < 64, h, 0.0).astype(BF16)

    own_seq = c * 2
    other_seq = (1 - c) * 2

    def part1(first):
        @pl.loop(0, 6)
        def _(i):
            hidden(first + i // 3, in1, i % 3, i % 3)

    def part2(first):
        @pl.loop(0, 4)
        def _(i):
            hidden(first + i // 2, in2, i % 2, 3 + i % 2)

        @pl.loop(0, 2)
        def _(i):
            hidden_last(first + i)

    part1(own_seq)
    g_wd.step(4, 5, 6)
    for k in range(2):
        fn_copy(k, (1 - c) * 512).wait_recv()
    part1(other_seq)
    g_in2.rest()
    part2(own_seq)
    part2(other_seq)
    g_wd.rest()

    hops = (2, 1, 3, 0)

    def dd_copy(k):
        cols = pl.ds(k * 256, 256)
        return pltpu.make_async_remote_copy(
            src_ref=dsend.at[:, cols], dst_ref=drecv.at[:, cols],
            send_sem=dss.at[4 + k], recv_sem=drs.at[4 + k], device_id=sib, device_id_type=MESH,
        )

    def wd_cols(k, parity):
        t = lax.rem(x + hops[k], 4)
        return pl.ds(mul((t * 2 + parity) * 256, 256), 256)

    def down_theirs(k):
        cols = wd_cols(k, 1 - c)

        @pl.loop(0, 4)
        def _(i):
            r = pl.ds(mul(i * 256, 256), 256)
            dsend[r, k * 256 : k * 256 + 256] = dot(hid[r, :], wd[:, cols]).astype(BF16)

        dd_copy(k).start()

    def down_mine(k, i):
        r = pl.ds(mul(i * 256, 256), 256)
        return dot(hid[r, :], wd[:, wd_cols(k, c)]) + drecv[r, k * 256 : k * 256 + 256].astype(F32)

    def x_copy(slot, src, dst, step):
        return pltpu.make_async_remote_copy(
            src_ref=src, dst_ref=dst, send_sem=xss.at[slot], recv_sem=xrs.at[slot],
            device_id={"x": lax.rem(x + 4 + step, 4)}, device_id_type=MESH,
        )

    up, lo = pl.ds(0, 512), pl.ds(512, 512)
    x_copies = (
        x_copy(0, xs.at[0, up], xr2.at[up], 1),
        x_copy(1, xs.at[0, lo], xr2.at[lo], -1),
        x_copy(2, xs.at[1, lo], xr1.at[0, lo], 1),
        x_copy(3, xs.at[2, up], xr1.at[1, up], -1),
        x_copy(4, xs.at[1, up], xr1.at[0, up], 1),
        x_copy(5, xs.at[2, lo], xr1.at[1, lo], -1),
    )

    def fill(k, first, extra):
        @pl.loop(first, first + 2)
        def _(i):
            r = pl.ds(mul(i * 256, 256), 256)
            v = down_mine(k, i)
            if extra:
                v = v + xr2[r, :].astype(F32)
            xs[k, r, :] = v.astype(BF16)

    down_theirs(0)
    down_theirs(1)
    dd_copy(0).wait_recv()
    fill(0, 0, False)
    x_copies[0].start()
    fill(0, 2, False)
    x_copies[1].start()
    down_theirs(2)
    dd_copy(1).wait_recv()
    fill(1, 2, False)
    x_copies[2].start()
    dd_copy(2).wait_recv()
    fill(2, 0, False)
    x_copies[3].start()
    down_theirs(3)
    x_copies[0].wait_recv()
    fill(1, 0, True)
    x_copies[4].start()
    x_copies[1].wait_recv()
    fill(2, 2, True)
    x_copies[5].start()
    dd_copy(3).wait_recv()

    @pl.loop(0, 4)
    def _(i):
        r = pl.ds(mul(i * 256, 256), 256)
        acc[r, :] = down_mine(3, i) + SCALE * fn[r, pl.ds(mul(j * 256, 256), 256)].astype(F32)

    for k in (2, 3, 4, 5):
        x_copies[k].wait_recv()

    @pl.loop(0, 8)
    def _(n):
        r = pl.ds(mul(n * 128, 128), 128)
        v = acc[r, :] + (xr1[0, r, :].astype(F32) + xr1[1, r, :].astype(F32))
        acc[r, :] = v
        a, b = v[:, :128], v[:, 128:]
        st2[0, pl.ds(n, 1), :] = jnp.sum((a + b).T, axis=0, keepdims=True)
        st2[0, pl.ds(n + 8, 1), :] = jnp.sum((a * a + b * b).T, axis=0, keepdims=True)

    s2.start()
    gain2 = g2[pl.ds(j, 1), :]
    for g in (g_gv, g_mo, g_in1, g_in2, g_wd, r_mo, r_so, s1):
        g.sent()
    for k in range(2):
        mix_copy(k).wait_send()
        fn_copy(k, mine).wait_send()
    for k in range(4):
        dd_copy(k).wait_send()
    for k in range(6):
        x_copies[k].wait_send()
    tot[...] = s2.total()

    @pl.loop(0, 8)
    def _(n):
        r = pl.ds(mul(n * 128, 128), 128)
        mean = spread(tot[pl.ds(n, 1), :] * (1.0 / D))
        square = spread(tot[pl.ds(n + 8, 1), :] * (1.0 / D))
        inv = lax.rsqrt(square - mean * mean + EPS)
        for h in range(2):
            cols = slice(h * 128, h * 128 + 128)
            out[r, cols] = ((acc[r, cols] - mean) * inv * gain2[:, cols]).astype(BF16)

    s2.sent()


def pairs(gate, up):
    tiles = []
    for i in range(5):
        tiles += [gate[:, i * 128 : i * 128 + 128], up[:, i * 128 : i * 128 + 128]]
    return tiles + [gate[:, 640:], up[:, 640:]]


def per_device(
    tokens, w_gate_side, w_value_side, spatial_gain, w_spatial, spatial_bias, w_mixer_out,
    first_gain, w_ff_gate, w_ff_up, conv_gate_taps, conv_up_taps, w_ff_down, second_gain,
):
    gv = jnp.concatenate([w_gate_side, w_value_side], axis=1)
    cut = pairs(w_ff_gate, w_ff_up)
    in1 = jnp.concatenate(cut[:6], axis=1)
    in2 = jnp.concatenate(cut[6:], axis=1)
    taps = jnp.concatenate(pairs(conv_gate_taps, conv_up_taps), axis=1)
    bias = jnp.repeat(spatial_bias.T, 64, axis=1)
    vmem = pl.BlockSpec(memory_space=pltpu.VMEM)
    hbm = pl.BlockSpec(memory_space=pl.ANY)
    V, DMA = pltpu.VMEM, pltpu.SemaphoreType.DMA
    return pl.pallas_call(
        kernel,
        out_shape=jax.ShapeDtypeStruct((ROWS, 256), BF16),
        in_specs=[hbm] * 6 + [vmem] * 6,
        out_specs=vmem,
        scratch_shapes=[
            V((ROWS, D), BF16),
            V((D, 256), BF16),
            V((512, D), BF16),
            V((D, 768), BF16),
            V((D, 640), BF16),
            V((768, D), BF16),
            V((ROWS, 128), F32),
            V((ROWS, 128), F32),
            V((8, 16, 128), F32),
            V((8, 16, 128), F32),
            V((16, 128), F32),
            V((ROWS, 512), BF16),
            V((512, D), BF16),
            V((512, D), BF16),
            V((512, D), F32),
            V((ROWS, D), BF16),
            V((ROWS, 768), BF16),
            V((ROWS, 1024), BF16),
            V((ROWS, 1024), BF16),
            V((3, ROWS, 256), BF16),
            V((ROWS, 256), BF16),
            V((2, ROWS, 256), BF16),
            V((ROWS, 256), F32),
            DMA((6,)),
            DMA((5, 2, 16)),
            DMA((5, 2, 16)),
            DMA((2, 6)),
            DMA((2, 6)),
            DMA((2, 8)),
            DMA((2, 8)),
            DMA((8,)),
            DMA((8,)),
            DMA((6,)),
            DMA((6,)),
        ],
        compiler_params=pltpu.CompilerParams(
            collective_id=0, has_side_effects=True, vmem_limit_bytes=60 * 1024 * 1024
        ),
    )(
        tokens, gv, w_mixer_out, in1, in2, w_ff_down, spatial_gain.reshape(1, 128), w_spatial,
        bias, first_gain.reshape(1, D), taps, second_gain.reshape(8, 256),
    )


def solution(mesh):
    finer = Mesh(mesh.devices.reshape(4, 4, 4, 2), ("z", "y", "x", "c"))
    in_specs = (
        P(FS, None), P(FS, TP), P(FS, TP), P(TP), P(TP, None, None), P(TP, None), P(TP, FS), P(),
        P(FS, TP), P(FS, TP), P(None, TP), P(None, TP), P(TP, FS), P(),
    )
    return jax.shard_map(
        per_device, mesh=finer, in_specs=in_specs, out_specs=P(FS, TP), check_vma=False
    )
```

```python
import jax
import jax.numpy as jnp
from jax import lax
from jax.experimental import pallas as pl
from jax.experimental.pallas import tpu as pltpu
from jax.sharding import Mesh
from jax.sharding import PartitionSpec as P

ROWS = 1024
D = 2048
SG_WIDTH = 1024
SEQ = 256
FS = ("z", "y")
TP = ("x", "c")
SCALE = 2.0**0.25
EPS = 1e-05
F32 = jnp.float32
BF16 = jnp.bfloat16
MESH = pl.DeviceIdType.MESH


def mul(i, n):
    return pl.multiple_of(i, n)


def dot(a, b):
    return jnp.dot(a, b, preferred_element_type=F32)


ORDER = ((1, 0), (3, 0), (0, 1), (2, 0), (1, 3), (3, 3), (2, 1))
LAST = ((0, 3), (1, 1), (3, 1), (2, 3), (0, 2), (1, 2), (3, 2), (2, 2))


class PlaneGather:
    def __init__(self, block, pos, send_sem, recv_sem, flip=0, then=None):
        self.block, self.pos, self.then = block, pos, then
        self.send_sem, self.recv_sem = send_sem, recv_sem
        self.flip = flip

    def axes(self, half):
        return ("y", "z") if half == 0 else ("z", "y")

    def ref(self, half, d):
        a1, a2 = self.axes(half)
        at = {
            a1: lax.rem(self.pos[a1] + 4 - d[0], 4),
            a2: lax.rem(self.pos[a2] + 4 - d[1], 4),
        }
        return self.block(half, at["z"] * 4 + at["y"])

    def copy(self, half, target, source, axis, step):
        ref = self.ref(half, source)
        i = target[0] * 4 + target[1]
        return pltpu.make_async_remote_copy(
            src_ref=ref,
            dst_ref=ref,
            send_sem=self.send_sem.at[half, i],
            recv_sem=self.recv_sem.at[half, i],
            device_id={axis: lax.rem(self.pos[axis] + 4 + step, 4)},
            device_id_type=MESH,
        )

    def route(self, half, target):
        a1, a2 = self.axes(half)
        d1, d2 = target
        if d2 == 0:
            if d1 == 2:
                plus = (half + self.flip) % 2 == 0
                return ((1, 0), a1, 1) if plus else ((3, 0), a1, -1)
            return ((0, 0), a1, 1 if d1 == 1 else -1)
        if d2 == 2:
            return ((d1, 1), a2, 1) if d1 % 2 == 0 else ((d1, 3), a2, -1)
        return ((d1, 0), a2, 1 if d2 == 1 else -1)

    def send(self, half, target):
        source, axis, step = self.route(half, target)
        self.copy(half, target, source, axis, step).start()

    def after(self, half, source, first=True, second=True):
        for target in ((1, 0), (3, 0), (2, 0)):
            if first and self.route(half, target)[0] == source:
                self.send(half, target)
        for d1 in range(4) if second else ():
            for d2 in (1, 3, 2):
                if self.route(half, (d1, d2))[0] == source:
                    self.send(half, (d1, d2))

    def own(self, first=True, second=True):
        for half in (0, 1):
            self.after(half, (0, 0), first, second)
            if self.then:
                self.then(half, self.ref(half, (0, 0)))

    def arrived(self, half, d):
        i = d[0] * 4 + d[1]
        ref = self.ref(half, d)
        pltpu.make_async_remote_copy(
            src_ref=ref,
            dst_ref=ref,
            send_sem=self.send_sem.at[half, i],
            recv_sem=self.recv_sem.at[half, i],
            device_id={"y": lax.rem(self.pos["y"] + 1, 4)},
            device_id_type=MESH,
        ).wait_recv()
        if self.then:
            self.then(half, ref)

    def step(self, *which):
        for k in which:
            for half in (0, 1):
                self.arrived(half, ORDER[k])
                self.after(half, ORDER[k])

    def rest(self):
        for d in LAST:
            for half in (0, 1):
                self.arrived(half, d)

    def sent(self):
        for half in (0, 1):
            for d1 in range(4):
                for d2 in range(4):
                    if d1 or d2:
                        source, axis, step = self.route(half, (d1, d2))
                        self.copy(half, (d1, d2), source, axis, step).wait_send()


class RingGather:
    def __init__(self, block, x, send_sem, recv_sem):
        self.block, self.x = block, x
        self.send_sem, self.recv_sem = send_sem, recv_sem

    def copy(self, back, part, slot, step):
        ref = self.block(lax.rem(self.x + 4 - back, 4), part)
        return pltpu.make_async_remote_copy(
            src_ref=ref,
            dst_ref=ref,
            send_sem=self.send_sem.at[slot],
            recv_sem=self.recv_sem.at[slot],
            device_id={"x": lax.rem(self.x + 4 + step, 4)},
            device_id_type=MESH,
        )

    def sends(self):
        return ((0, 0, 0, 1), (0, 1, 1, -1), (0, 1, 2, 1), (0, 0, 3, -1), (1, 0, 4, 1), (3, 1, 5, -1))

    def own(self):
        for c in self.sends()[:4]:
            self.copy(*c).start()

    def piece(self, part, ref):
        for slot, step in ((0, 1), (3, -1)) if part == 0 else ((2, 1), (1, -1)):
            pltpu.make_async_remote_copy(
                src_ref=ref,
                dst_ref=ref,
                send_sem=self.send_sem.at[slot],
                recv_sem=self.recv_sem.at[slot],
                device_id={"x": lax.rem(self.x + 4 + step, 4)},
                device_id_type=MESH,
            ).start()

    def forward(self):
        self.copy(1, 0, 0, 1).wait_recv()
        self.copy(*self.sends()[4]).start()
        self.copy(3, 1, 1, 1).wait_recv()
        self.copy(*self.sends()[5]).start()

    def rest(self):
        self.copy(1, 1, 2, 1).wait_recv()
        self.copy(3, 0, 3, 1).wait_recv()
        self.copy(2, 0, 4, 1).wait_recv()
        self.copy(2, 1, 5, 1).wait_recv()

    def sent(self):
        for c in self.sends():
            self.copy(*c).wait_send()


class Stats:
    def __init__(self, ref, x, c, send_sem, recv_sem):
        self.ref, self.x, self.c = ref, x, c
        self.send_sem, self.recv_sem = send_sem, recv_sem

    def copies(self):
        out = []
        for k in (4, 5, 2, 6, 3, 7, 1):
            dx, dc = k // 2, k % 2
            out.append(
                pltpu.make_async_remote_copy(
                    src_ref=self.ref.at[0],
                    dst_ref=self.ref.at[k],
                    send_sem=self.send_sem.at[k],
                    recv_sem=self.recv_sem.at[k],
                    device_id={"x": lax.rem(self.x + dx, 4), "c": lax.rem(self.c + dc, 2)},
                    device_id_type=MESH,
                )
            )
        return out

    def start(self):
        for c in self.copies():
            c.start()

    def total(self):
        for c in self.copies():
            c.wait_recv()
        total = self.ref[0]
        for k in range(1, 8):
            total = total + self.ref[k]
        return total

    def sent(self):
        for c in self.copies():
            c.wait_send()


def spread(row):
    return jnp.broadcast_to(row, (128, 128)).T


def kernel(
    tok_h, gate_h, value_h, mo_h, fg_h, fu_h, wd_h, gain, wsp, bias, g1, taps_g, taps_u, g2,
    out,
    tok, wgt, wvl, mo, wfg, wfu, wd, ga, va, st1, st2, tot, so, taps,
    msend, mrecv, mown, fn, hid, dsend, drecv, xs, xr2, xr1, acc,
    lsem, psend, precv, rsend, rrecv, ssend, srecv, dss, drs, dds, ddr, xss, xrs,
):
    z, y = lax.axis_index("z"), lax.axis_index("y")
    x, c = lax.axis_index("x"), lax.axis_index("c")
    pos = {"z": z, "y": y}
    f = z * 4 + y
    j = x * 2 + c
    sib = {"c": 1 - c}

    def gv_block(half, b):
        return (wgt, wvl)[half].at[pl.ds(mul(b * 128, 128), 128), :]

    def mo_block(half, b):
        return mo.at[b, pl.ds(mul(x * 128 + half * 64, 64), 64), :]

    def in1_block(half, b):
        return (wfg, wfu)[half].at[b, pl.ds(0, 384), :]

    def in2_block(half, b):
        return (wfg, wfu)[half].at[b, pl.ds(384, 320), :]

    def wd_block(half, b):
        return wd.at[b, pl.ds(half * 352, 352), :]

    r_mo = RingGather(
        lambda b, part: mo.at[:, pl.ds(mul(b * 128 + part * 64, 64), 64), :], x, rsend.at[0], rrecv.at[0]
    )
    r_so = RingGather(lambda b, part: so.at[b, pl.ds(part * 512, 512), :], x, rsend.at[1], rrecv.at[1])
    g_gv = PlaneGather(gv_block, pos, psend.at[0], precv.at[0], 0)
    g_mo = PlaneGather(mo_block, pos, psend.at[1], precv.at[1], 1, r_mo.piece)
    g_in1 = PlaneGather(in1_block, pos, psend.at[2], precv.at[2], 0)
    g_in2 = PlaneGather(in2_block, pos, psend.at[3], precv.at[3], 1)
    g_wd = PlaneGather(wd_block, pos, psend.at[4], precv.at[4], 0)
    s1 = Stats(st1, x, c, ssend.at[0], srecv.at[0])
    s2 = Stats(st2, x, c, ssend.at[1], srecv.at[1])

    rows_f = pl.ds(mul(f * 128, 128), 128)
    loads = [
        pltpu.make_async_copy(gate_h, wgt.at[rows_f, :], lsem.at[0]),
        pltpu.make_async_copy(value_h, wvl.at[rows_f, :], lsem.at[1]),
        pltpu.make_async_copy(mo_h, mo.at[f, pl.ds(mul(x * 128, 128), 128), :], lsem.at[2]),
        pltpu.make_async_copy(fg_h, wfg.at[f], lsem.at[3]),
        pltpu.make_async_copy(fu_h, wfu.at[f], lsem.at[4]),
        pltpu.make_async_copy(wd_h, wd.at[f, pl.ds(0, 704), :], lsem.at[5]),
        pltpu.make_async_copy(tok_h, tok, lsem.at[6]),
    ]
    for l in loads:
        l.start()

    barrier = pltpu.get_barrier_semaphore()
    peers = [{a: lax.rem(pos[a] + s, 4)} for a in ("y", "z") for s in (1, 3)]
    peers += [
        {"x": lax.rem(x + k // 2, 4), "c": lax.rem(c + k % 2, 2)} for k in range(1, 8)
    ]
    for p in peers:
        pl.semaphore_signal(barrier, inc=1, device_id=p, device_id_type=MESH)
    for b in range(16):
        wd[b, 704:768, :] = jnp.zeros((64, 128), BF16)
    for i in range(5):
        t = slice(i * 128, i * 128 + 128)
        taps[0:3, i * 256 : i * 256 + 128] = taps_g[:, t]
        taps[0:3, i * 256 + 128 : i * 256 + 256] = taps_u[:, t]
    taps[0:3, 1280:1344] = taps_g[:, 640:704]
    taps[0:3, 1344:1408] = taps_u[:, 640:704]
    for k in range(3):
        loads[k].wait()
    pl.semaphore_wait(barrier, len(peers))

    g_mo.own()
    g_gv.own()
    g_mo.step(0, 1)
    g_gv.step(0, 1)
    g_mo.step(2, 3)
    g_gv.step(2, 3)
    loads[3].wait()
    loads[4].wait()
    g_in1.own(second=False)
    g_mo.step(4, 5, 6)
    g_gv.step(4, 5, 6)
    g_in1.own(first=False)
    g_mo.rest()
    g_gv.rest()
    loads[6].wait()
    g_in1.step(0, 1)

    @pl.loop(0, 4)
    def _(i):
        r = pl.ds(mul(i * 256, 256), 256)
        pre = dot(tok[r, :], jnp.concatenate([wgt[...], wvl[...]], axis=1))
        act = jax.nn.gelu(pre)
        ga[r, :] = act[:, :128]
        va[r, :] = act[:, 128:]
        for h in range(2):
            v = act[h * 128 : h * 128 + 128, 128:].T
            st1[0, pl.ds(i * 2 + h, 1), :] = jnp.sum(v, axis=0, keepdims=True)
            st1[0, pl.ds(i * 2 + h + 8, 1), :] = jnp.sum(v * v, axis=0, keepdims=True)

    s1.start()
    g_in1.step(2)
    g_in2.own(second=False)
    r_mo.forward()
    tot[...] = s1.total()

    lane = lax.broadcasted_iota(jnp.int32, (128, 128), 1)
    low = lax.broadcasted_iota(jnp.int32, (128, 128), 0) >= lane
    w0 = jnp.where(low, wsp[0], jnp.zeros((128, 128), BF16))
    w1 = jnp.where(low, wsp[1], jnp.zeros((128, 128), BF16))
    shift = jnp.where(lane < 64, spread(bias[0:1, :]), spread(bias[1:2, :]))

    @pl.loop(0, 8)
    def _(n):
        r = pl.ds(mul(n * 128, 128), 128)
        mean = spread(tot[pl.ds(n, 1), :] * (1.0 / SG_WIDTH))
        square = spread(tot[pl.ds(n + 8, 1), :] * (1.0 / SG_WIDTH))
        inv = lax.rsqrt(square - mean * mean + EPS)
        vn = ((va[r, :] - mean) * inv * gain[...]).astype(BF16)
        mixed = jnp.where(lane < 64, dot(w0, vn), dot(w1, vn)) + shift
        so[x, r, :] = (ga[r, :] * mixed).astype(BF16)

    r_so.own()
    g_in1.step(3)
    g_in2.own(first=False)
    g_in1.step(4, 5, 6)
    g_in2.step(0, 1)
    r_so.forward()
    g_in2.step(2, 3)
    loads[5].wait()
    g_wd.own()
    r_mo.rest()
    r_so.rest()

    theirs = (1 - c) * 512
    mine = c * 512

    def mix_copy(k):
        return pltpu.make_async_remote_copy(
            src_ref=msend.at[pl.ds(k * 256, 256), :],
            dst_ref=mrecv.at[pl.ds(k * 256, 256), :],
            send_sem=dss.at[k], recv_sem=drs.at[k], device_id=sib, device_id_type=MESH,
        )

    def fn_copy(k, base):
        ref = fn.at[pl.ds(mul(base + k * 256, 256), 256), :]
        return pltpu.make_async_remote_copy(
            src_ref=ref, dst_ref=ref,
            send_sem=dss.at[2 + k], recv_sem=drs.at[2 + k], device_id=sib, device_id_type=MESH,
        )

    def mix(base, i):
        r = pl.ds(mul(base, 256), 256)
        left = jnp.concatenate([so[b, r, :] for b in range(4)], axis=1)
        return dot(left, jnp.concatenate([mo[i * 4 + q] for q in range(4)], axis=1))

    for k in range(2):
        @pl.loop(0, 4)
        def _(i):
            msend[k * 256 : k * 256 + 256, pl.ds(mul(i * 512, 512), 512)] = mix(
                theirs + k * 256, i
            ).astype(BF16)

        mix_copy(k).start()
    for k in range(2):
        @pl.loop(0, 4)
        def _(i):
            mown[k * 256 : k * 256 + 256, pl.ds(mul(i * 512, 512), 512)] = mix(mine + k * 256, i)

    g_in2.step(4, 5, 6)
    g_wd.step(0, 1)
    for k in range(2):
        mix_copy(k).wait_recv()

        @pl.loop(0, 8)
        def _(i):
            r = pl.ds(mul(k * 256 + i * 32, 32), 32)
            g = pl.ds(mul(mine + k * 256 + i * 32, 32), 32)
            v = SCALE * tok[g, :].astype(F32) + (mown[r, :] + mrecv[r, :].astype(F32))
            mean = jnp.sum(v, axis=1, keepdims=True) * (1.0 / D)
            square = jnp.sum(v * v, axis=1, keepdims=True) * (1.0 / D)
            inv = lax.rsqrt(square - mean * mean + EPS)
            fn[g, :] = ((v - mean) * inv * g1[...]).astype(BF16)

        fn_copy(k, mine).start()

    g_in1.rest()
    g_wd.step(2, 3)

    row = lax.broadcasted_iota(jnp.int32, (SEQ, 256), 0)
    lane2 = lax.broadcasted_iota(jnp.int32, (SEQ, 128), 1)

    def conv(p, t):
        n = p.shape[1]
        p1 = jnp.where(row[:, :n] >= 1, pltpu.roll(p, 1, 0), 0.0)
        p2 = jnp.where(row[:, :n] >= 2, pltpu.roll(p, 2, 0), 0.0)
        return p2 * t[0:1, :] + p1 * t[1:2, :] + p * t[2:3, :]

    def dot_t(a, rows):
        w = jnp.concatenate(
            [jnp.concatenate([buf[b, rows, :] for b in range(16)], axis=1) for buf in (wfg, wfu)],
            axis=0,
        )
        return lax.dot_general(a, w, (((1,), (1,)), ((), ())), preferred_element_type=F32)

    def hidden(seq, tile):
        r = pl.ds(mul(seq * SEQ, SEQ), SEQ)
        p = dot_t(fn[r, :], pl.ds(mul(tile * 128, 128), 128))
        q = conv(p, taps[:, pl.ds(mul(tile * 256, 256), 256)])
        hid[r, pl.ds(mul(tile * 128, 128), 128)] = (
            jax.nn.silu(q[:, :128]) * q[:, 128:]
        ).astype(BF16)

    def hidden_last(seq):
        r = pl.ds(mul(seq * SEQ, SEQ), SEQ)
        p = dot_t(fn[r, :], pl.ds(640, 64))
        q = conv(p, taps[:, 1280:1408])
        h = jax.nn.silu(q) * pltpu.roll(q, 64, 1)
        hid[r, 640:768] = jnp.where(lane2 < 64, h, 0.0).astype(BF16)

    own_seq = c * 2
    other_seq = (1 - c) * 2

    def part1(first):
        @pl.loop(0, 6)
        def _(i):
            hidden(first + i // 3, i % 3)

    def part2(first):
        @pl.loop(0, 4)
        def _(i):
            hidden(first + i // 2, 3 + i % 2)

        @pl.loop(0, 2)
        def _(i):
            hidden_last(first + i)

    part1(own_seq)
    g_wd.step(4, 5, 6)
    for k in range(2):
        fn_copy(k, (1 - c) * 512).wait_recv()
    part1(other_seq)
    g_in2.rest()
    part2(own_seq)
    part2(other_seq)
    g_wd.rest()

    hops = (2, 1, 3, 0)

    def dd_copy(k, h):
        r = pl.ds(h * 512, 512)
        return pltpu.make_async_remote_copy(
            src_ref=dsend.at[k, r, :], dst_ref=drecv.at[k, r, :],
            send_sem=dds.at[k, h], recv_sem=ddr.at[k, h], device_id=sib, device_id_type=MESH,
        )

    def down(k, i, parity):
        b = (lax.rem(x + hops[k], 4) * 2 + parity) * 2
        return dot(
            hid[pl.ds(mul(i * 256, 256), 256), :], jnp.concatenate([wd[b], wd[b + 1]], axis=1)
        )

    def down_theirs(k, h):
        @pl.loop(h * 2, h * 2 + 2)
        def _(i):
            dsend[k, pl.ds(mul(i * 256, 256), 256), :] = down(k, i, 1 - c).astype(BF16)

        dd_copy(k, h).start()

    def x_copy(slot, src, dst, step):
        return pltpu.make_async_remote_copy(
            src_ref=src, dst_ref=dst, send_sem=xss.at[slot], recv_sem=xrs.at[slot],
            device_id={"x": lax.rem(x + 4 + step, 4)}, device_id_type=MESH,
        )

    up, lo = pl.ds(0, 512), pl.ds(512, 512)
    x_copies = (
        x_copy(0, xs.at[0, up], xr2.at[up], 1),
        x_copy(1, xs.at[0, lo], xr2.at[lo], -1),
        x_copy(2, xs.at[1, lo], xr1.at[0, lo], 1),
        x_copy(3, xs.at[2, up], xr1.at[1, up], -1),
        x_copy(4, xs.at[1, up], xr1.at[0, up], 1),
        x_copy(5, xs.at[2, lo], xr1.at[1, lo], -1),
    )

    def fill(k, h, slot, extra=False):
        dd_copy(k, h).wait_recv()

        @pl.loop(h * 2, h * 2 + 2)
        def _(i):
            r = pl.ds(mul(i * 256, 256), 256)
            v = down(k, i, c) + drecv[k, r, :].astype(F32)
            if extra:
                v = v + xr2[r, :].astype(F32)
            xs[k, r, :] = v.astype(BF16)

        x_copies[slot].start()

    down_theirs(0, 0)
    down_theirs(0, 1)
    down_theirs(1, 1)
    fill(0, 0, 0)
    fill(0, 1, 1)
    down_theirs(2, 0)
    fill(1, 1, 2)
    fill(2, 0, 3)
    down_theirs(1, 0)
    down_theirs(2, 1)
    down_theirs(3, 0)
    down_theirs(3, 1)
    x_copies[0].wait_recv()
    fill(1, 0, 4, True)
    x_copies[1].wait_recv()
    fill(2, 1, 5, True)
    for h in range(2):
        dd_copy(3, h).wait_recv()

        @pl.loop(h * 2, h * 2 + 2)
        def _(i):
            r = pl.ds(mul(i * 256, 256), 256)
            acc[r, :] = (
                down(3, i, c)
                + drecv[3, r, :].astype(F32)
                + SCALE * fn[r, pl.ds(mul(j * 256, 256), 256)].astype(F32)
            )

    for g in (g_gv, g_mo, g_in1, g_in2, g_wd, r_mo, r_so, s1):
        g.sent()
    for k in range(2):
        mix_copy(k).wait_send()
        fn_copy(k, mine).wait_send()
    for k in range(4):
        for h in range(2):
            dd_copy(k, h).wait_send()
    for k in (2, 3, 4, 5):
        x_copies[k].wait_recv()

    @pl.loop(0, 8)
    def _(n):
        r = pl.ds(mul(n * 128, 128), 128)
        v = acc[r, :] + (xr1[0, r, :].astype(F32) + xr1[1, r, :].astype(F32))
        acc[r, :] = v
        a, b = v[:, :128], v[:, 128:]
        st2[0, pl.ds(n, 1), :] = jnp.sum((a + b).T, axis=0, keepdims=True)
        st2[0, pl.ds(n + 8, 1), :] = jnp.sum((a * a + b * b).T, axis=0, keepdims=True)

    s2.start()
    gain2 = g2[:, pl.ds(mul(j * 256, 256), 256)]
    for k in range(6):
        x_copies[k].wait_send()
    tot[...] = s2.total()

    @pl.loop(0, 8)
    def _(n):
        r = pl.ds(mul(n * 128, 128), 128)
        mean = spread(tot[pl.ds(n, 1), :] * (1.0 / D))
        square = spread(tot[pl.ds(n + 8, 1), :] * (1.0 / D))
        inv = lax.rsqrt(square - mean * mean + EPS)
        for h in range(2):
            cols = slice(h * 128, h * 128 + 128)
            out[r, cols] = ((acc[r, cols] - mean) * inv * gain2[:, cols]).astype(BF16)

    s2.sent()


def per_device(
    tokens, w_gate_side, w_value_side, spatial_gain, w_spatial, spatial_bias, w_mixer_out,
    first_gain, w_ff_gate, w_ff_up, conv_gate_taps, conv_up_taps, w_ff_down, second_gain,
):
    vmem = pl.BlockSpec(memory_space=pltpu.VMEM)
    hbm = pl.BlockSpec(memory_space=pl.ANY)
    V, DMA = pltpu.VMEM, pltpu.SemaphoreType.DMA
    return pl.pallas_call(
        kernel,
        out_shape=jax.ShapeDtypeStruct((ROWS, 256), BF16),
        in_specs=[hbm] * 7 + [vmem] * 7,
        out_specs=vmem,
        scratch_shapes=[
            V((ROWS, D), BF16),
            V((D, 128), BF16),
            V((D, 128), BF16),
            V((16, 512, 128), BF16),
            V((16, 704, 128), BF16),
            V((16, 704, 128), BF16),
            V((16, 768, 128), BF16),
            V((ROWS, 128), F32),
            V((ROWS, 128), F32),
            V((8, 16, 128), F32),
            V((8, 16, 128), F32),
            V((16, 128), F32),
            V((4, ROWS, 128), BF16),
            V((8, 1408), F32),
            V((512, D), BF16),
            V((512, D), BF16),
            V((512, D), F32),
            V((ROWS, D), BF16),
            V((ROWS, 768), BF16),
            V((4, ROWS, 256), BF16),
            V((4, ROWS, 256), BF16),
            V((3, ROWS, 256), BF16),
            V((ROWS, 256), BF16),
            V((2, ROWS, 256), BF16),
            V((ROWS, 256), F32),
            DMA((7,)),
            DMA((5, 2, 16)),
            DMA((5, 2, 16)),
            DMA((2, 6)),
            DMA((2, 6)),
            DMA((2, 8)),
            DMA((2, 8)),
            DMA((4,)),
            DMA((4,)),
            DMA((4, 2)),
            DMA((4, 2)),
            DMA((6,)),
            DMA((6,)),
        ],
        compiler_params=pltpu.CompilerParams(
            collective_id=0, has_side_effects=True, vmem_limit_bytes=60 * 1024 * 1024
        ),
    )(
        tokens, w_gate_side, w_value_side, w_mixer_out, w_ff_gate.T, w_ff_up.T, w_ff_down,
        spatial_gain.reshape(1, 128), w_spatial, spatial_bias, first_gain.reshape(1, D),
        conv_gate_taps, conv_up_taps, second_gain.reshape(1, D),
    )


def solution(mesh):
    finer = Mesh(mesh.devices.reshape(4, 4, 4, 2), ("z", "y", "x", "c"))
    in_specs = (
        P(FS, None), P(FS, TP), P(FS, TP), P(TP), P(TP, None, None), P(TP, None), P(TP, FS), P(),
        P(FS, TP), P(FS, TP), P(None, TP), P(None, TP), P(TP, FS), P(),
    )
    return jax.shard_map(
        per_device, mesh=finer, in_specs=in_specs, out_specs=P(FS, TP), check_vma=False
    )
```

```python
import jax
import jax.numpy as jnp
from jax import lax
from jax.experimental import pallas as pl
from jax.experimental.pallas import tpu as pltpu
from jax.sharding import Mesh
from jax.sharding import PartitionSpec as P

ROWS = 1024
D = 2048
SG_WIDTH = 1024
SEQ = 256
FS = ("z", "y")
TP = ("x", "c")
SCALE = 2.0**0.25
EPS = 1e-05
F32 = jnp.float32
BF16 = jnp.bfloat16
MESH = pl.DeviceIdType.MESH


def mul(i, n):
    return pl.multiple_of(i, n)


def dot(a, b):
    return jnp.dot(a, b, preferred_element_type=F32)


ORDER = ((1, 0), (3, 0), (0, 1), (2, 0), (1, 3), (3, 3), (2, 1))
LAST = ((0, 3), (1, 1), (3, 1), (2, 3), (0, 2), (1, 2), (3, 2), (2, 2))


class PlaneGather:
    def __init__(self, block, pos, send_sem, recv_sem, flip=0, then=None, direct=False):
        self.block, self.pos, self.then, self.direct = block, pos, then, direct
        self.send_sem, self.recv_sem = send_sem, recv_sem
        self.flip = flip

    def axes(self, half):
        return ("y", "z") if half == 0 else ("z", "y")

    def ref(self, half, d):
        a1, a2 = self.axes(half)
        at = {
            a1: lax.rem(self.pos[a1] + 4 - d[0], 4),
            a2: lax.rem(self.pos[a2] + 4 - d[1], 4),
        }
        return self.block(half, at["z"] * 4 + at["y"])

    def copy(self, half, target, source, axis, step):
        ref = self.ref(half, source)
        i = target[0] * 4 + target[1]
        return pltpu.make_async_remote_copy(
            src_ref=ref,
            dst_ref=ref,
            send_sem=self.send_sem.at[half, i],
            recv_sem=self.recv_sem.at[half, i],
            device_id={axis: lax.rem(self.pos[axis] + 4 + step, 4)},
            device_id_type=MESH,
        )

    def route(self, half, target):
        a1, a2 = self.axes(half)
        d1, d2 = target
        if self.direct:
            return ((d1, 0), a2, d2) if d2 else ((0, 0), a1, d1)
        if d2 == 0:
            if d1 == 2:
                plus = (half + self.flip) % 2 == 0
                return ((1, 0), a1, 1) if plus else ((3, 0), a1, -1)
            return ((0, 0), a1, 1 if d1 == 1 else -1)
        if d2 == 2:
            return ((d1, 1), a2, 1) if d1 % 2 == 0 else ((d1, 3), a2, -1)
        return ((d1, 0), a2, 1 if d2 == 1 else -1)

    def send(self, half, target):
        source, axis, step = self.route(half, target)
        self.copy(half, target, source, axis, step).start()

    def after(self, half, source, first=True, second=True):
        for target in ((1, 0), (3, 0), (2, 0)):
            if first and self.route(half, target)[0] == source:
                self.send(half, target)
        for d1 in range(4) if second else ():
            for d2 in (1, 3, 2):
                if self.route(half, (d1, d2))[0] == source:
                    self.send(half, (d1, d2))

    def own(self, first=True, second=True):
        for half in (0, 1):
            self.after(half, (0, 0), first, second)
            if self.then and first:
                self.then(half, self.ref(half, (0, 0)))

    def arrived(self, half, d):
        i = d[0] * 4 + d[1]
        ref = self.ref(half, d)
        pltpu.make_async_remote_copy(
            src_ref=ref,
            dst_ref=ref,
            send_sem=self.send_sem.at[half, i],
            recv_sem=self.recv_sem.at[half, i],
            device_id={"y": lax.rem(self.pos["y"] + 1, 4)},
            device_id_type=MESH,
        ).wait_recv()
        if self.then:
            self.then(half, ref)

    def step(self, *which):
        for k in which:
            for half in (0, 1):
                self.arrived(half, ORDER[k])
                self.after(half, ORDER[k])

    def rest(self):
        for d in LAST + (tuple(ORDER[k] for k in (2, 4, 5, 6)) if self.direct else ()):
            for half in (0, 1):
                self.arrived(half, d)

    def sent(self):
        for half in (0, 1):
            for d1 in range(4):
                for d2 in range(4):
                    if d1 or d2:
                        source, axis, step = self.route(half, (d1, d2))
                        self.copy(half, (d1, d2), source, axis, step).wait_send()


class RingGather:
    def __init__(self, block, x, send_sem, recv_sem, chunks):
        self.block, self.x, self.chunks = block, x, chunks
        self.send_sem, self.recv_sem = send_sem, recv_sem

    def move(self, ref, slot, step):
        return pltpu.make_async_remote_copy(
            src_ref=ref,
            dst_ref=ref,
            send_sem=self.send_sem.at[slot],
            recv_sem=self.recv_sem.at[slot],
            device_id={"x": lax.rem(self.x + 4 + step, 4)},
            device_id_type=MESH,
        )

    def copy(self, back, part, slot, step):
        return self.move(self.block(lax.rem(self.x + 4 - back, 4), part), slot, step)

    def far_copy(self, back, part, chunk, step):
        b = lax.rem(self.x + 4 - back, 4)
        slot = 4 + part * self.chunks + chunk
        return self.move(self.block(b, part, chunk), slot, step)

    def sends(self):
        return ((0, 0, 0, 1), (0, 1, 1, -1), (0, 1, 2, 1), (0, 0, 3, -1))

    def own(self, part):
        for c in self.sends():
            if c[1] == part:
                self.copy(*c).start()

    def piece(self, part, ref):
        for slot, step in ((0, 1), (3, -1)) if part == 0 else ((2, 1), (1, -1)):
            self.move(ref, slot, step).start()

    def forward(self, chunk):
        if chunk == 0:
            self.copy(1, 0, 0, 1).wait_recv()
        self.far_copy(1, 0, chunk, 1).start()
        if chunk == 0:
            self.copy(3, 1, 1, 1).wait_recv()
        self.far_copy(3, 1, chunk, -1).start()

    def near(self):
        self.copy(1, 1, 2, 1).wait_recv()
        self.copy(3, 0, 3, 1).wait_recv()

    def far(self):
        for chunk in range(self.chunks):
            for part in (0, 1):
                self.far_copy(2, part, chunk, 1).wait_recv()

    def sent(self):
        for c in self.sends():
            self.copy(*c).wait_send()
        for chunk in range(self.chunks):
            self.far_copy(1, 0, chunk, 1).wait_send()
            self.far_copy(3, 1, chunk, -1).wait_send()


class Stats:
    def __init__(self, ref, x, c, send_sem, recv_sem):
        self.ref, self.x, self.c = ref, x, c
        self.send_sem, self.recv_sem = send_sem, recv_sem

    def copies(self):
        out = []
        for k in (4, 5, 2, 6, 3, 7, 1):
            dx, dc = k // 2, k % 2
            out.append(
                pltpu.make_async_remote_copy(
                    src_ref=self.ref.at[0],
                    dst_ref=self.ref.at[k],
                    send_sem=self.send_sem.at[k],
                    recv_sem=self.recv_sem.at[k],
                    device_id={"x": lax.rem(self.x + dx, 4), "c": lax.rem(self.c + dc, 2)},
                    device_id_type=MESH,
                )
            )
        return out

    def start(self):
        for c in self.copies():
            c.start()

    def total(self):
        for c in self.copies():
            c.wait_recv()
        total = self.ref[0]
        for k in range(1, 8):
            total = total + self.ref[k]
        return total

    def sent(self):
        for c in self.copies():
            c.wait_send()


def spread(row):
    return jnp.broadcast_to(row, (128, 128)).T


def kernel(
    tok_h, gate_h, value_h, mo_h, fg_h, fu_h, wd_h, gain_h, wsp_h, bias_h, g1_h, tg_h, tu_h, g2_h,
    out,
    tok, wgt, wvl, mo, wfg, wfu, wd, ga, va, st1, st2, tot, so, taps, gain, wsp, bias, g1, taps_g, taps_u, g2,
    msend, mrecv, mown, mtheir, fn, hid, dsend, drecv, xs, xr2, xr1, acc,
    lsem, psend, precv, rsend, rrecv, ssend, srecv, dss, drs, dds, ddr, xss, xrs,
):
    z, y = lax.axis_index("z"), lax.axis_index("y")
    x, c = lax.axis_index("x"), lax.axis_index("c")
    pos = {"z": z, "y": y}
    f = z * 4 + y
    j = x * 2 + c
    sib = {"c": 1 - c}

    def gv_block(half, b):
        return (wgt, wvl)[half].at[pl.ds(mul(b * 128, 128), 128), :]

    def mo_block(half, b):
        return mo.at[b, pl.ds(mul(x * 128 + half * 64, 64), 64), :]

    def in1_block(half, b):
        return (wfg, wfu)[half].at[b, pl.ds(0, 384), :]

    def in2_block(half, b):
        return (wfg, wfu)[half].at[b, pl.ds(384, 320), :]

    def wd_block(half, b):
        return wd.at[b, pl.ds(half * 352, 352), :]

    def mo_ring(b, part, chunk=None):
        cut = slice(None) if chunk is None else pl.ds(chunk * 8, 8)
        return mo.at[cut, pl.ds(mul(b * 128 + part * 64, 64), 64), :]

    def so_ring(b, part, chunk=None):
        return so.at[b, pl.ds(part * 512, 512), :]

    r_mo = RingGather(mo_ring, x, rsend.at[0], rrecv.at[0], 2)
    r_so = RingGather(so_ring, x, rsend.at[1], rrecv.at[1], 1)
    g_gv = PlaneGather(gv_block, pos, psend.at[0], precv.at[0], 0)
    g_mo = PlaneGather(mo_block, pos, psend.at[1], precv.at[1], 1, r_mo.piece)
    g_in1 = PlaneGather(in1_block, pos, psend.at[2], precv.at[2], 0)
    g_in2 = PlaneGather(in2_block, pos, psend.at[3], precv.at[3], 1)
    g_wd = PlaneGather(wd_block, pos, psend.at[4], precv.at[4], 0)
    s1 = Stats(st1, x, c, ssend.at[0], srecv.at[0])
    s2 = Stats(st2, x, c, ssend.at[1], srecv.at[1])

    rows_f = pl.ds(mul(f * 128, 128), 128)
    loads = [
        pltpu.make_async_copy(gate_h, wgt.at[rows_f, :], lsem.at[0]),
        pltpu.make_async_copy(value_h, wvl.at[rows_f, :], lsem.at[1]),
        pltpu.make_async_copy(mo_h, mo.at[f, pl.ds(mul(x * 128, 128), 128), :], lsem.at[2]),
        pltpu.make_async_copy(fg_h, wfg.at[f], lsem.at[3]),
        pltpu.make_async_copy(fu_h, wfu.at[f], lsem.at[4]),
        pltpu.make_async_copy(wd_h, wd.at[f, pl.ds(0, 704), :], lsem.at[5]),
        pltpu.make_async_copy(tok_h, tok, lsem.at[6]),
    ]
    small = [
        pltpu.make_async_copy(a, b, lsem.at[7 + k])
        for k, (a, b) in enumerate(
            zip(
                (tg_h, tu_h, gain_h, wsp_h, bias_h, g1_h, g2_h),
                (taps_g, taps_u, gain, wsp, bias, g1, g2),
            )
        )
    ]
    for l in loads + small:
        l.start()

    barrier = pltpu.get_barrier_semaphore()
    peers = [{a: lax.rem(pos[a] + s, 4)} for a in ("y", "z") for s in (1, 3)]
    peers += [
        {"x": lax.rem(x + k // 2, 4), "c": lax.rem(c + k % 2, 2)} for k in range(1, 8)
    ]
    for p in peers:
        pl.semaphore_signal(barrier, inc=1, device_id=p, device_id_type=MESH)
    for b in range(16):
        wd[b, 704:768, :] = jnp.zeros((64, 128), BF16)
    for l in small:
        l.wait()
    for i in range(5):
        t = slice(i * 128, i * 128 + 128)
        taps[0:3, i * 256 : i * 256 + 128] = taps_g[:, t]
        taps[0:3, i * 256 + 128 : i * 256 + 256] = taps_u[:, t]
    taps[0:3, 1280:1344] = taps_g[:, 640:704]
    taps[0:3, 1344:1408] = taps_u[:, 640:704]
    for k in range(3):
        loads[k].wait()
    pl.semaphore_wait(barrier, len(peers))

    g_mo.own(second=False)
    g_gv.own(second=False)
    loads[3].wait()
    loads[4].wait()
    g_in1.own(second=False)
    g_gv.own(first=False)
    g_mo.step(0)
    g_mo.step(1)
    g_gv.step(1)
    g_gv.step(0)
    g_mo.own(first=False)
    g_in1.step(1)
    g_gv.step(5)
    g_mo.step(3)
    g_mo.step(5)
    g_gv.step(3)
    g_gv.step(4)
    g_mo.step(2)
    g_mo.step(4)
    g_in2.own(second=False)
    g_gv.step(2)
    g_mo.step(6)
    g_gv.step(6)
    g_in1.step(0)
    loads[5].wait()
    g_wd.own(second=False)
    g_mo.rest()
    g_in1.own(first=False)
    g_gv.rest()
    loads[6].wait()
    @pl.loop(0, 4)
    def _(i):
        r = pl.ds(mul(i * 256, 256), 256)
        pre = dot(tok[r, :], jnp.concatenate([wgt[...], wvl[...]], axis=1))
        act = jax.nn.gelu(pre)
        ga[r, :] = act[:, :128]
        va[r, :] = act[:, 128:]
        for h in range(2):
            v = act[h * 128 : h * 128 + 128, 128:].T
            st1[0, pl.ds(i * 2 + h, 1), :] = jnp.sum(v, axis=0, keepdims=True)
            st1[0, pl.ds(i * 2 + h + 8, 1), :] = jnp.sum(v * v, axis=0, keepdims=True)

    s1.start()
    g_in2.step(0)
    r_mo.forward(0)
    g_in2.step(1)
    g_wd.step(0)
    tot[...] = s1.total()
    lane = lax.broadcasted_iota(jnp.int32, (128, 128), 1)
    low = lax.broadcasted_iota(jnp.int32, (128, 128), 0) >= lane
    w0 = jnp.where(low, wsp[0], jnp.zeros((128, 128), BF16))
    w1 = jnp.where(low, wsp[1], jnp.zeros((128, 128), BF16))
    shift = jnp.where(lane < 64, spread(bias[0:1, :]), spread(bias[1:2, :]))

    for part in range(2):
        @pl.loop(part * 4, part * 4 + 4)
        def _(n):
            r = pl.ds(mul(n * 128, 128), 128)
            mean = spread(tot[pl.ds(n, 1), :] * (1.0 / SG_WIDTH))
            square = spread(tot[pl.ds(n + 8, 1), :] * (1.0 / SG_WIDTH))
            inv = lax.rsqrt(square - mean * mean + EPS)
            vn = ((va[r, :] - mean) * inv * gain[...]).astype(BF16)
            mixed = jnp.where(lane < 64, dot(w0, vn), dot(w1, vn)) + shift
            so[x, r, :] = (ga[r, :] * mixed).astype(BF16)

        r_so.own(part)

    g_wd.step(1)
    r_mo.forward(1)
    g_in1.step(3)
    g_in2.step(3)
    g_in2.own(first=False)
    g_in1.step(2)
    g_in1.step(4)
    r_so.forward(0)
    r_mo.near()
    r_so.near()
    g_in1.step(5)
    theirs = (1 - c) * 512
    mine = c * 512

    def mix_copy(k):
        return pltpu.make_async_remote_copy(
            src_ref=msend.at[pl.ds(k * 256, 256), :],
            dst_ref=mrecv.at[pl.ds(k * 256, 256), :],
            send_sem=dss.at[k], recv_sem=drs.at[k], device_id=sib, device_id_type=MESH,
        )

    def fn_copy(k, base):
        ref = fn.at[pl.ds(mul(base + k * 256, 256), 256), :]
        return pltpu.make_async_remote_copy(
            src_ref=ref, dst_ref=ref,
            send_sem=dss.at[2 + k], recv_sem=drs.at[2 + k], device_id=sib, device_id_type=MESH,
        )

    def mix(base, i, blocks):
        r = pl.ds(mul(base, 256), 256)
        left = jnp.concatenate([so[b, r, :] for b in blocks], axis=1)
        right = jnp.concatenate(
            [
                jnp.concatenate([mo[i * 4 + q, pl.ds(mul(b * 128, 128), 128), :] for b in blocks], axis=0)
                for q in range(4)
            ],
            axis=1,
        )
        return dot(left, right)

    near = (x, lax.rem(x + 3, 4))
    far = (lax.rem(x + 1, 4), lax.rem(x + 2, 4))

    for k in range(2):
        @pl.loop(0, 4)
        def _(i):
            at = (slice(k * 256, k * 256 + 256), pl.ds(mul(i * 512, 512), 512))
            mtheir[at] = mix(theirs + k * 256, i, near)
            mown[at] = mix(mine + k * 256, i, near)

    g_in1.step(6)
    g_wd.own(first=False)
    g_in2.step(4)
    g_in2.step(5)
    g_in2.step(6)
    r_mo.far()
    r_so.far()
    g_wd.step(4)
    g_wd.step(3)
    for k in range(2):
        @pl.loop(0, 4)
        def _(i):
            at = (slice(k * 256, k * 256 + 256), pl.ds(mul(i * 512, 512), 512))
            msend[at] = (mtheir[at] + mix(theirs + k * 256, i, far)).astype(BF16)

        mix_copy(k).start()
    for k in range(2):
        @pl.loop(0, 4)
        def _(i):
            at = (slice(k * 256, k * 256 + 256), pl.ds(mul(i * 512, 512), 512))
            mown[at] = mown[at] + mix(mine + k * 256, i, far)

    g_in2.step(2)
    g_wd.step(5)
    for k in range(2):
        mix_copy(k).wait_recv()

        @pl.loop(0, 8)
        def _(i):
            r = pl.ds(mul(k * 256 + i * 32, 32), 32)
            g = pl.ds(mul(mine + k * 256 + i * 32, 32), 32)
            v = SCALE * tok[g, :].astype(F32) + (mown[r, :] + mrecv[r, :].astype(F32))
            mean = jnp.sum(v, axis=1, keepdims=True) * (1.0 / D)
            square = jnp.sum(v * v, axis=1, keepdims=True) * (1.0 / D)
            inv = lax.rsqrt(square - mean * mean + EPS)
            fn[g, :] = ((v - mean) * inv * g1[...]).astype(BF16)

        fn_copy(k, mine).start()

    row = lax.broadcasted_iota(jnp.int32, (SEQ, 256), 0)
    lane2 = lax.broadcasted_iota(jnp.int32, (SEQ, 128), 1)

    def conv(p, t):
        n = p.shape[1]
        p1 = jnp.where(row[:, :n] >= 1, pltpu.roll(p, 1, 0), 0.0)
        p2 = jnp.where(row[:, :n] >= 2, pltpu.roll(p, 2, 0), 0.0)
        return p2 * t[0:1, :] + p1 * t[1:2, :] + p * t[2:3, :]

    def dot_t(a, rows):
        w = jnp.concatenate(
            [jnp.concatenate([buf[b, rows, :] for b in range(16)], axis=1) for buf in (wfg, wfu)],
            axis=0,
        )
        return lax.dot_general(a, w, (((1,), (1,)), ((), ())), preferred_element_type=F32)

    def tiles(first, start, stop):
        @pl.loop(start, stop)
        def _(i):
            p = dot_t(fn[pl.ds(mul(first * SEQ, SEQ), 2 * SEQ), :], pl.ds(mul(i * 128, 128), 128))
            for h in range(2):
                q = conv(p[h * SEQ : h * SEQ + SEQ], taps[:, pl.ds(mul(i * 256, 256), 256)])
                hid[pl.ds(mul((first + h) * SEQ, SEQ), SEQ), pl.ds(mul(i * 128, 128), 128)] = (
                    jax.nn.silu(q[:, :128]) * q[:, 128:]
                ).astype(BF16)

    def last(first):
        p = dot_t(fn[pl.ds(mul(first * SEQ, SEQ), 2 * SEQ), :], pl.ds(640, 64))
        for k in range(2):
            q = conv(p[k * SEQ : k * SEQ + SEQ], taps[:, 1280:1408])
            h = jax.nn.silu(q) * pltpu.roll(q, 64, 1)
            hid[pl.ds(mul((first + k) * SEQ, SEQ), SEQ), 640:768] = jnp.where(
                lane2 < 64, h, 0.0
            ).astype(BF16)

    g_wd.step(2)
    g_in1.rest()
    tiles(c * 2, 0, 3)
    g_wd.step(6)
    for k in range(2):
        fn_copy(k, (1 - c) * 512).wait_recv()
    tiles((1 - c) * 2, 0, 3)
    g_in2.rest()
    tiles(0, 3, 5)
    last(0)
    g_wd.rest()

    hops = (2, 1, 3, 0)

    def dd_copy(k, h):
        r = pl.ds(h * 512, 512)
        return pltpu.make_async_remote_copy(
            src_ref=dsend.at[k, r, :], dst_ref=drecv.at[k, r, :],
            send_sem=dds.at[k, h], recv_sem=ddr.at[k, h], device_id=sib, device_id_type=MESH,
        )

    def down(k, i, parity):
        b = (lax.rem(x + hops[k], 4) * 2 + parity) * 2
        return dot(
            hid[pl.ds(mul(i * 256, 256), 256), :], jnp.concatenate([wd[b], wd[b + 1]], axis=1)
        )

    def down_theirs(k, h):
        @pl.loop(h * 2, h * 2 + 2)
        def _(i):
            dsend[k, pl.ds(mul(i * 256, 256), 256), :] = down(k, i, 1 - c).astype(BF16)

        dd_copy(k, h).start()

    def x_copy(slot, src, dst, step):
        return pltpu.make_async_remote_copy(
            src_ref=src, dst_ref=dst, send_sem=xss.at[slot], recv_sem=xrs.at[slot],
            device_id={"x": lax.rem(x + 4 + step, 4)}, device_id_type=MESH,
        )

    up, lo = pl.ds(0, 512), pl.ds(512, 512)
    x_copies = (
        x_copy(0, xs.at[0, up], xr2.at[up], 1),
        x_copy(1, xs.at[0, lo], xr2.at[lo], -1),
        x_copy(2, xs.at[1, lo], xr1.at[0, lo], 1),
        x_copy(3, xs.at[2, up], xr1.at[1, up], -1),
        x_copy(4, xs.at[1, up], xr1.at[0, up], 1),
        x_copy(5, xs.at[2, lo], xr1.at[1, lo], -1),
    )

    def fill(k, h, slot, extra=False):
        dd_copy(k, h).wait_recv()

        @pl.loop(h * 2, h * 2 + 2)
        def _(i):
            r = pl.ds(mul(i * 256, 256), 256)
            v = down(k, i, c) + drecv[k, r, :].astype(F32)
            if extra:
                v = v + xr2[r, :].astype(F32)
            xs[k, r, :] = v.astype(BF16)

        x_copies[slot].start()

    down_theirs(0, 0)
    down_theirs(2, 0)
    tiles(2, 3, 5)
    fill(0, 0, 0)
    fill(2, 0, 3)
    last(2)
    down_theirs(0, 1)
    down_theirs(1, 1)
    down_theirs(1, 0)
    fill(0, 1, 1)
    fill(1, 1, 2)
    down_theirs(2, 1)
    down_theirs(3, 0)
    down_theirs(3, 1)
    x_copies[0].wait_recv()
    fill(1, 0, 4, True)
    x_copies[1].wait_recv()
    fill(2, 1, 5, True)
    for h in range(2):
        dd_copy(3, h).wait_recv()

        @pl.loop(h * 2, h * 2 + 2)
        def _(i):
            r = pl.ds(mul(i * 256, 256), 256)
            acc[r, :] = (
                down(3, i, c)
                + drecv[3, r, :].astype(F32)
                + SCALE * fn[r, pl.ds(mul(j * 256, 256), 256)].astype(F32)
            )

    for g in (g_gv, g_mo, g_in1, g_in2, g_wd, r_mo, r_so, s1):
        g.sent()
    for k in range(2):
        mix_copy(k).wait_send()
        fn_copy(k, mine).wait_send()
    for k in range(4):
        for h in range(2):
            dd_copy(k, h).wait_send()
    for k in (2, 3, 4, 5):
        x_copies[k].wait_recv()

    @pl.loop(0, 8)
    def _(n):
        r = pl.ds(mul(n * 128, 128), 128)
        v = acc[r, :] + (xr1[0, r, :].astype(F32) + xr1[1, r, :].astype(F32))
        acc[r, :] = v
        a, b = v[:, :128], v[:, 128:]
        st2[0, pl.ds(n, 1), :] = jnp.sum((a + b).T, axis=0, keepdims=True)
        st2[0, pl.ds(n + 8, 1), :] = jnp.sum((a * a + b * b).T, axis=0, keepdims=True)

    s2.start()
    gain2 = g2[:, pl.ds(mul(j * 256, 256), 256)]
    for k in range(6):
        x_copies[k].wait_send()
    tot[...] = s2.total()

    @pl.loop(0, 8)
    def _(n):
        r = pl.ds(mul(n * 128, 128), 128)
        mean = spread(tot[pl.ds(n, 1), :] * (1.0 / D))
        square = spread(tot[pl.ds(n + 8, 1), :] * (1.0 / D))
        inv = lax.rsqrt(square - mean * mean + EPS)
        for h in range(2):
            cols = slice(h * 128, h * 128 + 128)
            out[r, cols] = ((acc[r, cols] - mean) * inv * gain2[:, cols]).astype(BF16)

    s2.sent()


def per_device(
    tokens, w_gate_side, w_value_side, spatial_gain, w_spatial, spatial_bias, w_mixer_out,
    first_gain, w_ff_gate, w_ff_up, conv_gate_taps, conv_up_taps, w_ff_down, second_gain,
):
    vmem = pl.BlockSpec(memory_space=pltpu.VMEM)
    hbm = pl.BlockSpec(memory_space=pl.ANY)
    V, DMA = pltpu.VMEM, pltpu.SemaphoreType.DMA
    return pl.pallas_call(
        kernel,
        out_shape=jax.ShapeDtypeStruct((ROWS, 256), BF16),
        in_specs=[hbm] * 14,
        out_specs=vmem,
        scratch_shapes=[
            V((ROWS, D), BF16),
            V((D, 128), BF16),
            V((D, 128), BF16),
            V((16, 512, 128), BF16),
            V((16, 704, 128), BF16),
            V((16, 704, 128), BF16),
            V((16, 768, 128), BF16),
            V((ROWS, 128), F32),
            V((ROWS, 128), F32),
            V((8, 16, 128), F32),
            V((8, 16, 128), F32),
            V((16, 128), F32),
            V((4, ROWS, 128), BF16),
            V((8, 1408), F32),
            V((1, 128), F32),
            V((2, 128, 128), BF16),
            V((2, 128), F32),
            V((1, D), F32),
            V((3, 704), F32),
            V((3, 704), F32),
            V((1, D), F32),
            V((512, D), BF16),
            V((512, D), BF16),
            V((512, D), F32),
            V((512, D), F32),
            V((ROWS, D), BF16),
            V((ROWS, 768), BF16),
            V((4, ROWS, 256), BF16),
            V((4, ROWS, 256), BF16),
            V((3, ROWS, 256), BF16),
            V((ROWS, 256), BF16),
            V((2, ROWS, 256), BF16),
            V((ROWS, 256), F32),
            DMA((14,)),
            DMA((5, 2, 16)),
            DMA((5, 2, 16)),
            DMA((2, 8)),
            DMA((2, 8)),
            DMA((2, 8)),
            DMA((2, 8)),
            DMA((4,)),
            DMA((4,)),
            DMA((4, 2)),
            DMA((4, 2)),
            DMA((6,)),
            DMA((6,)),
        ],
        compiler_params=pltpu.CompilerParams(
            collective_id=0, has_side_effects=True, vmem_limit_bytes=60 * 1024 * 1024
        ),
    )(
        tokens, w_gate_side, w_value_side, w_mixer_out, w_ff_gate.T, w_ff_up.T, w_ff_down,
        spatial_gain.reshape(1, 128), w_spatial, spatial_bias, first_gain.reshape(1, D),
        conv_gate_taps, conv_up_taps, second_gain.reshape(1, D),
    )


def solution(mesh):
    finer = Mesh(mesh.devices.reshape(4, 4, 4, 2), ("z", "y", "x", "c"))
    in_specs = (
        P(FS, None), P(FS, TP), P(FS, TP), P(TP), P(TP, None, None), P(TP, None), P(TP, FS), P(),
        P(FS, TP), P(FS, TP), P(None, TP), P(None, TP), P(TP, FS), P(),
    )
    return jax.shard_map(
        per_device, mesh=finer, in_specs=in_specs, out_specs=P(FS, TP), check_vma=False
    )
```

```python
import jax
import jax.numpy as jnp
from jax import lax
from jax.experimental import pallas as pl
from jax.experimental.pallas import tpu as pltpu
from jax.sharding import Mesh
from jax.sharding import PartitionSpec as P

ROWS = 1024
D = 2048
SG_WIDTH = 1024
SEQ = 256
FS = ("z", "y")
TP = ("x", "c")
SCALE = 2.0**0.25
EPS = 1e-05
F32 = jnp.float32
BF16 = jnp.bfloat16
MESH = pl.DeviceIdType.MESH


def mul(i, n):
    return pl.multiple_of(i, n)


def dot(a, b):
    return jnp.dot(a, b, preferred_element_type=F32)


ORDER = ((1, 0), (3, 0), (0, 1), (2, 0), (1, 3), (3, 3), (2, 1))
LAST = ((0, 3), (1, 1), (3, 1), (2, 3), (0, 2), (1, 2), (3, 2), (2, 2))


class PlaneGather:
    def __init__(self, block, pos, send_sem, recv_sem, flip=0, then=None, direct=False):
        self.block, self.pos, self.then, self.direct = block, pos, then, direct
        self.send_sem, self.recv_sem = send_sem, recv_sem
        self.flip = flip

    def axes(self, half):
        return ("y", "z") if half == 0 else ("z", "y")

    def ref(self, half, d):
        a1, a2 = self.axes(half)
        at = {
            a1: lax.rem(self.pos[a1] + 4 - d[0], 4),
            a2: lax.rem(self.pos[a2] + 4 - d[1], 4),
        }
        return self.block(half, at["z"] * 4 + at["y"])

    def copy(self, half, target, source, axis, step):
        ref = self.ref(half, source)
        i = target[0] * 4 + target[1]
        return pltpu.make_async_remote_copy(
            src_ref=ref,
            dst_ref=ref,
            send_sem=self.send_sem.at[half, i],
            recv_sem=self.recv_sem.at[half, i],
            device_id={axis: lax.rem(self.pos[axis] + 4 + step, 4)},
            device_id_type=MESH,
        )

    def route(self, half, target):
        a1, a2 = self.axes(half)
        d1, d2 = target
        if self.direct:
            return ((d1, 0), a2, d2) if d2 else ((0, 0), a1, d1)
        if d2 == 0:
            if d1 == 2:
                plus = (half + self.flip) % 2 == 0
                return ((1, 0), a1, 1) if plus else ((3, 0), a1, -1)
            return ((0, 0), a1, 1 if d1 == 1 else -1)
        if d2 == 2:
            return ((d1, 1), a2, 1) if d1 % 2 == 0 else ((d1, 3), a2, -1)
        return ((d1, 0), a2, 1 if d2 == 1 else -1)

    def send(self, half, target):
        source, axis, step = self.route(half, target)
        self.copy(half, target, source, axis, step).start()

    def after(self, half, source, first=True, second=True):
        for target in ((1, 0), (3, 0), (2, 0)):
            if first and self.route(half, target)[0] == source:
                self.send(half, target)
        for d1 in range(4) if second else ():
            for d2 in (1, 3, 2):
                if self.route(half, (d1, d2))[0] == source:
                    self.send(half, (d1, d2))

    def own(self, first=True, second=True):
        for half in (0, 1):
            self.after(half, (0, 0), first, second)
            if self.then and first:
                self.then(half, self.ref(half, (0, 0)))

    def arrived(self, half, d):
        i = d[0] * 4 + d[1]
        ref = self.ref(half, d)
        pltpu.make_async_remote_copy(
            src_ref=ref,
            dst_ref=ref,
            send_sem=self.send_sem.at[half, i],
            recv_sem=self.recv_sem.at[half, i],
            device_id={"y": lax.rem(self.pos["y"] + 1, 4)},
            device_id_type=MESH,
        ).wait_recv()
        if self.then:
            self.then(half, ref)

    def step(self, *which):
        for k in which:
            for half in (0, 1):
                self.arrived(half, ORDER[k])
                self.after(half, ORDER[k])

    def rest(self):
        for d in LAST + (tuple(ORDER[k] for k in (2, 4, 5, 6)) if self.direct else ()):
            for half in (0, 1):
                self.arrived(half, d)

    def sent(self):
        for half in (0, 1):
            for d1 in range(4):
                for d2 in range(4):
                    if d1 or d2:
                        source, axis, step = self.route(half, (d1, d2))
                        self.copy(half, (d1, d2), source, axis, step).wait_send()


class RingGather:
    def __init__(self, block, x, send_sem, recv_sem, chunks):
        self.block, self.x, self.chunks = block, x, chunks
        self.send_sem, self.recv_sem = send_sem, recv_sem

    def move(self, ref, slot, step):
        return pltpu.make_async_remote_copy(
            src_ref=ref,
            dst_ref=ref,
            send_sem=self.send_sem.at[slot],
            recv_sem=self.recv_sem.at[slot],
            device_id={"x": lax.rem(self.x + 4 + step, 4)},
            device_id_type=MESH,
        )

    def copy(self, back, part, slot, step):
        return self.move(self.block(lax.rem(self.x + 4 - back, 4), part), slot, step)

    def far_copy(self, back, part, chunk, step):
        b = lax.rem(self.x + 4 - back, 4)
        slot = 4 + part * self.chunks + chunk
        return self.move(self.block(b, part, chunk), slot, step)

    def sends(self):
        return ((0, 0, 0, 1), (0, 1, 1, -1), (0, 1, 2, 1), (0, 0, 3, -1))

    def own(self, part):
        for c in self.sends():
            if c[1] == part:
                self.copy(*c).start()

    def piece(self, part, ref):
        for slot, step in ((0, 1), (3, -1)) if part == 0 else ((2, 1), (1, -1)):
            self.move(ref, slot, step).start()

    def forward(self, chunk):
        if chunk == 0:
            self.copy(1, 0, 0, 1).wait_recv()
        self.far_copy(1, 0, chunk, 1).start()
        if chunk == 0:
            self.copy(3, 1, 1, 1).wait_recv()
        self.far_copy(3, 1, chunk, -1).start()

    def near(self):
        self.copy(1, 1, 2, 1).wait_recv()
        self.copy(3, 0, 3, 1).wait_recv()

    def far(self):
        for chunk in range(self.chunks):
            for part in (0, 1):
                self.far_copy(2, part, chunk, 1).wait_recv()

    def sent(self):
        for c in self.sends():
            self.copy(*c).wait_send()
        for chunk in range(self.chunks):
            self.far_copy(1, 0, chunk, 1).wait_send()
            self.far_copy(3, 1, chunk, -1).wait_send()


class Stats:
    def __init__(self, ref, x, c, send_sem, recv_sem, half=None):
        self.ref, self.x, self.c, self.half = ref, x, c, half
        self.send_sem, self.recv_sem = send_sem, recv_sem

    def at(self, k):
        return k if self.half is None else (k, self.half)

    def copies(self):
        out = []
        for k in (4, 5, 2, 6, 3, 7, 1):
            dx, dc = k // 2, k % 2
            out.append(
                pltpu.make_async_remote_copy(
                    src_ref=self.ref.at[self.at(0)],
                    dst_ref=self.ref.at[self.at(k)],
                    send_sem=self.send_sem.at[k],
                    recv_sem=self.recv_sem.at[k],
                    device_id={"x": lax.rem(self.x + dx, 4), "c": lax.rem(self.c + dc, 2)},
                    device_id_type=MESH,
                )
            )
        return out

    def start(self):
        for c in self.copies():
            c.start()

    def total(self):
        for c in self.copies():
            c.wait_recv()
        total = self.ref[self.at(0)]
        for k in range(1, 8):
            total = total + self.ref[self.at(k)]
        return total

    def sent(self):
        for c in self.copies():
            c.wait_send()


def spread(row):
    return jnp.broadcast_to(row, (128, 128)).T


def kernel(
    tok_h, gate_h, value_h, mo_h, fg_h, fu_h, wd_h, gain_h, wsp_h, bias_h, g1_h, tg_h, tu_h, g2_h,
    out,
    tok, wgt, wvl, mo, wfg, wfu, wd, ga, va, st1, st2, tot, so, taps, gain, wsp, bias, g1, taps_g, taps_u, g2,
    msend, mrecv, mown, mtheir, fn, hid, dsend, drecv, xs, xr, pend, acc,
    lsem, psend, precv, rsend, rrecv, ssend, srecv, dss, drs, dds, ddr, xss, xrs,
):
    z, y = lax.axis_index("z"), lax.axis_index("y")
    x, c = lax.axis_index("x"), lax.axis_index("c")
    pos = {"z": z, "y": y}
    f = z * 4 + y
    j = x * 2 + c
    sib = {"c": 1 - c}

    def gv_block(half, b):
        return (wgt, wvl)[half].at[pl.ds(mul(b * 128, 128), 128), :]

    def mo_block(half, b):
        return mo.at[b, pl.ds(mul(x * 128 + half * 64, 64), 64), :]

    def in1_block(half, b):
        return (wfg, wfu)[half].at[b, pl.ds(0, 384), :]

    def in2_block(half, b):
        return (wfg, wfu)[half].at[b, pl.ds(384, 320), :]

    def wd_block(half, b):
        return wd.at[b, pl.ds(half * 352, 352), :]

    def mo_ring(b, part, chunk=None):
        cut = slice(None) if chunk is None else pl.ds(chunk * 8, 8)
        return mo.at[cut, pl.ds(mul(b * 128 + part * 64, 64), 64), :]

    def so_ring(b, part, chunk=None):
        return so.at[b, pl.ds(part * 512, 512), :]

    r_mo = RingGather(mo_ring, x, rsend.at[0], rrecv.at[0], 2)
    r_so = RingGather(so_ring, x, rsend.at[1], rrecv.at[1], 1)
    g_gv = PlaneGather(gv_block, pos, psend.at[0], precv.at[0], 0)
    g_mo = PlaneGather(mo_block, pos, psend.at[1], precv.at[1], 0, r_mo.piece)
    g_in1 = PlaneGather(in1_block, pos, psend.at[2], precv.at[2], 0)
    g_in2 = PlaneGather(in2_block, pos, psend.at[3], precv.at[3], 1)
    g_wd = PlaneGather(wd_block, pos, psend.at[4], precv.at[4], 1)
    s1 = Stats(st1, x, c, ssend.at[0], srecv.at[0])
    s2 = [Stats(st2, x, c, ssend.at[1 + h], srecv.at[1 + h], h) for h in range(2)]

    rows_f = pl.ds(mul(f * 128, 128), 128)
    loads = [
        pltpu.make_async_copy(gate_h, wgt.at[rows_f, :], lsem.at[0]),
        pltpu.make_async_copy(value_h, wvl.at[rows_f, :], lsem.at[1]),
        pltpu.make_async_copy(mo_h, mo.at[f, pl.ds(mul(x * 128, 128), 128), :], lsem.at[2]),
        pltpu.make_async_copy(fg_h, wfg.at[f], lsem.at[3]),
        pltpu.make_async_copy(fu_h, wfu.at[f], lsem.at[4]),
        pltpu.make_async_copy(wd_h, wd.at[f, pl.ds(0, 704), :], lsem.at[5]),
        pltpu.make_async_copy(tok_h, tok, lsem.at[6]),
    ]
    small = [
        pltpu.make_async_copy(a, b, lsem.at[7 + k])
        for k, (a, b) in enumerate(
            zip(
                (tg_h, tu_h, gain_h, wsp_h, bias_h, g1_h, g2_h),
                (taps_g, taps_u, gain, wsp, bias, g1, g2),
            )
        )
    ]
    for l in loads + small:
        l.start()

    barrier = pltpu.get_barrier_semaphore()
    peers = [{a: lax.rem(pos[a] + s, 4)} for a in ("y", "z") for s in (1, 3)]
    peers += [
        {"x": lax.rem(x + k // 2, 4), "c": lax.rem(c + k % 2, 2)} for k in range(1, 8)
    ]
    for p in peers:
        pl.semaphore_signal(barrier, inc=1, device_id=p, device_id_type=MESH)
    for b in range(16):
        wd[b, 704:768, :] = jnp.zeros((64, 128), BF16)
    for l in small:
        l.wait()
    for i in range(5):
        t = slice(i * 128, i * 128 + 128)
        taps[0:3, i * 256 : i * 256 + 128] = taps_g[:, t]
        taps[0:3, i * 256 + 128 : i * 256 + 256] = taps_u[:, t]
    taps[0:3, 1280:1344] = taps_g[:, 640:704]
    taps[0:3, 1344:1408] = taps_u[:, 640:704]
    for k in range(3):
        loads[k].wait()
    pl.semaphore_wait(barrier, len(peers))

    g_mo.own(second=False)
    g_gv.own(second=False)
    g_mo.own(first=False)
    loads[3].wait()
    loads[4].wait()
    g_in1.own(second=False)
    g_mo.step(0)
    g_mo.step(1)
    g_gv.step(1)
    g_gv.step(0)
    g_gv.own(first=False)
    g_in2.own(second=False)
    g_mo.step(3)
    g_gv.step(3)
    loads[5].wait()
    g_wd.own(second=False)
    g_gv.step(4)
    g_mo.step(5)
    g_mo.step(4)
    g_gv.step(2)
    g_mo.step(2)
    g_mo.step(6)
    g_gv.step(5)
    g_gv.step(6)
    g_in1.own(first=False)
    g_in1.step(0)
    g_in1.step(1)
    g_in2.step(1)
    g_mo.rest()
    g_gv.rest()
    loads[6].wait()
    @pl.loop(0, 4)
    def _(i):
        r = pl.ds(mul(i * 256, 256), 256)
        pre = dot(tok[r, :], jnp.concatenate([wgt[...], wvl[...]], axis=1))
        act = jax.nn.gelu(pre)
        ga[r, :] = act[:, :128]
        va[r, :] = act[:, 128:]
        for h in range(2):
            v = act[h * 128 : h * 128 + 128, 128:].T
            st1[0, pl.ds(i * 2 + h, 1), :] = jnp.sum(v, axis=0, keepdims=True)
            st1[0, pl.ds(i * 2 + h + 8, 1), :] = jnp.sum(v * v, axis=0, keepdims=True)

    s1.start()
    g_in2.step(0)
    r_mo.forward(0)
    g_in1.step(4)
    g_wd.step(0)
    g_in1.step(5)
    g_wd.step(1)
    tot[...] = s1.total()
    lane = lax.broadcasted_iota(jnp.int32, (128, 128), 1)
    low = lax.broadcasted_iota(jnp.int32, (128, 128), 0) >= lane
    w0 = jnp.where(low, wsp[0], jnp.zeros((128, 128), BF16))
    w1 = jnp.where(low, wsp[1], jnp.zeros((128, 128), BF16))
    shift = jnp.where(lane < 64, spread(bias[0:1, :]), spread(bias[1:2, :]))

    for part in range(2):
        @pl.loop(part * 4, part * 4 + 4)
        def _(n):
            r = pl.ds(mul(n * 128, 128), 128)
            mean = spread(tot[pl.ds(n, 1), :] * (1.0 / SG_WIDTH))
            square = spread(tot[pl.ds(n + 8, 1), :] * (1.0 / SG_WIDTH))
            inv = lax.rsqrt(square - mean * mean + EPS)
            vn = ((va[r, :] - mean) * inv * gain[...]).astype(BF16)
            mixed = jnp.where(lane < 64, dot(w0, vn), dot(w1, vn)) + shift
            so[x, r, :] = (ga[r, :] * mixed).astype(BF16)

        r_so.own(part)

    g_in1.step(3)
    g_in2.step(3)
    g_in2.own(first=False)
    r_mo.forward(1)
    g_wd.own(first=False)
    r_so.forward(0)
    r_mo.near()
    r_so.near()
    g_wd.step(4)
    g_in2.step(4)
    theirs = (1 - c) * 512
    mine = c * 512

    def mix_copy(k):
        return pltpu.make_async_remote_copy(
            src_ref=msend.at[pl.ds(k * 256, 256), :],
            dst_ref=mrecv.at[pl.ds(k * 256, 256), :],
            send_sem=dss.at[k], recv_sem=drs.at[k], device_id=sib, device_id_type=MESH,
        )

    def fn_copy(k, base):
        ref = fn.at[pl.ds(mul(base + k * 256, 256), 256), :]
        return pltpu.make_async_remote_copy(
            src_ref=ref, dst_ref=ref,
            send_sem=dss.at[2 + k], recv_sem=drs.at[2 + k], device_id=sib, device_id_type=MESH,
        )

    def mix(base, i, blocks):
        r = pl.ds(mul(base, 256), 256)
        left = jnp.concatenate([so[b, r, :] for b in blocks], axis=1)
        right = jnp.concatenate(
            [
                jnp.concatenate([mo[i * 4 + q, pl.ds(mul(b * 128, 128), 128), :] for b in blocks], axis=0)
                for q in range(4)
            ],
            axis=1,
        )
        return dot(left, right)

    near = (x, lax.rem(x + 3, 4))
    far = (lax.rem(x + 1, 4), lax.rem(x + 2, 4))

    for k in range(2):
        @pl.loop(0, 4)
        def _(i):
            at = (slice(k * 256, k * 256 + 256), pl.ds(mul(i * 512, 512), 512))
            mtheir[at] = mix(theirs + k * 256, i, near)
            mown[at] = mix(mine + k * 256, i, near)

    g_in1.step(2)
    g_in1.step(6)
    g_in2.step(5)
    g_in2.step(6)
    g_wd.step(5)
    g_wd.step(3)
    r_mo.far()
    r_so.far()
    for k in range(2):
        @pl.loop(0, 4)
        def _(i):
            at = (slice(k * 256, k * 256 + 256), pl.ds(mul(i * 512, 512), 512))
            msend[at] = (mtheir[at] + mix(theirs + k * 256, i, far)).astype(BF16)

        mix_copy(k).start()
    for k in range(2):
        @pl.loop(0, 4)
        def _(i):
            at = (slice(k * 256, k * 256 + 256), pl.ds(mul(i * 512, 512), 512))
            mown[at] = mown[at] + mix(mine + k * 256, i, far)

    g_in2.step(2)
    for k in range(2):
        mix_copy(k).wait_recv()

        @pl.loop(0, 8)
        def _(i):
            r = pl.ds(mul(k * 256 + i * 32, 32), 32)
            g = pl.ds(mul(mine + k * 256 + i * 32, 32), 32)
            v = SCALE * tok[g, :].astype(F32) + (mown[r, :] + mrecv[r, :].astype(F32))
            mean = jnp.sum(v, axis=1, keepdims=True) * (1.0 / D)
            square = jnp.sum(v * v, axis=1, keepdims=True) * (1.0 / D)
            inv = lax.rsqrt(square - mean * mean + EPS)
            fn[g, :] = ((v - mean) * inv * g1[...]).astype(BF16)

        fn_copy(k, mine).start()

    row = lax.broadcasted_iota(jnp.int32, (SEQ, 256), 0)
    lane2 = lax.broadcasted_iota(jnp.int32, (SEQ, 128), 1)

    def conv(p, t):
        n = p.shape[1]
        p1 = jnp.where(row[:, :n] >= 1, pltpu.roll(p, 1, 0), 0.0)
        p2 = jnp.where(row[:, :n] >= 2, pltpu.roll(p, 2, 0), 0.0)
        return p2 * t[0:1, :] + p1 * t[1:2, :] + p * t[2:3, :]

    def dot_t(a, rows):
        w = jnp.concatenate(
            [jnp.concatenate([buf[b, rows, :] for b in range(16)], axis=1) for buf in (wfg, wfu)],
            axis=0,
        )
        return lax.dot_general(a, w, (((1,), (1,)), ((), ())), preferred_element_type=F32)

    def tiles(first, start, stop):
        @pl.loop(start, stop)
        def _(i):
            p = dot_t(fn[pl.ds(mul(first * SEQ, SEQ), 2 * SEQ), :], pl.ds(mul(i * 128, 128), 128))
            for h in range(2):
                q = conv(p[h * SEQ : h * SEQ + SEQ], taps[:, pl.ds(mul(i * 256, 256), 256)])
                hid[pl.ds(mul((first + h) * SEQ, SEQ), SEQ), pl.ds(mul(i * 128, 128), 128)] = (
                    jax.nn.silu(q[:, :128]) * q[:, 128:]
                ).astype(BF16)

    def last(first):
        p = dot_t(fn[pl.ds(mul(first * SEQ, SEQ), 2 * SEQ), :], pl.ds(640, 64))
        for k in range(2):
            q = conv(p[k * SEQ : k * SEQ + SEQ], taps[:, 1280:1408])
            h = jax.nn.silu(q) * pltpu.roll(q, 64, 1)
            hid[pl.ds(mul((first + k) * SEQ, SEQ), SEQ), 640:768] = jnp.where(
                lane2 < 64, h, 0.0
            ).astype(BF16)

    g_wd.step(2)
    g_in1.rest()
    tiles(c * 2, 0, 3)
    for k in range(2):
        fn_copy(k, (1 - c) * 512).wait_recv()
    tiles((1 - c) * 2, 0, 3)
    g_wd.step(6)
    g_in2.rest()
    tiles(0, 3, 5)
    last(0)
    g_wd.rest()

    hops = (2, 1, 3, 0)
    groups = ((0, 1), (1, 2), (3, 1))

    def seq_rows(s):
        return pl.ds(s * SEQ, SEQ)

    def dd_copy(g, s):
        ref = (pl.ds(groups[g][0], groups[g][1]), seq_rows(s), slice(None))
        return pltpu.make_async_remote_copy(
            src_ref=dsend.at[ref], dst_ref=drecv.at[ref],
            send_sem=dds.at[g, s], recv_sem=ddr.at[g, s], device_id=sib, device_id_type=MESH,
        )

    def down(g, s, parity):
        cols = []
        for k in range(groups[g][0], groups[g][0] + groups[g][1]):
            b = (lax.rem(x + hops[k], 4) * 2 + parity) * 2
            cols += [wd[b], wd[b + 1]]
        return dot(hid[seq_rows(s), :], jnp.concatenate(cols, axis=1))

    def theirs_of(g, s):
        p = down(g, s, 1 - c)
        for i in range(groups[g][1]):
            dsend[groups[g][0] + i, seq_rows(s), :] = p[:, i * 256 : i * 256 + 256].astype(BF16)
        dd_copy(g, s).start()

    def ours(g, s):
        dd_copy(g, s).wait_recv()
        p = down(g, s, c)
        return [
            p[:, i * 256 : i * 256 + 256] + drecv[groups[g][0] + i, seq_rows(s), :].astype(F32)
            for i in range(groups[g][1])
        ]

    def x_copy(i, s):
        return pltpu.make_async_remote_copy(
            src_ref=xs.at[i, seq_rows(s), :], dst_ref=xr.at[i, seq_rows(s), :],
            send_sem=xss.at[i, s], recv_sem=xrs.at[i, s],
            device_id={"x": lax.rem(x + (1 if i % 2 == 0 else 3), 4)}, device_id_type=MESH,
        )

    def put(i, s, v):
        xs[i, seq_rows(s), :] = v.astype(BF16)
        x_copy(i, s).start()

    def got(i, s):
        return xr[i, seq_rows(s), :].astype(F32)

    def far_out(s):
        v = ours(0, s)[0]
        put(0, s, v[:, :128])
        put(1, s, v[:, 128:])

    def near_out(s):
        p, m = ours(1, s)
        put(2, s, p[:, 128:])
        put(3, s, m[:, :128])
        pend[0, seq_rows(s), :] = p[:, :128]
        pend[1, seq_rows(s), :] = m[:, 128:]

    def joined_out(s):
        for i in range(2):
            x_copy(i, s).wait_recv()
            put(4 + i, s, pend[i, seq_rows(s), :] + got(i, s))

    def own_out(s):
        acc[seq_rows(s), :] = ours(2, s)[0] + SCALE * fn[
            seq_rows(s), pl.ds(mul(j * 256, 256), 256)
        ].astype(F32)

    def finish(s):
        for i in range(2, 6):
            x_copy(i, s).wait_recv()
        a = acc[seq_rows(s), :128] + (got(4, s) + got(3, s))
        b = acc[seq_rows(s), 128:] + (got(2, s) + got(5, s))
        acc[seq_rows(s), :128] = a
        acc[seq_rows(s), 128:] = b
        half, row = s // 2, s % 2 * 2
        total, square = a + b, a * a + b * b
        for i in range(2):
            r = slice(i * 128, i * 128 + 128)
            st2[0, half, row + i : row + i + 1, :] = jnp.sum(total[r].T, axis=0, keepdims=True)
            st2[0, half, row + i + 4 : row + i + 5, :] = jnp.sum(square[r].T, axis=0, keepdims=True)

    def normed(h, sums):
        for i in range(4):
            r = slice(h * 512 + i * 128, h * 512 + i * 128 + 128)
            mean = spread(sums[i : i + 1, :] * (1.0 / D))
            square = spread(sums[i + 4 : i + 5, :] * (1.0 / D))
            inv = lax.rsqrt(square - mean * mean + EPS)
            for q in range(2):
                cols = slice(q * 128, q * 128 + 128)
                out[r, cols] = ((acc[r, cols] - mean) * inv * gain2[:, cols]).astype(BF16)

    theirs_of(0, 0)
    theirs_of(1, 0)
    theirs_of(0, 1)
    theirs_of(1, 1)
    far_out(0)
    near_out(0)
    far_out(1)
    near_out(1)
    tiles(2, 3, 4)
    tiles(2, 4, 5)
    last(2)
    joined_out(0)
    theirs_of(0, 2)
    theirs_of(1, 2)
    theirs_of(0, 3)
    theirs_of(1, 3)
    joined_out(1)
    far_out(2)
    far_out(3)
    near_out(2)
    near_out(3)
    for s in range(4):
        theirs_of(2, s)
    joined_out(2)
    joined_out(3)
    for s in range(4):
        own_out(s)
    for g in (g_gv, g_mo, g_in1, g_in2, g_wd, r_mo, r_so, s1):
        g.sent()
    for k in range(2):
        mix_copy(k).wait_send()
        fn_copy(k, mine).wait_send()
    for g in range(3):
        for s in range(4):
            dd_copy(g, s).wait_send()
    gain2 = g2[:, pl.ds(mul(j * 256, 256), 256)]
    finish(0)
    finish(1)
    s2[0].start()
    finish(2)
    finish(3)
    s2[1].start()
    normed(0, s2[0].total())
    for i in range(6):
        for s in range(4):
            x_copy(i, s).wait_send()
    last_sums = s2[1].total()
    normed(1, last_sums)
    for s in s2:
        s.sent()


def per_device(
    tokens, w_gate_side, w_value_side, spatial_gain, w_spatial, spatial_bias, w_mixer_out,
    first_gain, w_ff_gate, w_ff_up, conv_gate_taps, conv_up_taps, w_ff_down, second_gain,
):
    vmem = pl.BlockSpec(memory_space=pltpu.VMEM)
    hbm = pl.BlockSpec(memory_space=pl.ANY)
    V, DMA = pltpu.VMEM, pltpu.SemaphoreType.DMA
    return pl.pallas_call(
        kernel,
        out_shape=jax.ShapeDtypeStruct((ROWS, 256), BF16),
        in_specs=[hbm] * 14,
        out_specs=vmem,
        scratch_shapes=[
            V((ROWS, D), BF16),
            V((D, 128), BF16),
            V((D, 128), BF16),
            V((16, 512, 128), BF16),
            V((16, 704, 128), BF16),
            V((16, 704, 128), BF16),
            V((16, 768, 128), BF16),
            V((ROWS, 128), F32),
            V((ROWS, 128), F32),
            V((8, 16, 128), F32),
            V((8, 2, 8, 128), F32),
            V((16, 128), F32),
            V((4, ROWS, 128), BF16),
            V((8, 1408), F32),
            V((1, 128), F32),
            V((2, 128, 128), BF16),
            V((2, 128), F32),
            V((1, D), F32),
            V((3, 704), F32),
            V((3, 704), F32),
            V((1, D), F32),
            V((512, D), BF16),
            V((512, D), BF16),
            V((512, D), F32),
            V((512, D), F32),
            V((ROWS, D), BF16),
            V((ROWS, 768), BF16),
            V((4, ROWS, 256), BF16),
            V((4, ROWS, 256), BF16),
            V((6, ROWS, 128), BF16),
            V((6, ROWS, 128), BF16),
            V((2, ROWS, 128), F32),
            V((ROWS, 256), F32),
            DMA((14,)),
            DMA((5, 2, 16)),
            DMA((5, 2, 16)),
            DMA((2, 8)),
            DMA((2, 8)),
            DMA((3, 8)),
            DMA((3, 8)),
            DMA((4,)),
            DMA((4,)),
            DMA((3, 4)),
            DMA((3, 4)),
            DMA((6, 4)),
            DMA((6, 4)),
        ],
        compiler_params=pltpu.CompilerParams(
            collective_id=0, has_side_effects=True, vmem_limit_bytes=60 * 1024 * 1024
        ),
    )(
        tokens, w_gate_side, w_value_side, w_mixer_out, w_ff_gate.T, w_ff_up.T, w_ff_down,
        spatial_gain.reshape(1, 128), w_spatial, spatial_bias, first_gain.reshape(1, D),
        conv_gate_taps, conv_up_taps, second_gain.reshape(1, D),
    )


def solution(mesh):
    finer = Mesh(mesh.devices.reshape(4, 4, 4, 2), ("z", "y", "x", "c"))
    in_specs = (
        P(FS, None), P(FS, TP), P(FS, TP), P(TP), P(TP, None, None), P(TP, None), P(TP, FS), P(),
        P(FS, TP), P(FS, TP), P(None, TP), P(None, TP), P(TP, FS), P(),
    )
    return jax.shard_map(
        per_device, mesh=finer, in_specs=in_specs, out_specs=P(FS, TP), check_vma=False
    )
```

```python
import jax
import jax.numpy as jnp
from jax import lax
from jax.experimental import pallas as pl
from jax.experimental.pallas import tpu as pltpu
from jax.sharding import Mesh
from jax.sharding import PartitionSpec as P

ROWS = 1024
D = 2048
SG_WIDTH = 1024
SEQ = 256
FS = ("z", "y")
TP = ("x", "c")
SCALE = 2.0**0.25
EPS = 1e-05
F32 = jnp.float32
BF16 = jnp.bfloat16
MESH = pl.DeviceIdType.MESH


def mul(i, n):
    return pl.multiple_of(i, n)


def dot(a, b):
    return jnp.dot(a, b, preferred_element_type=F32)


ORDER = ((1, 0), (3, 0), (0, 1), (2, 0), (1, 3), (3, 3), (2, 1))
LAST = ((0, 3), (1, 1), (3, 1), (2, 3), (0, 2), (1, 2), (3, 2), (2, 2))


class PlaneGather:
    def __init__(self, block, pos, send_sem, recv_sem, flip=0, then=None, direct=False):
        self.block, self.pos, self.then, self.direct = block, pos, then, direct
        self.send_sem, self.recv_sem = send_sem, recv_sem
        self.flip = flip

    def axes(self, half):
        return ("y", "z") if half == 0 else ("z", "y")

    def ref(self, half, d):
        a1, a2 = self.axes(half)
        at = {
            a1: lax.rem(self.pos[a1] + 4 - d[0], 4),
            a2: lax.rem(self.pos[a2] + 4 - d[1], 4),
        }
        return self.block(half, at["z"] * 4 + at["y"])

    def copy(self, half, target, source, axis, step):
        ref = self.ref(half, source)
        i = target[0] * 4 + target[1]
        return pltpu.make_async_remote_copy(
            src_ref=ref,
            dst_ref=ref,
            send_sem=self.send_sem.at[half, i],
            recv_sem=self.recv_sem.at[half, i],
            device_id={axis: lax.rem(self.pos[axis] + 4 + step, 4)},
            device_id_type=MESH,
        )

    def route(self, half, target):
        a1, a2 = self.axes(half)
        d1, d2 = target
        if self.direct:
            return ((d1, 0), a2, d2) if d2 else ((0, 0), a1, d1)
        if d2 == 0:
            if d1 == 2:
                plus = (half + self.flip) % 2 == 0
                return ((1, 0), a1, 1) if plus else ((3, 0), a1, -1)
            return ((0, 0), a1, 1 if d1 == 1 else -1)
        if d2 == 2:
            return ((d1, 1), a2, 1) if d1 % 2 == 0 else ((d1, 3), a2, -1)
        return ((d1, 0), a2, 1 if d2 == 1 else -1)

    def send(self, half, target):
        source, axis, step = self.route(half, target)
        self.copy(half, target, source, axis, step).start()

    def after(self, half, source, first=True, second=True):
        for target in ((1, 0), (3, 0), (2, 0)):
            if first and self.route(half, target)[0] == source:
                self.send(half, target)
        for d1 in range(4) if second else ():
            for d2 in (1, 3, 2):
                if self.route(half, (d1, d2))[0] == source:
                    self.send(half, (d1, d2))

    def own(self, first=True, second=True):
        for half in (0, 1):
            self.after(half, (0, 0), first, second)
            if self.then and first:
                self.then(half, self.ref(half, (0, 0)))

    def arrived(self, half, d):
        i = d[0] * 4 + d[1]
        ref = self.ref(half, d)
        pltpu.make_async_remote_copy(
            src_ref=ref,
            dst_ref=ref,
            send_sem=self.send_sem.at[half, i],
            recv_sem=self.recv_sem.at[half, i],
            device_id={"y": lax.rem(self.pos["y"] + 1, 4)},
            device_id_type=MESH,
        ).wait_recv()
        if self.then:
            self.then(half, ref)

    def step(self, *which):
        for k in which:
            for half in (0, 1):
                self.arrived(half, ORDER[k])
                self.after(half, ORDER[k])

    def rest(self):
        for d in LAST + (tuple(ORDER[k] for k in (2, 4, 5, 6)) if self.direct else ()):
            for half in (0, 1):
                self.arrived(half, d)

    def sent(self):
        for half in (0, 1):
            for d1 in range(4):
                for d2 in range(4):
                    if d1 or d2:
                        source, axis, step = self.route(half, (d1, d2))
                        self.copy(half, (d1, d2), source, axis, step).wait_send()


class RingGather:
    def __init__(self, block, x, send_sem, recv_sem, chunks):
        self.block, self.x, self.chunks = block, x, chunks
        self.send_sem, self.recv_sem = send_sem, recv_sem

    def move(self, ref, slot, step):
        return pltpu.make_async_remote_copy(
            src_ref=ref,
            dst_ref=ref,
            send_sem=self.send_sem.at[slot],
            recv_sem=self.recv_sem.at[slot],
            device_id={"x": lax.rem(self.x + 4 + step, 4)},
            device_id_type=MESH,
        )

    def copy(self, back, part, slot, step):
        return self.move(self.block(lax.rem(self.x + 4 - back, 4), part), slot, step)

    def far_copy(self, back, part, chunk, step):
        b = lax.rem(self.x + 4 - back, 4)
        slot = 4 + part * self.chunks + chunk
        return self.move(self.block(b, part, chunk), slot, step)

    def sends(self):
        return ((0, 0, 0, 1), (0, 1, 1, -1), (0, 1, 2, 1), (0, 0, 3, -1))

    def own(self, part):
        for c in self.sends():
            if c[1] == part:
                self.copy(*c).start()

    def piece(self, part, ref):
        for slot, step in ((0, 1), (3, -1)) if part == 0 else ((2, 1), (1, -1)):
            self.move(ref, slot, step).start()

    def forward(self, chunk):
        if chunk == 0:
            self.copy(1, 0, 0, 1).wait_recv()
        self.far_copy(1, 0, chunk, 1).start()
        if chunk == 0:
            self.copy(3, 1, 1, 1).wait_recv()
        self.far_copy(3, 1, chunk, -1).start()

    def near(self):
        self.copy(1, 1, 2, 1).wait_recv()
        self.copy(3, 0, 3, 1).wait_recv()

    def far(self):
        for chunk in range(self.chunks):
            for part in (0, 1):
                self.far_copy(2, part, chunk, 1).wait_recv()

    def sent(self):
        for c in self.sends():
            self.copy(*c).wait_send()
        for chunk in range(self.chunks):
            self.far_copy(1, 0, chunk, 1).wait_send()
            self.far_copy(3, 1, chunk, -1).wait_send()


class Stats:
    def __init__(self, ref, x, c, send_sem, recv_sem, half=None):
        self.ref, self.x, self.c, self.half = ref, x, c, half
        self.send_sem, self.recv_sem = send_sem, recv_sem

    def at(self, k):
        return k if self.half is None else (k, self.half)

    def copies(self):
        out = []
        for k in (4, 5, 2, 6, 3, 7, 1):
            dx, dc = k // 2, k % 2
            out.append(
                pltpu.make_async_remote_copy(
                    src_ref=self.ref.at[self.at(0)],
                    dst_ref=self.ref.at[self.at(k)],
                    send_sem=self.send_sem.at[k],
                    recv_sem=self.recv_sem.at[k],
                    device_id={"x": lax.rem(self.x + dx, 4), "c": lax.rem(self.c + dc, 2)},
                    device_id_type=MESH,
                )
            )
        return out

    def start(self):
        for c in self.copies():
            c.start()

    def total(self):
        for c in self.copies():
            c.wait_recv()
        total = self.ref[self.at(0)]
        for k in range(1, 8):
            total = total + self.ref[self.at(k)]
        return total

    def sent(self):
        for c in self.copies():
            c.wait_send()


def spread(row):
    return jnp.broadcast_to(row, (128, 128)).T


def kernel(
    tok_h, gate_h, value_h, mo_h, fg_h, fu_h, wd_h, gain_h, wsp_h, bias_h, g1_h, tg_h, tu_h, g2_h,
    out,
    tok, wgt, wvl, mo, wfg, wfu, wd, ga, va, st1, st2, tot, so, taps, gain, wsp, bias, g1, taps_g, taps_u, g2,
    msend, mrecv, mown, mtheir, fn, hid, dsend, drecv, xs, xr, pend, acc,
    lsem, psend, precv, rsend, rrecv, ssend, srecv, dss, drs, dds, ddr, xss, xrs,
):
    z, y = lax.axis_index("z"), lax.axis_index("y")
    x, c = lax.axis_index("x"), lax.axis_index("c")
    pos = {"z": z, "y": y}
    f = z * 4 + y
    j = x * 2 + c
    sib = {"c": 1 - c}

    def gv_block(half, b):
        return (wgt, wvl)[half].at[pl.ds(mul(b * 128, 128), 128), :]

    def mo_block(half, b):
        return mo.at[b, pl.ds(mul(x * 128 + half * 64, 64), 64), :]

    def in1_block(half, b):
        return (wfg, wfu)[half].at[b, pl.ds(0, 384), :]

    def in2_block(half, b):
        return (wfg, wfu)[half].at[b, pl.ds(384, 320), :]

    def wd_block(half, b):
        return wd.at[b, pl.ds(half * 352, 352), :]

    def mo_ring(b, part, chunk=None):
        cut = slice(None) if chunk is None else pl.ds(chunk * 8, 8)
        return mo.at[cut, pl.ds(mul(b * 128 + part * 64, 64), 64), :]

    def so_ring(b, part, chunk=None):
        return so.at[b, pl.ds(part * 512, 512), :]

    r_mo = RingGather(mo_ring, x, rsend.at[0], rrecv.at[0], 2)
    r_so = RingGather(so_ring, x, rsend.at[1], rrecv.at[1], 1)
    g_gv = PlaneGather(gv_block, pos, psend.at[0], precv.at[0], 0)
    g_mo = PlaneGather(mo_block, pos, psend.at[1], precv.at[1], 0, r_mo.piece)
    g_in1 = PlaneGather(in1_block, pos, psend.at[2], precv.at[2], 0)
    g_in2 = PlaneGather(in2_block, pos, psend.at[3], precv.at[3], 1)
    g_wd = PlaneGather(wd_block, pos, psend.at[4], precv.at[4], 1)
    s1 = Stats(st1, x, c, ssend.at[0], srecv.at[0])
    s2 = [Stats(st2, x, c, ssend.at[1 + h], srecv.at[1 + h], h) for h in range(2)]

    rows_f = pl.ds(mul(f * 128, 128), 128)
    loads = [
        pltpu.make_async_copy(gate_h, wgt.at[rows_f, :], lsem.at[0]),
        pltpu.make_async_copy(value_h, wvl.at[rows_f, :], lsem.at[1]),
        pltpu.make_async_copy(mo_h, mo.at[f, pl.ds(mul(x * 128, 128), 128), :], lsem.at[2]),
        pltpu.make_async_copy(fg_h, wfg.at[f, pl.ds(0, 704), :], lsem.at[3]),
        pltpu.make_async_copy(fu_h, wfu.at[f, pl.ds(0, 704), :], lsem.at[4]),
        pltpu.make_async_copy(wd_h, wd.at[f, pl.ds(0, 704), :], lsem.at[5]),
        pltpu.make_async_copy(tok_h, tok, lsem.at[6]),
    ]
    small = [
        pltpu.make_async_copy(a, b, lsem.at[7 + k])
        for k, (a, b) in enumerate(
            zip(
                (tg_h, tu_h, gain_h, wsp_h, bias_h, g1_h, g2_h),
                (taps_g, taps_u, gain, wsp, bias, g1, g2),
            )
        )
    ]
    for l in loads + small:
        l.start()

    barrier = pltpu.get_barrier_semaphore()
    peers = [{a: lax.rem(pos[a] + s, 4)} for a in ("y", "z") for s in (1, 3)]
    peers += [
        {"x": lax.rem(x + k // 2, 4), "c": lax.rem(c + k % 2, 2)} for k in range(1, 8)
    ]
    for p in peers:
        pl.semaphore_signal(barrier, inc=1, device_id=p, device_id_type=MESH)
    for buf in (wd, wfg, wfu):
        @pl.loop(0, 16)
        def _(b):
            buf[b, 704:768, :] = jnp.zeros((64, 128), BF16)

    for l in small:
        l.wait()
    for i in range(5):
        t = slice(i * 128, i * 128 + 128)
        taps[0:3, i * 256 : i * 256 + 128] = taps_g[:, t]
        taps[0:3, i * 256 + 128 : i * 256 + 256] = taps_u[:, t]
    taps[:, 1280:1536] = jnp.zeros((8, 256), F32)
    taps[0:3, 1280:1344] = taps_g[:, 640:704]
    taps[0:3, 1408:1472] = taps_u[:, 640:704]
    for k in range(3):
        loads[k].wait()
    pl.semaphore_wait(barrier, len(peers))

    g_mo.own(second=False)
    g_gv.own(second=False)
    g_mo.own(first=False)
    loads[3].wait()
    loads[4].wait()
    g_in1.own(second=False)
    g_mo.step(0)
    g_mo.step(1)
    g_gv.step(1)
    g_gv.step(0)
    g_gv.own(first=False)
    g_in2.own(second=False)
    g_mo.step(3)
    g_gv.step(3)
    loads[5].wait()
    g_wd.own(second=False)
    g_gv.step(4)
    g_mo.step(5)
    g_mo.step(4)
    g_gv.step(2)
    g_mo.step(2)
    g_mo.step(6)
    g_gv.step(5)
    g_gv.step(6)
    g_in1.own(first=False)
    g_in1.step(0)
    g_in1.step(1)
    g_in2.step(1)
    g_mo.rest()
    g_gv.rest()
    loads[6].wait()
    @pl.loop(0, 4)
    def _(i):
        r = pl.ds(mul(i * 256, 256), 256)
        pre = dot(tok[r, :], jnp.concatenate([wgt[...], wvl[...]], axis=1))
        act = jax.nn.gelu(pre)
        ga[r, :] = act[:, :128]
        va[r, :] = act[:, 128:]
        for h in range(2):
            v = act[h * 128 : h * 128 + 128, 128:].T
            st1[0, pl.ds(i * 2 + h, 1), :] = jnp.sum(v, axis=0, keepdims=True)
            st1[0, pl.ds(i * 2 + h + 8, 1), :] = jnp.sum(v * v, axis=0, keepdims=True)

    s1.start()
    g_in2.step(0)
    r_mo.forward(0)
    g_in1.step(4)
    g_wd.step(0)
    g_in1.step(5)
    g_wd.step(1)
    tot[...] = s1.total()
    lane = lax.broadcasted_iota(jnp.int32, (128, 128), 1)
    low = lax.broadcasted_iota(jnp.int32, (128, 128), 0) >= lane
    w0 = jnp.where(low, wsp[0], jnp.zeros((128, 128), BF16))
    w1 = jnp.where(low, wsp[1], jnp.zeros((128, 128), BF16))
    shift = jnp.where(lane < 64, spread(bias[0:1, :]), spread(bias[1:2, :]))

    @pl.loop(0, 8)
    def _(n):
        r = pl.ds(mul(n * 128, 128), 128)
        mean = spread(tot[pl.ds(n, 1), :] * (1.0 / SG_WIDTH))
        square = spread(tot[pl.ds(n + 8, 1), :] * (1.0 / SG_WIDTH))
        inv = lax.rsqrt(square - mean * mean + EPS)
        vn = ((va[r, :] - mean) * inv * gain[...]).astype(BF16)
        mixed = jnp.where(lane < 64, dot(w0, vn), dot(w1, vn)) + shift
        so[x, r, :] = (ga[r, :] * mixed).astype(BF16)
        for part in range(2):
            @pl.when(n == part * 4 + 3)
            def _():
                r_so.own(part)

    g_in1.step(3)
    g_in2.step(3)
    g_in2.own(first=False)
    r_mo.forward(1)
    g_wd.own(first=False)
    r_so.forward(0)
    r_mo.near()
    r_so.near()
    g_wd.step(4)
    g_in2.step(4)
    theirs = (1 - c) * 512
    mine = c * 512

    def mix_copy(k):
        return pltpu.make_async_remote_copy(
            src_ref=msend.at[pl.ds(k * 256, 256), :],
            dst_ref=mrecv.at[pl.ds(k * 256, 256), :],
            send_sem=dss.at[k], recv_sem=drs.at[k], device_id=sib, device_id_type=MESH,
        )

    def fn_copy(k, base):
        ref = fn.at[pl.ds(mul(base + k * 256, 256), 256), :]
        return pltpu.make_async_remote_copy(
            src_ref=ref, dst_ref=ref,
            send_sem=dss.at[2 + k], recv_sem=drs.at[2 + k], device_id=sib, device_id_type=MESH,
        )

    def mix(base, i, blocks):
        r = pl.ds(mul(base, 256), 256)
        left = jnp.concatenate([so[b, r, :] for b in blocks], axis=1)
        right = jnp.concatenate(
            [
                jnp.concatenate([mo[i * 4 + q, pl.ds(mul(b * 128, 128), 128), :] for b in blocks], axis=0)
                for q in range(4)
            ],
            axis=1,
        )
        return dot(left, right)

    near = (x, lax.rem(x + 3, 4))
    far = (lax.rem(x + 1, 4), lax.rem(x + 2, 4))

    def mix_at(i):
        return pl.ds(mul(i // 4 * 256, 256), 256), pl.ds(mul(i % 4 * 512, 512), 512)

    @pl.loop(0, 8)
    def _(i):
        mtheir[mix_at(i)] = mix(theirs + i // 4 * 256, i % 4, near)
        mown[mix_at(i)] = mix(mine + i // 4 * 256, i % 4, near)

    g_in1.step(2)
    g_in1.step(6)
    g_in2.step(5)
    g_in2.step(6)
    g_wd.step(5)
    g_wd.step(3)
    r_mo.far()
    r_so.far()
    @pl.loop(0, 8)
    def _(i):
        p = mix(theirs + i // 4 * 256, i % 4, far)
        msend[mix_at(i)] = (mtheir[mix_at(i)] + p).astype(BF16)
        for k in range(2):
            @pl.when(i == k * 4 + 3)
            def _():
                mix_copy(k).start()

    @pl.loop(0, 8)
    def _(i):
        mown[mix_at(i)] = mown[mix_at(i)] + mix(mine + i // 4 * 256, i % 4, far)

    g_in2.step(2)
    @pl.loop(0, 16)
    def _(i):
        for k in range(2):
            @pl.when(i == k * 8)
            def _():
                mix_copy(k).wait_recv()

        r = pl.ds(mul(i * 32, 32), 32)
        g = pl.ds(mul(mine + i * 32, 32), 32)
        v = SCALE * tok[g, :].astype(F32) + (mown[r, :] + mrecv[r, :].astype(F32))
        mean = jnp.sum(v, axis=1, keepdims=True) * (1.0 / D)
        square = jnp.sum(v * v, axis=1, keepdims=True) * (1.0 / D)
        inv = lax.rsqrt(square - mean * mean + EPS)
        fn[g, :] = ((v - mean) * inv * g1[...]).astype(BF16)
        for k in range(2):
            @pl.when(i == k * 8 + 7)
            def _():
                fn_copy(k, mine).start()

    row = lax.broadcasted_iota(jnp.int32, (SEQ, 256), 0)

    def conv(p, t):
        n = p.shape[1]
        p1 = jnp.where(row[:, :n] >= 1, pltpu.roll(p, 1, 0), 0.0)
        p2 = jnp.where(row[:, :n] >= 2, pltpu.roll(p, 2, 0), 0.0)
        return p2 * t[0:1, :] + p1 * t[1:2, :] + p * t[2:3, :]

    def dot_t(a, rows):
        w = jnp.concatenate(
            [jnp.concatenate([buf[b, rows, :] for b in range(16)], axis=1) for buf in (wfg, wfu)],
            axis=0,
        )
        return lax.dot_general(a, w, (((1,), (1,)), ((), ())), preferred_element_type=F32)

    def tile(first, i):
        p = dot_t(fn[pl.ds(mul(first * SEQ, SEQ), 2 * SEQ), :], pl.ds(mul(i * 128, 128), 128))
        for h in range(2):
            q = conv(p[h * SEQ : h * SEQ + SEQ], taps[:, pl.ds(mul(i * 256, 256), 256)])
            hid[pl.ds(mul((first + h) * SEQ, SEQ), SEQ), pl.ds(mul(i * 128, 128), 128)] = (
                jax.nn.silu(q[:, :128]) * q[:, 128:]
            ).astype(BF16)

    g_wd.step(2)
    g_in1.rest()
    @pl.loop(0, 9)
    def _(i):
        @pl.when(i == 3)
        def _():
            for k in range(2):
                fn_copy(k, (1 - c) * 512).wait_recv()

        @pl.when(i == 4)
        def _():
            g_wd.step(6)

        @pl.when(i == 6)
        def _():
            g_in2.rest()

        q = i // 3
        tile((1 - q // 2) * (2 * c * (1 - q) + (2 - 2 * c) * q), i % 3 + q // 2 * 3)

    g_wd.rest()

    hops = (2, 1, 3, 0)
    groups = ((0, 1), (1, 2), (3, 1))

    def seq_rows(s):
        return pl.ds(mul(s * SEQ, SEQ), SEQ)

    def dd_copy(g, s):
        ref = (pl.ds(groups[g][0], groups[g][1]), seq_rows(s), slice(None))
        return pltpu.make_async_remote_copy(
            src_ref=dsend.at[ref], dst_ref=drecv.at[ref],
            send_sem=dds.at[g, s], recv_sem=ddr.at[g, s], device_id=sib, device_id_type=MESH,
        )

    def down(g, s, parity):
        cols = []
        for k in range(groups[g][0], groups[g][0] + groups[g][1]):
            b = (lax.rem(x + hops[k], 4) * 2 + parity) * 2
            cols += [wd[b], wd[b + 1]]
        return dot(hid[seq_rows(s), :], jnp.concatenate(cols, axis=1))

    def theirs_of(g, s):
        p = down(g, s, 1 - c)
        for i in range(groups[g][1]):
            dsend[groups[g][0] + i, seq_rows(s), :] = p[:, i * 256 : i * 256 + 256].astype(BF16)
        dd_copy(g, s).start()

    def ours(g, s):
        dd_copy(g, s).wait_recv()
        p = down(g, s, c)
        return [
            p[:, i * 256 : i * 256 + 256] + drecv[groups[g][0] + i, seq_rows(s), :].astype(F32)
            for i in range(groups[g][1])
        ]

    def x_copy(i, s):
        return pltpu.make_async_remote_copy(
            src_ref=xs.at[i, seq_rows(s), :], dst_ref=xr.at[i, seq_rows(s), :],
            send_sem=xss.at[i, s], recv_sem=xrs.at[i, s],
            device_id={"x": lax.rem(x + (1 if i % 2 == 0 else 3), 4)}, device_id_type=MESH,
        )

    def put(i, s, v):
        xs[i, seq_rows(s), :] = v.astype(BF16)
        x_copy(i, s).start()

    def got(i, s):
        return xr[i, seq_rows(s), :].astype(F32)

    def far_out(s):
        v = ours(0, s)[0]
        put(0, s, v[:, :128])
        put(1, s, v[:, 128:])

    def near_out(s):
        p, m = ours(1, s)
        put(2, s, p[:, 128:])
        put(3, s, m[:, :128])
        pend[0, seq_rows(s), :] = p[:, :128]
        pend[1, seq_rows(s), :] = m[:, 128:]

    def joined_out(s):
        for i in range(2):
            x_copy(i, s).wait_recv()
            put(4 + i, s, pend[i, seq_rows(s), :] + got(i, s))

    def own_out(s):
        acc[seq_rows(s), :] = ours(2, s)[0] + SCALE * fn[
            seq_rows(s), pl.ds(mul(j * 256, 256), 256)
        ].astype(F32)

    def finish(s):
        for i in range(2, 6):
            x_copy(i, s).wait_recv()
        a = acc[seq_rows(s), :128] + (got(4, s) + got(3, s))
        b = acc[seq_rows(s), 128:] + (got(2, s) + got(5, s))
        acc[seq_rows(s), :128] = a
        acc[seq_rows(s), 128:] = b
        half, row = s // 2, s % 2 * 2
        total, square = a + b, a * a + b * b
        for i in range(2):
            r = slice(i * 128, i * 128 + 128)
            st2[0, half, row + i : row + i + 1, :] = jnp.sum(total[r].T, axis=0, keepdims=True)
            st2[0, half, row + i + 4 : row + i + 5, :] = jnp.sum(square[r].T, axis=0, keepdims=True)

    def normed(h, sums):
        for i in range(4):
            r = slice(h * 512 + i * 128, h * 512 + i * 128 + 128)
            mean = spread(sums[i : i + 1, :] * (1.0 / D))
            square = spread(sums[i + 4 : i + 5, :] * (1.0 / D))
            inv = lax.rsqrt(square - mean * mean + EPS)
            for q in range(2):
                cols = slice(q * 128, q * 128 + 128)
                out[r, cols] = ((acc[r, cols] - mean) * inv * gain2[:, cols]).astype(BF16)

    @pl.loop(0, 2)
    def _(s):
        theirs_of(0, s)
        theirs_of(1, s)

    @pl.loop(0, 2)
    def _(s):
        far_out(s)
        near_out(s)

    @pl.loop(3, 6)
    def _(i):
        tile(2, i)

    joined_out(0)
    @pl.loop(2, 4)
    def _(s):
        theirs_of(0, s)
        theirs_of(1, s)

    joined_out(1)
    @pl.loop(2, 4)
    def _(s):
        far_out(s)

    @pl.loop(2, 4)
    def _(s):
        near_out(s)

    @pl.loop(0, 4)
    def _(s):
        theirs_of(2, s)

    joined_out(2)
    joined_out(3)
    @pl.loop(0, 4)
    def _(s):
        own_out(s)

    for g in (g_gv, g_mo, g_in1, g_in2, g_wd, r_mo, r_so, s1):
        g.sent()
    for k in range(2):
        mix_copy(k).wait_send()
        fn_copy(k, mine).wait_send()
    for g in range(3):
        for s in range(4):
            dd_copy(g, s).wait_send()
    gain2 = g2[:, pl.ds(mul(j * 256, 256), 256)]
    finish(0)
    finish(1)
    s2[0].start()
    finish(2)
    finish(3)
    s2[1].start()
    normed(0, s2[0].total())
    for i in range(6):
        for s in range(4):
            x_copy(i, s).wait_send()
    last_sums = s2[1].total()
    normed(1, last_sums)
    for s in s2:
        s.sent()


def per_device(
    tokens, w_gate_side, w_value_side, spatial_gain, w_spatial, spatial_bias, w_mixer_out,
    first_gain, w_ff_gate, w_ff_up, conv_gate_taps, conv_up_taps, w_ff_down, second_gain,
):
    vmem = pl.BlockSpec(memory_space=pltpu.VMEM)
    hbm = pl.BlockSpec(memory_space=pl.ANY)
    V, DMA = pltpu.VMEM, pltpu.SemaphoreType.DMA
    return pl.pallas_call(
        kernel,
        out_shape=jax.ShapeDtypeStruct((ROWS, 256), BF16),
        in_specs=[hbm] * 14,
        out_specs=vmem,
        scratch_shapes=[
            V((ROWS, D), BF16),
            V((D, 128), BF16),
            V((D, 128), BF16),
            V((16, 512, 128), BF16),
            V((16, 768, 128), BF16),
            V((16, 768, 128), BF16),
            V((16, 768, 128), BF16),
            V((ROWS, 128), F32),
            V((ROWS, 128), F32),
            V((8, 16, 128), F32),
            V((8, 2, 8, 128), F32),
            V((16, 128), F32),
            V((4, ROWS, 128), BF16),
            V((8, 1536), F32),
            V((1, 128), F32),
            V((2, 128, 128), BF16),
            V((2, 128), F32),
            V((1, D), F32),
            V((3, 704), F32),
            V((3, 704), F32),
            V((1, D), F32),
            V((512, D), BF16),
            V((512, D), BF16),
            V((512, D), F32),
            V((512, D), F32),
            V((ROWS, D), BF16),
            V((ROWS, 768), BF16),
            V((4, ROWS, 256), BF16),
            V((4, ROWS, 256), BF16),
            V((6, ROWS, 128), BF16),
            V((6, ROWS, 128), BF16),
            V((2, ROWS, 128), F32),
            V((ROWS, 256), F32),
            DMA((14,)),
            DMA((5, 2, 16)),
            DMA((5, 2, 16)),
            DMA((2, 8)),
            DMA((2, 8)),
            DMA((3, 8)),
            DMA((3, 8)),
            DMA((4,)),
            DMA((4,)),
            DMA((3, 4)),
            DMA((3, 4)),
            DMA((6, 4)),
            DMA((6, 4)),
        ],
        compiler_params=pltpu.CompilerParams(
            collective_id=0, has_side_effects=True, vmem_limit_bytes=60 * 1024 * 1024
        ),
    )(
        tokens, w_gate_side, w_value_side, w_mixer_out, w_ff_gate.T, w_ff_up.T, w_ff_down,
        spatial_gain.reshape(1, 128), w_spatial, spatial_bias, first_gain.reshape(1, D),
        conv_gate_taps, conv_up_taps, second_gain.reshape(1, D),
    )


def solution(mesh):
    finer = Mesh(mesh.devices.reshape(4, 4, 4, 2), ("z", "y", "x", "c"))
    in_specs = (
        P(FS, None), P(FS, TP), P(FS, TP), P(TP), P(TP, None, None), P(TP, None), P(TP, FS), P(),
        P(FS, TP), P(FS, TP), P(None, TP), P(None, TP), P(TP, FS), P(),
    )
    return jax.shard_map(
        per_device, mesh=finer, in_specs=in_specs, out_specs=P(FS, TP), check_vma=False
    )
```

```python
import jax
import jax.numpy as jnp
from jax import lax
from jax.experimental import pallas as pl
from jax.experimental.pallas import tpu as pltpu
from jax.sharding import Mesh
from jax.sharding import PartitionSpec as P

ROWS = 1024
D = 2048
SG_WIDTH = 1024
SEQ = 256
FS = ("z", "y")
TP = ("x", "c")
SCALE = 2.0**0.25
EPS = 1e-05
F32 = jnp.float32
BF16 = jnp.bfloat16
MESH = pl.DeviceIdType.MESH


def mul(i, n):
    return pl.multiple_of(i, n)


def dot(a, b):
    return jnp.dot(a, b, preferred_element_type=F32)


ORDER = ((1, 0), (3, 0), (0, 1), (2, 0), (1, 3), (3, 3), (2, 1))
LAST = ((0, 3), (1, 1), (3, 1), (2, 3), (0, 2), (1, 2), (3, 2), (2, 2))


class PlaneGather:
    def __init__(self, block, pos, send_sem, recv_sem, flip=0, then=None, direct=False):
        self.block, self.pos, self.then, self.direct = block, pos, then, direct
        self.send_sem, self.recv_sem = send_sem, recv_sem
        self.flip = flip

    def axes(self, half):
        return ("y", "z") if half == 0 else ("z", "y")

    def ref(self, half, d):
        a1, a2 = self.axes(half)
        at = {
            a1: lax.rem(self.pos[a1] + 4 - d[0], 4),
            a2: lax.rem(self.pos[a2] + 4 - d[1], 4),
        }
        return self.block(half, at["z"] * 4 + at["y"])

    def copy(self, half, target, source, axis, step):
        ref = self.ref(half, source)
        i = target[0] * 4 + target[1]
        return pltpu.make_async_remote_copy(
            src_ref=ref,
            dst_ref=ref,
            send_sem=self.send_sem.at[half, i],
            recv_sem=self.recv_sem.at[half, i],
            device_id={axis: lax.rem(self.pos[axis] + 4 + step, 4)},
            device_id_type=MESH,
        )

    def route(self, half, target):
        a1, a2 = self.axes(half)
        d1, d2 = target
        if self.direct:
            return ((d1, 0), a2, d2) if d2 else ((0, 0), a1, d1)
        if d2 == 0:
            if d1 == 2:
                plus = (half + self.flip) % 2 == 0
                return ((1, 0), a1, 1) if plus else ((3, 0), a1, -1)
            return ((0, 0), a1, 1 if d1 == 1 else -1)
        if d2 == 2:
            return ((d1, 1), a2, 1) if d1 % 2 == 0 else ((d1, 3), a2, -1)
        return ((d1, 0), a2, 1 if d2 == 1 else -1)

    def send(self, half, target):
        source, axis, step = self.route(half, target)
        self.copy(half, target, source, axis, step).start()

    def after(self, half, source, first=True, second=True):
        for target in ((1, 0), (3, 0), (2, 0)):
            if first and self.route(half, target)[0] == source:
                self.send(half, target)
        for d1 in range(4) if second else ():
            for d2 in (1, 3, 2):
                if self.route(half, (d1, d2))[0] == source:
                    self.send(half, (d1, d2))

    def own(self, first=True, second=True):
        for half in (0, 1):
            self.after(half, (0, 0), first, second)
            if self.then and first:
                self.then(half, self.ref(half, (0, 0)))

    def arrived(self, half, d):
        i = d[0] * 4 + d[1]
        ref = self.ref(half, d)
        pltpu.make_async_remote_copy(
            src_ref=ref,
            dst_ref=ref,
            send_sem=self.send_sem.at[half, i],
            recv_sem=self.recv_sem.at[half, i],
            device_id={"y": lax.rem(self.pos["y"] + 1, 4)},
            device_id_type=MESH,
        ).wait_recv()
        if self.then:
            self.then(half, ref)

    def step(self, *which):
        for k in which:
            for half in (0, 1):
                self.arrived(half, ORDER[k])
                self.after(half, ORDER[k])

    def rest(self):
        for d in LAST + (tuple(ORDER[k] for k in (2, 4, 5, 6)) if self.direct else ()):
            for half in (0, 1):
                self.arrived(half, d)

    def sent(self):
        for half in (0, 1):
            for d1 in range(4):
                for d2 in range(4):
                    if d1 or d2:
                        source, axis, step = self.route(half, (d1, d2))
                        self.copy(half, (d1, d2), source, axis, step).wait_send()


class RingGather:
    def __init__(self, block, x, send_sem, recv_sem, chunks):
        self.block, self.x, self.chunks = block, x, chunks
        self.send_sem, self.recv_sem = send_sem, recv_sem

    def move(self, ref, slot, step):
        return pltpu.make_async_remote_copy(
            src_ref=ref,
            dst_ref=ref,
            send_sem=self.send_sem.at[slot],
            recv_sem=self.recv_sem.at[slot],
            device_id={"x": lax.rem(self.x + 4 + step, 4)},
            device_id_type=MESH,
        )

    def copy(self, back, part, slot, step):
        return self.move(self.block(lax.rem(self.x + 4 - back, 4), part), slot, step)

    def far_copy(self, back, part, chunk, step):
        b = lax.rem(self.x + 4 - back, 4)
        slot = 4 + part * self.chunks + chunk
        return self.move(self.block(b, part, chunk), slot, step)

    def sends(self):
        return ((0, 0, 0, 1), (0, 1, 1, -1), (0, 1, 2, 1), (0, 0, 3, -1))

    def own(self, part):
        for c in self.sends():
            if c[1] == part:
                self.copy(*c).start()

    def piece(self, part, ref):
        for slot, step in ((0, 1), (3, -1)) if part == 0 else ((2, 1), (1, -1)):
            self.move(ref, slot, step).start()

    def forward(self, chunk):
        if chunk == 0:
            self.copy(1, 0, 0, 1).wait_recv()
        self.far_copy(1, 0, chunk, 1).start()
        if chunk == 0:
            self.copy(3, 1, 1, 1).wait_recv()
        self.far_copy(3, 1, chunk, -1).start()

    def near(self):
        self.copy(1, 1, 2, 1).wait_recv()
        self.copy(3, 0, 3, 1).wait_recv()

    def far(self):
        for chunk in range(self.chunks):
            for part in (0, 1):
                self.far_copy(2, part, chunk, 1).wait_recv()

    def sent(self):
        for c in self.sends():
            self.copy(*c).wait_send()
        for chunk in range(self.chunks):
            self.far_copy(1, 0, chunk, 1).wait_send()
            self.far_copy(3, 1, chunk, -1).wait_send()


class Stats:
    def __init__(self, ref, x, c, send_sem, recv_sem, half=None):
        self.ref, self.x, self.c, self.half = ref, x, c, half
        self.send_sem, self.recv_sem = send_sem, recv_sem

    def at(self, k):
        return k if self.half is None else (k, self.half)

    def copies(self):
        out = []
        for k in (4, 5, 2, 6, 3, 7, 1):
            dx, dc = k // 2, k % 2
            out.append(
                pltpu.make_async_remote_copy(
                    src_ref=self.ref.at[self.at(0)],
                    dst_ref=self.ref.at[self.at(k)],
                    send_sem=self.send_sem.at[k],
                    recv_sem=self.recv_sem.at[k],
                    device_id={"x": lax.rem(self.x + dx, 4), "c": lax.rem(self.c + dc, 2)},
                    device_id_type=MESH,
                )
            )
        return out

    def start(self):
        for c in self.copies():
            c.start()

    def total(self):
        for c in self.copies():
            c.wait_recv()
        total = self.ref[self.at(0)]
        for k in range(1, 8):
            total = total + self.ref[self.at(k)]
        return total

    def sent(self):
        for c in self.copies():
            c.wait_send()


def spread(row):
    return jnp.broadcast_to(row, (128, 128)).T


def kernel(
    tok_h, gate_h, value_h, mo_h, fg_h, fu_h, wd_h, gain_h, wsp_h, bias_h, g1_h, tg_h, tu_h, g2_h,
    out,
    tok, wgt, wvl, mo, wfg, wfu, wd, ga, va, st1, st2, tot, so, taps, gain, wsp, bias, g1, taps_g, taps_u, g2,
    msend, mrecv, mown, mtheir, fn, hid, dsend, drecv, xs, xr, pend, acc,
    lsem, psend, precv, rsend, rrecv, ssend, srecv, dss, drs, dds, ddr, xss, xrs,
):
    z, y = lax.axis_index("z"), lax.axis_index("y")
    x, c = lax.axis_index("x"), lax.axis_index("c")
    pos = {"z": z, "y": y}
    f = z * 4 + y
    j = x * 2 + c
    sib = {"c": 1 - c}

    def gv_block(half, b):
        return (wgt, wvl)[half].at[pl.ds(mul(b * 128, 128), 128), :]

    def mo_block(half, b):
        return mo.at[b, pl.ds(mul(x * 128 + half * 64, 64), 64), :]

    def in1_block(half, b):
        return (wfg, wfu)[half].at[b, pl.ds(0, 384), :]

    def in2_block(half, b):
        return (wfg, wfu)[half].at[b, pl.ds(384, 320), :]

    def wd_block(half, b):
        return wd.at[b, pl.ds(half * 352, 352), :]

    def mo_ring(b, part, chunk=None):
        cut = slice(None) if chunk is None else pl.ds(chunk * 8, 8)
        return mo.at[cut, pl.ds(mul(b * 128 + part * 64, 64), 64), :]

    def so_ring(b, part, chunk=None):
        return so.at[b, pl.ds(part * 512, 512), :]

    r_mo = RingGather(mo_ring, x, rsend.at[0], rrecv.at[0], 2)
    r_so = RingGather(so_ring, x, rsend.at[1], rrecv.at[1], 1)
    g_gv = PlaneGather(gv_block, pos, psend.at[0], precv.at[0], 0)
    g_mo = PlaneGather(mo_block, pos, psend.at[1], precv.at[1], 0, r_mo.piece)
    g_in1 = PlaneGather(in1_block, pos, psend.at[2], precv.at[2], 0)
    g_in2 = PlaneGather(in2_block, pos, psend.at[3], precv.at[3], 1)
    g_wd = PlaneGather(wd_block, pos, psend.at[4], precv.at[4], 1)
    s1 = Stats(st1, x, c, ssend.at[0], srecv.at[0])
    s2 = [Stats(st2, x, c, ssend.at[1 + h], srecv.at[1 + h], h) for h in range(2)]

    rows_f = pl.ds(mul(f * 128, 128), 128)
    loads = [
        pltpu.make_async_copy(gate_h, wgt.at[rows_f, :], lsem.at[0]),
        pltpu.make_async_copy(value_h, wvl.at[rows_f, :], lsem.at[1]),
        pltpu.make_async_copy(mo_h, mo.at[f, pl.ds(mul(x * 128, 128), 128), :], lsem.at[2]),
        pltpu.make_async_copy(fg_h, wfg.at[f, pl.ds(0, 704), :], lsem.at[3]),
        pltpu.make_async_copy(fu_h, wfu.at[f, pl.ds(0, 704), :], lsem.at[4]),
        pltpu.make_async_copy(wd_h, wd.at[f, pl.ds(0, 704), :], lsem.at[5]),
        pltpu.make_async_copy(tok_h, tok, lsem.at[6]),
    ]
    small = [
        pltpu.make_async_copy(a, b, lsem.at[7 + k])
        for k, (a, b) in enumerate(
            zip(
                (tg_h, tu_h, gain_h, wsp_h, bias_h, g1_h, g2_h),
                (taps_g, taps_u, gain, wsp, bias, g1, g2),
            )
        )
    ]
    for l in loads + small:
        l.start()

    barrier = pltpu.get_barrier_semaphore()
    peers = [{a: lax.rem(pos[a] + s, 4)} for a in ("y", "z") for s in (1, 3)]
    peers += [
        {"x": lax.rem(x + k // 2, 4), "c": lax.rem(c + k % 2, 2)} for k in range(1, 8)
    ]
    for p in peers:
        pl.semaphore_signal(barrier, inc=1, device_id=p, device_id_type=MESH)
    for buf in (wd, wfg, wfu):
        @pl.loop(0, 16)
        def _(b):
            buf[b, 704:768, :] = jnp.zeros((64, 128), BF16)

    for l in small:
        l.wait()
    for i in range(5):
        t = slice(i * 128, i * 128 + 128)
        taps[0:3, i * 256 : i * 256 + 128] = taps_g[:, t]
        taps[0:3, i * 256 + 128 : i * 256 + 256] = taps_u[:, t]
    taps[:, 1280:1536] = jnp.zeros((8, 256), F32)
    taps[0:3, 1280:1344] = taps_g[:, 640:704]
    taps[0:3, 1408:1472] = taps_u[:, 640:704]
    for k in range(3):
        loads[k].wait()
    pl.semaphore_wait(barrier, len(peers))

    g_mo.own(second=False)
    g_gv.own(second=False)
    g_mo.own(first=False)
    loads[3].wait()
    loads[4].wait()
    g_in1.own(second=False)
    g_mo.step(0)
    g_mo.step(1)
    g_gv.step(1)
    g_gv.step(0)
    g_gv.own(first=False)
    g_in2.own(second=False)
    g_mo.step(3)
    g_gv.step(3)
    loads[5].wait()
    g_wd.own(second=False)
    g_gv.step(4)
    g_mo.step(5)
    g_mo.step(4)
    g_gv.step(2)
    g_mo.step(2)
    g_mo.step(6)
    g_gv.step(5)
    g_gv.step(6)
    g_in1.own(first=False)
    g_in1.step(0)
    g_in1.step(1)
    g_in2.step(1)
    g_mo.rest()
    g_gv.rest()
    loads[6].wait()
    @pl.loop(0, 4)
    def _(i):
        r = pl.ds(mul(i * 256, 256), 256)
        pre = dot(tok[r, :], jnp.concatenate([wgt[...], wvl[...]], axis=1))
        act = jax.nn.gelu(pre)
        ga[r, :] = act[:, :128]
        va[r, :] = act[:, 128:]
        for h in range(2):
            v = act[h * 128 : h * 128 + 128, 128:].T
            st1[0, pl.ds(i * 2 + h, 1), :] = jnp.sum(v, axis=0, keepdims=True)
            st1[0, pl.ds(i * 2 + h + 8, 1), :] = jnp.sum(v * v, axis=0, keepdims=True)

    s1.start()
    g_in2.step(0)
    r_mo.forward(0)
    g_in1.step(4)
    g_wd.step(0)
    g_in1.step(5)
    g_wd.step(1)
    tot[...] = s1.total()
    lane = lax.broadcasted_iota(jnp.int32, (128, 128), 1)
    low = lax.broadcasted_iota(jnp.int32, (128, 128), 0) >= lane
    w0 = jnp.where(low, wsp[0], jnp.zeros((128, 128), BF16))
    w1 = jnp.where(low, wsp[1], jnp.zeros((128, 128), BF16))
    shift = jnp.where(lane < 64, spread(bias[0:1, :]), spread(bias[1:2, :]))

    @pl.loop(0, 8)
    def _(n):
        r = pl.ds(mul(n * 128, 128), 128)
        mean = spread(tot[pl.ds(n, 1), :] * (1.0 / SG_WIDTH))
        square = spread(tot[pl.ds(n + 8, 1), :] * (1.0 / SG_WIDTH))
        inv = lax.rsqrt(square - mean * mean + EPS)
        vn = ((va[r, :] - mean) * inv * gain[...]).astype(BF16)
        mixed = jnp.where(lane < 64, dot(w0, vn), dot(w1, vn)) + shift
        so[x, r, :] = (ga[r, :] * mixed).astype(BF16)
        for part in range(2):
            @pl.when(n == part * 4 + 3)
            def _():
                r_so.own(part)

    g_in1.step(3)
    g_in2.step(3)
    g_in2.own(first=False)
    r_mo.forward(1)
    g_wd.own(first=False)
    r_so.forward(0)
    r_mo.near()
    r_so.near()
    g_wd.step(4)
    g_in2.step(4)
    theirs = (1 - c) * 512
    mine = c * 512

    def mix_copy(k):
        return pltpu.make_async_remote_copy(
            src_ref=msend.at[pl.ds(k * 256, 256), :],
            dst_ref=mrecv.at[pl.ds(k * 256, 256), :],
            send_sem=dss.at[k], recv_sem=drs.at[k], device_id=sib, device_id_type=MESH,
        )

    def fn_copy(k, base):
        ref = fn.at[pl.ds(mul(base + k * 256, 256), 256), :]
        return pltpu.make_async_remote_copy(
            src_ref=ref, dst_ref=ref,
            send_sem=dss.at[2 + k], recv_sem=drs.at[2 + k], device_id=sib, device_id_type=MESH,
        )

    def mix(base, i, blocks):
        r = pl.ds(mul(base, 256), 256)
        left = jnp.concatenate([so[b, r, :] for b in blocks], axis=1)
        right = jnp.concatenate(
            [
                jnp.concatenate([mo[i * 4 + q, pl.ds(mul(b * 128, 128), 128), :] for b in blocks], axis=0)
                for q in range(4)
            ],
            axis=1,
        )
        return dot(left, right)

    near = (x, lax.rem(x + 3, 4))
    far = (lax.rem(x + 1, 4), lax.rem(x + 2, 4))

    def mix_at(i):
        return pl.ds(mul(i // 4 * 256, 256), 256), pl.ds(mul(i % 4 * 512, 512), 512)

    @pl.loop(0, 8)
    def _(i):
        mtheir[mix_at(i)] = mix(theirs + i // 4 * 256, i % 4, near)
        mown[mix_at(i)] = mix(mine + i // 4 * 256, i % 4, near)

    g_in1.step(2)
    g_in1.step(6)
    g_in2.step(5)
    g_in2.step(6)
    g_wd.step(5)
    g_wd.step(3)
    r_mo.far()
    r_so.far()
    @pl.loop(0, 8)
    def _(i):
        p = mix(theirs + i // 4 * 256, i % 4, far)
        msend[mix_at(i)] = (mtheir[mix_at(i)] + p).astype(BF16)
        for k in range(2):
            @pl.when(i == k * 4 + 3)
            def _():
                mix_copy(k).start()

    @pl.loop(0, 8)
    def _(i):
        mown[mix_at(i)] = mown[mix_at(i)] + mix(mine + i // 4 * 256, i % 4, far)

    g_in2.step(2)
    @pl.loop(0, 8)
    def _(i):
        for k in range(2):
            @pl.when(i == k * 4)
            def _():
                mix_copy(k).wait_recv()

        r = pl.ds(mul(i * 64, 64), 64)
        g = pl.ds(mul(mine + i * 64, 64), 64)
        v = SCALE * tok[g, :].astype(F32) + (mown[r, :] + mrecv[r, :].astype(F32))
        mean = jnp.sum(v, axis=1, keepdims=True) * (1.0 / D)
        square = jnp.sum(v * v, axis=1, keepdims=True) * (1.0 / D)
        inv = lax.rsqrt(square - mean * mean + EPS)
        fn[g, :] = ((v - mean) * inv * g1[...]).astype(BF16)
        for k in range(2):
            @pl.when(i == k * 4 + 3)
            def _():
                fn_copy(k, mine).start()

    row = lax.broadcasted_iota(jnp.int32, (SEQ, 256), 0)

    def conv(p, t):
        n = p.shape[1]
        p1 = jnp.where(row[:, :n] >= 1, pltpu.roll(p, 1, 0), 0.0)
        p2 = jnp.where(row[:, :n] >= 2, pltpu.roll(p, 2, 0), 0.0)
        return p2 * t[0:1, :] + p1 * t[1:2, :] + p * t[2:3, :]

    def dot_t(a, rows):
        w = jnp.concatenate(
            [jnp.concatenate([buf[b, rows, :] for b in range(16)], axis=1) for buf in (wfg, wfu)],
            axis=0,
        )
        return lax.dot_general(a, w, (((1,), (1,)), ((), ())), preferred_element_type=F32)

    def tile(first, i):
        p = dot_t(fn[pl.ds(mul(first * SEQ, SEQ), 2 * SEQ), :], pl.ds(mul(i * 128, 128), 128))
        for h in range(2):
            q = conv(p[h * SEQ : h * SEQ + SEQ], taps[:, pl.ds(mul(i * 256, 256), 256)])
            hid[pl.ds(mul((first + h) * SEQ, SEQ), SEQ), pl.ds(mul(i * 128, 128), 128)] = (
                jax.nn.silu(q[:, :128]) * q[:, 128:]
            ).astype(BF16)

    g_wd.step(2)
    g_in1.rest()
    @pl.loop(0, 9)
    def _(i):
        @pl.when(i == 3)
        def _():
            for k in range(2):
                fn_copy(k, (1 - c) * 512).wait_recv()

        @pl.when(i == 4)
        def _():
            g_wd.step(6)

        @pl.when(i == 6)
        def _():
            g_in2.rest()

        q = i // 3
        tile((1 - q // 2) * (2 * c * (1 - q) + (2 - 2 * c) * q), i % 3 + q // 2 * 3)

    g_wd.rest()

    hops = (2, 1, 3, 0)
    groups = ((0, 1), (1, 2), (3, 1))

    def seq_rows(s):
        return pl.ds(mul(s * SEQ, SEQ), SEQ)

    def dd_copy(g, s):
        ref = (pl.ds(groups[g][0], groups[g][1]), seq_rows(s), slice(None))
        return pltpu.make_async_remote_copy(
            src_ref=dsend.at[ref], dst_ref=drecv.at[ref],
            send_sem=dds.at[g, s], recv_sem=ddr.at[g, s], device_id=sib, device_id_type=MESH,
        )

    def down(g, s, parity):
        cols = []
        for k in range(groups[g][0], groups[g][0] + groups[g][1]):
            b = (lax.rem(x + hops[k], 4) * 2 + parity) * 2
            cols += [wd[b], wd[b + 1]]
        return dot(hid[seq_rows(s), :], jnp.concatenate(cols, axis=1))

    def theirs_of(g, s):
        p = down(g, s, 1 - c)
        for i in range(groups[g][1]):
            dsend[groups[g][0] + i, seq_rows(s), :] = p[:, i * 256 : i * 256 + 256].astype(BF16)
        dd_copy(g, s).start()

    def ours(g, s):
        dd_copy(g, s).wait_recv()
        p = down(g, s, c)
        return [
            p[:, i * 256 : i * 256 + 256] + drecv[groups[g][0] + i, seq_rows(s), :].astype(F32)
            for i in range(groups[g][1])
        ]

    def x_copy(i, s):
        return pltpu.make_async_remote_copy(
            src_ref=xs.at[i, seq_rows(s), :], dst_ref=xr.at[i, seq_rows(s), :],
            send_sem=xss.at[i, s], recv_sem=xrs.at[i, s],
            device_id={"x": lax.rem(x + (1 if i % 2 == 0 else 3), 4)}, device_id_type=MESH,
        )

    def put(i, s, v):
        xs[i, seq_rows(s), :] = v.astype(BF16)
        x_copy(i, s).start()

    def got(i, s):
        return xr[i, seq_rows(s), :].astype(F32)

    def far_out(s):
        v = ours(0, s)[0]
        put(0, s, v[:, :128])
        put(1, s, v[:, 128:])

    def near_out(s):
        p, m = ours(1, s)
        put(2, s, p[:, 128:])
        put(3, s, m[:, :128])
        pend[0, seq_rows(s), :] = p[:, :128]
        pend[1, seq_rows(s), :] = m[:, 128:]

    def joined_out(s):
        for i in range(2):
            x_copy(i, s).wait_recv()
            put(4 + i, s, pend[i, seq_rows(s), :] + got(i, s))

    def own_out(s):
        acc[seq_rows(s), :] = ours(2, s)[0] + SCALE * fn[
            seq_rows(s), pl.ds(mul(j * 256, 256), 256)
        ].astype(F32)

    def finish(s):
        for i in range(2, 6):
            x_copy(i, s).wait_recv()
        a = acc[seq_rows(s), :128] + (got(4, s) + got(3, s))
        b = acc[seq_rows(s), 128:] + (got(2, s) + got(5, s))
        acc[seq_rows(s), :128] = a
        acc[seq_rows(s), 128:] = b
        half, row = s // 2, s % 2 * 2
        total, square = a + b, a * a + b * b
        for i in range(2):
            r = slice(i * 128, i * 128 + 128)
            st2[0, half, row + i : row + i + 1, :] = jnp.sum(total[r].T, axis=0, keepdims=True)
            st2[0, half, row + i + 4 : row + i + 5, :] = jnp.sum(square[r].T, axis=0, keepdims=True)

    def normed(h, sums):
        for i in range(4):
            r = slice(h * 512 + i * 128, h * 512 + i * 128 + 128)
            mean = spread(sums[i : i + 1, :] * (1.0 / D))
            square = spread(sums[i + 4 : i + 5, :] * (1.0 / D))
            inv = lax.rsqrt(square - mean * mean + EPS)
            for q in range(2):
                cols = slice(q * 128, q * 128 + 128)
                out[r, cols] = ((acc[r, cols] - mean) * inv * gain2[:, cols]).astype(BF16)

    @pl.loop(0, 2)
    def _(s):
        theirs_of(0, s)
        theirs_of(1, s)

    @pl.loop(0, 2)
    def _(s):
        far_out(s)
        near_out(s)

    @pl.loop(3, 6)
    def _(i):
        tile(2, i)

    joined_out(0)
    @pl.loop(2, 4)
    def _(s):
        theirs_of(0, s)
        theirs_of(1, s)

    joined_out(1)
    @pl.loop(2, 4)
    def _(s):
        far_out(s)

    @pl.loop(2, 4)
    def _(s):
        near_out(s)

    @pl.loop(0, 4)
    def _(s):
        theirs_of(2, s)

    joined_out(2)
    joined_out(3)
    @pl.loop(0, 4)
    def _(s):
        own_out(s)

    for g in (g_gv, g_mo, g_in1, g_in2, g_wd, r_mo, r_so, s1):
        g.sent()
    for k in range(2):
        mix_copy(k).wait_send()
        fn_copy(k, mine).wait_send()
    for g in range(3):
        for s in range(4):
            dd_copy(g, s).wait_send()
    gain2 = g2[:, pl.ds(mul(j * 256, 256), 256)]
    finish(0)
    finish(1)
    s2[0].start()
    finish(2)
    finish(3)
    s2[1].start()
    normed(0, s2[0].total())
    for i in range(6):
        for s in range(4):
            x_copy(i, s).wait_send()
    last_sums = s2[1].total()
    normed(1, last_sums)
    for s in s2:
        s.sent()


def per_device(
    tokens, w_gate_side, w_value_side, spatial_gain, w_spatial, spatial_bias, w_mixer_out,
    first_gain, w_ff_gate, w_ff_up, conv_gate_taps, conv_up_taps, w_ff_down, second_gain,
):
    vmem = pl.BlockSpec(memory_space=pltpu.VMEM)
    hbm = pl.BlockSpec(memory_space=pl.ANY)
    V, DMA = pltpu.VMEM, pltpu.SemaphoreType.DMA
    return pl.pallas_call(
        kernel,
        out_shape=jax.ShapeDtypeStruct((ROWS, 256), BF16),
        in_specs=[hbm] * 14,
        out_specs=vmem,
        scratch_shapes=[
            V((ROWS, D), BF16),
            V((D, 128), BF16),
            V((D, 128), BF16),
            V((16, 512, 128), BF16),
            V((16, 768, 128), BF16),
            V((16, 768, 128), BF16),
            V((16, 768, 128), BF16),
            V((ROWS, 128), F32),
            V((ROWS, 128), F32),
            V((8, 16, 128), F32),
            V((8, 2, 8, 128), F32),
            V((16, 128), F32),
            V((4, ROWS, 128), BF16),
            V((8, 1536), F32),
            V((1, 128), F32),
            V((2, 128, 128), BF16),
            V((2, 128), F32),
            V((1, D), F32),
            V((3, 704), F32),
            V((3, 704), F32),
            V((1, D), F32),
            V((512, D), BF16),
            V((512, D), BF16),
            V((512, D), F32),
            V((512, D), F32),
            V((ROWS, D), BF16),
            V((ROWS, 768), BF16),
            V((4, ROWS, 256), BF16),
            V((4, ROWS, 256), BF16),
            V((6, ROWS, 128), BF16),
            V((6, ROWS, 128), BF16),
            V((2, ROWS, 128), F32),
            V((ROWS, 256), F32),
            DMA((14,)),
            DMA((5, 2, 16)),
            DMA((5, 2, 16)),
            DMA((2, 8)),
            DMA((2, 8)),
            DMA((3, 8)),
            DMA((3, 8)),
            DMA((4,)),
            DMA((4,)),
            DMA((3, 4)),
            DMA((3, 4)),
            DMA((6, 4)),
            DMA((6, 4)),
        ],
        compiler_params=pltpu.CompilerParams(
            collective_id=0, has_side_effects=True, vmem_limit_bytes=60 * 1024 * 1024
        ),
    )(
        tokens, w_gate_side, w_value_side, w_mixer_out, w_ff_gate.T, w_ff_up.T, w_ff_down,
        spatial_gain.reshape(1, 128), w_spatial, spatial_bias, first_gain.reshape(1, D),
        conv_gate_taps, conv_up_taps, second_gain.reshape(1, D),
    )


def solution(mesh):
    finer = Mesh(mesh.devices.reshape(4, 4, 4, 2), ("z", "y", "x", "c"))
    in_specs = (
        P(FS, None), P(FS, TP), P(FS, TP), P(TP), P(TP, None, None), P(TP, None), P(TP, FS), P(),
        P(FS, TP), P(FS, TP), P(None, TP), P(None, TP), P(TP, FS), P(),
    )
    return jax.shard_map(
        per_device, mesh=finer, in_specs=in_specs, out_specs=P(FS, TP), check_vma=False
    )
```

```python
import jax
import jax.numpy as jnp
from jax import lax
from jax.experimental import pallas as pl
from jax.experimental.pallas import tpu as pltpu
from jax.sharding import Mesh
from jax.sharding import PartitionSpec as P

ROWS = 1024
D = 2048
SG_WIDTH = 1024
SEQ = 256
FS = ("z", "y")
TP = ("x", "c")
SCALE = 2.0**0.25
EPS = 1e-05
F32 = jnp.float32
BF16 = jnp.bfloat16
MESH = pl.DeviceIdType.MESH


def mul(i, n):
    return pl.multiple_of(i, n)


def dot(a, b):
    return jnp.dot(a, b, preferred_element_type=F32)


ORDER = ((1, 0), (3, 0), (0, 1), (2, 0), (1, 3), (3, 3), (2, 1))
LAST = ((0, 3), (1, 1), (3, 1), (2, 3), (0, 2), (1, 2), (3, 2), (2, 2))


class PlaneGather:
    def __init__(self, block, pos, send_sem, recv_sem, flip=0, then=None, direct=False):
        self.block, self.pos, self.then, self.direct = block, pos, then, direct
        self.send_sem, self.recv_sem = send_sem, recv_sem
        self.flip = flip

    def axes(self, half):
        return ("y", "z") if half == 0 else ("z", "y")

    def ref(self, half, d):
        a1, a2 = self.axes(half)
        at = {
            a1: lax.rem(self.pos[a1] + 4 - d[0], 4),
            a2: lax.rem(self.pos[a2] + 4 - d[1], 4),
        }
        return self.block(half, at["z"] * 4 + at["y"])

    def copy(self, half, target, source, axis, step):
        ref = self.ref(half, source)
        i = target[0] * 4 + target[1]
        return pltpu.make_async_remote_copy(
            src_ref=ref,
            dst_ref=ref,
            send_sem=self.send_sem.at[half, i],
            recv_sem=self.recv_sem.at[half, i],
            device_id={axis: lax.rem(self.pos[axis] + 4 + step, 4)},
            device_id_type=MESH,
        )

    def route(self, half, target):
        a1, a2 = self.axes(half)
        d1, d2 = target
        if self.direct:
            return ((d1, 0), a2, d2) if d2 else ((0, 0), a1, d1)
        if d2 == 0:
            if d1 == 2:
                plus = (half + self.flip) % 2 == 0
                return ((1, 0), a1, 1) if plus else ((3, 0), a1, -1)
            return ((0, 0), a1, 1 if d1 == 1 else -1)
        if d2 == 2:
            return ((d1, 1), a2, 1) if d1 % 2 == 0 else ((d1, 3), a2, -1)
        return ((d1, 0), a2, 1 if d2 == 1 else -1)

    def send(self, half, target):
        source, axis, step = self.route(half, target)
        self.copy(half, target, source, axis, step).start()

    def after(self, half, source, first=True, second=True):
        for target in ((1, 0), (3, 0), (2, 0)):
            if first and self.route(half, target)[0] == source:
                self.send(half, target)
        for d1 in range(4) if second else ():
            for d2 in (1, 3, 2):
                if self.route(half, (d1, d2))[0] == source:
                    self.send(half, (d1, d2))

    def own(self, first=True, second=True):
        for half in (0, 1):
            self.after(half, (0, 0), first, second)
            if self.then and first:
                self.then(half, self.ref(half, (0, 0)))

    def arrived(self, half, d):
        i = d[0] * 4 + d[1]
        ref = self.ref(half, d)
        pltpu.make_async_remote_copy(
            src_ref=ref,
            dst_ref=ref,
            send_sem=self.send_sem.at[half, i],
            recv_sem=self.recv_sem.at[half, i],
            device_id={"y": lax.rem(self.pos["y"] + 1, 4)},
            device_id_type=MESH,
        ).wait_recv()
        if self.then:
            self.then(half, ref)

    def step(self, *which):
        for k in which:
            for half in (0, 1):
                self.arrived(half, ORDER[k])
                self.after(half, ORDER[k])

    def rest(self):
        for d in LAST + (tuple(ORDER[k] for k in (2, 4, 5, 6)) if self.direct else ()):
            for half in (0, 1):
                self.arrived(half, d)

    def sent(self):
        for half in (0, 1):
            for d1 in range(4):
                for d2 in range(4):
                    if d1 or d2:
                        source, axis, step = self.route(half, (d1, d2))
                        self.copy(half, (d1, d2), source, axis, step).wait_send()


class RingGather:
    def __init__(self, block, x, send_sem, recv_sem, chunks):
        self.block, self.x, self.chunks = block, x, chunks
        self.send_sem, self.recv_sem = send_sem, recv_sem

    def move(self, ref, slot, step):
        return pltpu.make_async_remote_copy(
            src_ref=ref,
            dst_ref=ref,
            send_sem=self.send_sem.at[slot],
            recv_sem=self.recv_sem.at[slot],
            device_id={"x": lax.rem(self.x + 4 + step, 4)},
            device_id_type=MESH,
        )

    def copy(self, back, part, slot, step):
        return self.move(self.block(lax.rem(self.x + 4 - back, 4), part), slot, step)

    def far_copy(self, back, part, chunk, step):
        b = lax.rem(self.x + 4 - back, 4)
        slot = 4 + part * self.chunks + chunk
        return self.move(self.block(b, part, chunk), slot, step)

    def sends(self):
        return ((0, 0, 0, 1), (0, 1, 1, -1), (0, 1, 2, 1), (0, 0, 3, -1))

    def own(self, part):
        for c in self.sends():
            if c[1] == part:
                self.copy(*c).start()

    def piece(self, part, ref):
        for slot, step in ((0, 1), (3, -1)) if part == 0 else ((2, 1), (1, -1)):
            self.move(ref, slot, step).start()

    def forward(self, chunk):
        if chunk == 0:
            self.copy(1, 0, 0, 1).wait_recv()
        self.far_copy(1, 0, chunk, 1).start()
        if chunk == 0:
            self.copy(3, 1, 1, 1).wait_recv()
        self.far_copy(3, 1, chunk, -1).start()

    def near(self):
        self.copy(1, 1, 2, 1).wait_recv()
        self.copy(3, 0, 3, 1).wait_recv()

    def far(self):
        for chunk in range(self.chunks):
            for part in (0, 1):
                self.far_copy(2, part, chunk, 1).wait_recv()

    def sent(self):
        for c in self.sends():
            self.copy(*c).wait_send()
        for chunk in range(self.chunks):
            self.far_copy(1, 0, chunk, 1).wait_send()
            self.far_copy(3, 1, chunk, -1).wait_send()


class Stats:
    def __init__(self, ref, x, c, send_sem, recv_sem, half=None):
        self.ref, self.x, self.c, self.half = ref, x, c, half
        self.send_sem, self.recv_sem = send_sem, recv_sem

    def at(self, k):
        return k if self.half is None else (k, self.half)

    def copies(self):
        out = []
        for k in (4, 5, 2, 6, 3, 7, 1):
            dx, dc = k // 2, k % 2
            out.append(
                pltpu.make_async_remote_copy(
                    src_ref=self.ref.at[self.at(0)],
                    dst_ref=self.ref.at[self.at(k)],
                    send_sem=self.send_sem.at[k],
                    recv_sem=self.recv_sem.at[k],
                    device_id={"x": lax.rem(self.x + dx, 4), "c": lax.rem(self.c + dc, 2)},
                    device_id_type=MESH,
                )
            )
        return out

    def start(self):
        for c in self.copies():
            c.start()

    def total(self):
        for c in self.copies():
            c.wait_recv()
        total = self.ref[self.at(0)]
        for k in range(1, 8):
            total = total + self.ref[self.at(k)]
        return total

    def sent(self):
        for c in self.copies():
            c.wait_send()


def spread(row):
    return jnp.broadcast_to(row, (128, 128)).T


def kernel(
    tok_h, gate_h, value_h, mo_h, fg_h, fu_h, wd_h, gain_h, wsp_h, bias_h, g1_h, tg_h, tu_h, g2_h,
    out,
    tok, wgt, wvl, mo, wfg, wfu, wd, ga, va, st1, st2, tot, so, taps, gain, wsp, bias, g1, taps_g, taps_u, g2,
    msend, mrecv, mown, mtheir, fn, hid, dsend, drecv, xs, xr, pend, acc,
    lsem, psend, precv, rsend, rrecv, ssend, srecv, dss, drs, dds, ddr, xss, xrs,
):
    z, y = lax.axis_index("z"), lax.axis_index("y")
    x, c = lax.axis_index("x"), lax.axis_index("c")
    pos = {"z": z, "y": y}
    f = z * 4 + y
    j = x * 2 + c
    sib = {"c": 1 - c}

    def gv_block(half, b):
        return (wgt, wvl)[half].at[pl.ds(mul(b * 128, 128), 128), :]

    def mo_block(half, b):
        return mo.at[b, pl.ds(mul(x * 128 + half * 64, 64), 64), :]

    def in1_block(half, b):
        return (wfg, wfu)[half].at[b, pl.ds(0, 384), :]

    def in2_block(half, b):
        return (wfg, wfu)[half].at[b, pl.ds(384, 320), :]

    def wd_block(half, b):
        return wd.at[b, pl.ds(half * 352, 352), :]

    def mo_ring(b, part, chunk=None):
        cut = slice(None) if chunk is None else pl.ds(chunk * 8, 8)
        return mo.at[cut, pl.ds(mul(b * 128 + part * 64, 64), 64), :]

    def so_ring(b, part, chunk=None):
        return so.at[b, pl.ds(part * 512, 512), :]

    r_mo = RingGather(mo_ring, x, rsend.at[0], rrecv.at[0], 2)
    r_so = RingGather(so_ring, x, rsend.at[1], rrecv.at[1], 1)
    g_gv = PlaneGather(gv_block, pos, psend.at[0], precv.at[0], 0)
    g_mo = PlaneGather(mo_block, pos, psend.at[1], precv.at[1], 0, r_mo.piece)
    g_in1 = PlaneGather(in1_block, pos, psend.at[2], precv.at[2], 0)
    g_in2 = PlaneGather(in2_block, pos, psend.at[3], precv.at[3], 1)
    g_wd = PlaneGather(wd_block, pos, psend.at[4], precv.at[4], 1)
    s1 = Stats(st1, x, c, ssend.at[0], srecv.at[0])
    s2 = [Stats(st2, x, c, ssend.at[1 + h], srecv.at[1 + h], h) for h in range(2)]

    rows_f = pl.ds(mul(f * 128, 128), 128)
    loads = [
        pltpu.make_async_copy(gate_h, wgt.at[rows_f, :], lsem.at[0]),
        pltpu.make_async_copy(value_h, wvl.at[rows_f, :], lsem.at[1]),
        pltpu.make_async_copy(mo_h, mo.at[f, pl.ds(mul(x * 128, 128), 128), :], lsem.at[2]),
        pltpu.make_async_copy(fg_h, wfg.at[f, pl.ds(0, 704), :], lsem.at[3]),
        pltpu.make_async_copy(fu_h, wfu.at[f, pl.ds(0, 704), :], lsem.at[4]),
        pltpu.make_async_copy(wd_h, wd.at[f, pl.ds(0, 704), :], lsem.at[5]),
        pltpu.make_async_copy(tok_h, tok, lsem.at[6]),
    ]
    small = [
        pltpu.make_async_copy(a, b, lsem.at[7 + k])
        for k, (a, b) in enumerate(
            zip(
                (tg_h, tu_h, gain_h, wsp_h, bias_h, g1_h, g2_h),
                (taps_g, taps_u, gain, wsp, bias, g1, g2),
            )
        )
    ]
    for l in loads + small:
        l.start()

    barrier = pltpu.get_barrier_semaphore()
    peers = [{a: lax.rem(pos[a] + s, 4)} for a in ("y", "z") for s in (1, 3)]
    peers += [
        {"x": lax.rem(x + k // 2, 4), "c": lax.rem(c + k % 2, 2)} for k in range(1, 8)
    ]
    for p in peers:
        pl.semaphore_signal(barrier, inc=1, device_id=p, device_id_type=MESH)
    for buf in (wd, wfg, wfu):
        @pl.loop(0, 16)
        def _(b):
            buf[b, 704:768, :] = jnp.zeros((64, 128), BF16)

    for l in small:
        l.wait()
    for i in range(5):
        t = slice(i * 128, i * 128 + 128)
        taps[0:3, i * 256 : i * 256 + 128] = taps_g[:, t]
        taps[0:3, i * 256 + 128 : i * 256 + 256] = taps_u[:, t]
    taps[:, 1280:1536] = jnp.zeros((8, 256), F32)
    taps[0:3, 1280:1344] = taps_g[:, 640:704]
    taps[0:3, 1408:1472] = taps_u[:, 640:704]
    for k in range(3):
        loads[k].wait()
    pl.semaphore_wait(barrier, len(peers))

    g_mo.own(second=False)
    g_gv.own(second=False)
    g_mo.own(first=False)
    loads[3].wait()
    loads[4].wait()
    g_in1.own(second=False)
    g_mo.step(0)
    g_mo.step(1)
    g_gv.step(1)
    g_gv.step(0)
    g_gv.own(first=False)
    g_in2.own(second=False)
    g_mo.step(3)
    g_gv.step(3)
    loads[5].wait()
    g_wd.own(second=False)
    g_gv.step(4)
    g_mo.step(5)
    g_mo.step(4)
    g_gv.step(2)
    g_mo.step(2)
    g_mo.step(6)
    g_gv.step(5)
    g_gv.step(6)
    g_in1.own(first=False)
    g_in1.step(0)
    g_in1.step(1)
    g_in2.step(1)
    g_mo.rest()
    g_gv.rest()
    loads[6].wait()
    @pl.loop(0, 4)
    def _(i):
        r = pl.ds(mul(i * 256, 256), 256)
        pre = dot(tok[r, :], jnp.concatenate([wgt[...], wvl[...]], axis=1))
        act = jax.nn.gelu(pre)
        ga[r, :] = act[:, :128]
        va[r, :] = act[:, 128:]
        for h in range(2):
            v = act[h * 128 : h * 128 + 128, 128:].T
            st1[0, pl.ds(i * 2 + h, 1), :] = jnp.sum(v, axis=0, keepdims=True)
            st1[0, pl.ds(i * 2 + h + 8, 1), :] = jnp.sum(v * v, axis=0, keepdims=True)

    s1.start()
    g_in2.step(0)
    r_mo.forward(0)
    g_in1.step(4)
    g_wd.step(0)
    g_in1.step(5)
    g_wd.step(1)
    g_in1.step(3)
    tot[...] = s1.total()
    lane = lax.broadcasted_iota(jnp.int32, (128, 128), 1)
    low = lax.broadcasted_iota(jnp.int32, (128, 128), 0) >= lane
    w0 = jnp.where(low, wsp[0], jnp.zeros((128, 128), BF16))
    w1 = jnp.where(low, wsp[1], jnp.zeros((128, 128), BF16))
    shift = jnp.where(lane < 64, spread(bias[0:1, :]), spread(bias[1:2, :]))

    @pl.loop(0, 8)
    def _(n):
        r = pl.ds(mul(n * 128, 128), 128)
        mean = spread(tot[pl.ds(n, 1), :] * (1.0 / SG_WIDTH))
        square = spread(tot[pl.ds(n + 8, 1), :] * (1.0 / SG_WIDTH))
        inv = lax.rsqrt(square - mean * mean + EPS)
        vn = ((va[r, :] - mean) * inv * gain[...]).astype(BF16)
        mixed = jnp.where(lane < 64, dot(w0, vn), dot(w1, vn)) + shift
        so[x, r, :] = (ga[r, :] * mixed).astype(BF16)
        for part in range(2):
            @pl.when(n == part * 4 + 3)
            def _():
                r_so.own(part)

    g_in2.step(3)
    g_in2.own(first=False)
    r_mo.forward(1)
    g_wd.own(first=False)
    r_so.forward(0)
    r_mo.near()
    r_so.near()
    g_wd.step(4)
    g_in2.step(4)
    theirs = (1 - c) * 512
    mine = c * 512

    def mix_copy(k):
        return pltpu.make_async_remote_copy(
            src_ref=msend.at[pl.ds(k * 256, 256), :],
            dst_ref=mrecv.at[pl.ds(k * 256, 256), :],
            send_sem=dss.at[k], recv_sem=drs.at[k], device_id=sib, device_id_type=MESH,
        )

    def fn_copy(k, base):
        ref = fn.at[pl.ds(mul(base + k * 256, 256), 256), :]
        return pltpu.make_async_remote_copy(
            src_ref=ref, dst_ref=ref,
            send_sem=dss.at[2 + k], recv_sem=drs.at[2 + k], device_id=sib, device_id_type=MESH,
        )

    def mix(base, i, blocks):
        r = pl.ds(mul(base, 256), 256)
        left = jnp.concatenate([so[b, r, :] for b in blocks], axis=1)
        right = jnp.concatenate(
            [
                jnp.concatenate([mo[i * 4 + q, pl.ds(mul(b * 128, 128), 128), :] for b in blocks], axis=0)
                for q in range(4)
            ],
            axis=1,
        )
        return dot(left, right)

    near = (x, lax.rem(x + 3, 4))
    far = (lax.rem(x + 1, 4), lax.rem(x + 2, 4))

    def mix_at(i):
        return pl.ds(mul(i // 4 * 256, 256), 256), pl.ds(mul(i % 4 * 512, 512), 512)

    @pl.loop(0, 8)
    def _(i):
        mtheir[mix_at(i)] = mix(theirs + i // 4 * 256, i % 4, near)
        mown[mix_at(i)] = mix(mine + i // 4 * 256, i % 4, near)

    g_in1.step(2)
    g_in1.step(6)
    g_in2.step(5)
    g_in2.step(6)
    g_wd.step(5)
    g_wd.step(3)
    r_mo.far()
    r_so.far()
    @pl.loop(0, 8)
    def _(i):
        p = mix(theirs + i // 4 * 256, i % 4, far)
        msend[mix_at(i)] = (mtheir[mix_at(i)] + p).astype(BF16)
        for k in range(2):
            @pl.when(i == k * 4 + 3)
            def _():
                mix_copy(k).start()

    @pl.loop(0, 8)
    def _(i):
        mown[mix_at(i)] = mown[mix_at(i)] + mix(mine + i // 4 * 256, i % 4, far)

    g_in2.step(2)
    @pl.loop(0, 16)
    def _(i):
        for k in range(2):
            @pl.when(i == k * 8)
            def _():
                mix_copy(k).wait_recv()

        r = pl.ds(mul(i * 32, 32), 32)
        g = pl.ds(mul(mine + i * 32, 32), 32)
        v = SCALE * tok[g, :].astype(F32) + (mown[r, :] + mrecv[r, :].astype(F32))
        mean = jnp.sum(v, axis=1, keepdims=True) * (1.0 / D)
        square = jnp.sum(v * v, axis=1, keepdims=True) * (1.0 / D)
        inv = lax.rsqrt(square - mean * mean + EPS)
        fn[g, :] = ((v - mean) * inv * g1[...]).astype(BF16)
        for k in range(2):
            @pl.when(i == k * 8 + 7)
            def _():
                fn_copy(k, mine).start()

    row = lax.broadcasted_iota(jnp.int32, (SEQ, 256), 0)

    def conv(p, t):
        n = p.shape[1]
        p1 = jnp.where(row[:, :n] >= 1, pltpu.roll(p, 1, 0), 0.0)
        p2 = jnp.where(row[:, :n] >= 2, pltpu.roll(p, 2, 0), 0.0)
        return p2 * t[0:1, :] + p1 * t[1:2, :] + p * t[2:3, :]

    def dot_t(a, rows):
        w = jnp.concatenate(
            [jnp.concatenate([buf[b, rows, :] for b in range(16)], axis=1) for buf in (wfg, wfu)],
            axis=0,
        )
        return lax.dot_general(a, w, (((1,), (1,)), ((), ())), preferred_element_type=F32)

    def tile(first, i):
        p = dot_t(fn[pl.ds(mul(first * SEQ, SEQ), 2 * SEQ), :], pl.ds(mul(i * 128, 128), 128))
        for h in range(2):
            q = conv(p[h * SEQ : h * SEQ + SEQ], taps[:, pl.ds(mul(i * 256, 256), 256)])
            hid[pl.ds(mul((first + h) * SEQ, SEQ), SEQ), pl.ds(mul(i * 128, 128), 128)] = (
                jax.nn.silu(q[:, :128]) * q[:, 128:]
            ).astype(BF16)

    g_wd.step(2)
    g_in1.rest()
    @pl.loop(0, 9)
    def _(i):
        @pl.when(i == 3)
        def _():
            for k in range(2):
                fn_copy(k, (1 - c) * 512).wait_recv()

        @pl.when(i == 4)
        def _():
            g_wd.step(6)

        @pl.when(i == 6)
        def _():
            g_in2.rest()

        q = i // 3
        tile((1 - q // 2) * (2 * c * (1 - q) + (2 - 2 * c) * q), i % 3 + q // 2 * 3)

    g_wd.rest()

    hops = (2, 1, 3, 0)
    groups = ((0, 1), (1, 2), (3, 1))

    def seq_rows(s):
        return pl.ds(mul(s * SEQ, SEQ), SEQ)

    def dd_copy(g, s):
        ref = (pl.ds(groups[g][0], groups[g][1]), seq_rows(s), slice(None))
        return pltpu.make_async_remote_copy(
            src_ref=dsend.at[ref], dst_ref=drecv.at[ref],
            send_sem=dds.at[g, s], recv_sem=ddr.at[g, s], device_id=sib, device_id_type=MESH,
        )

    def down(g, s, parity):
        cols = []
        for k in range(groups[g][0], groups[g][0] + groups[g][1]):
            b = (lax.rem(x + hops[k], 4) * 2 + parity) * 2
            cols += [wd[b], wd[b + 1]]
        return dot(hid[seq_rows(s), :], jnp.concatenate(cols, axis=1))

    def theirs_of(g, s):
        p = down(g, s, 1 - c)
        for i in range(groups[g][1]):
            dsend[groups[g][0] + i, seq_rows(s), :] = p[:, i * 256 : i * 256 + 256].astype(BF16)
        dd_copy(g, s).start()

    def ours(g, s):
        dd_copy(g, s).wait_recv()
        p = down(g, s, c)
        return [
            p[:, i * 256 : i * 256 + 256] + drecv[groups[g][0] + i, seq_rows(s), :].astype(F32)
            for i in range(groups[g][1])
        ]

    def x_copy(i, s):
        return pltpu.make_async_remote_copy(
            src_ref=xs.at[i, seq_rows(s), :], dst_ref=xr.at[i, seq_rows(s), :],
            send_sem=xss.at[i, s], recv_sem=xrs.at[i, s],
            device_id={"x": lax.rem(x + (1 if i % 2 == 0 else 3), 4)}, device_id_type=MESH,
        )

    def put(i, s, v):
        xs[i, seq_rows(s), :] = v.astype(BF16)
        x_copy(i, s).start()

    def got(i, s):
        return xr[i, seq_rows(s), :].astype(F32)

    def far_out(s):
        v = ours(0, s)[0]
        put(0, s, v[:, :128])
        put(1, s, v[:, 128:])

    def near_out(s):
        p, m = ours(1, s)
        put(2, s, p[:, 128:])
        put(3, s, m[:, :128])
        pend[0, seq_rows(s), :] = p[:, :128]
        pend[1, seq_rows(s), :] = m[:, 128:]

    def joined_out(s):
        for i in range(2):
            x_copy(i, s).wait_recv()
            put(4 + i, s, pend[i, seq_rows(s), :] + got(i, s))

    def own_out(s):
        acc[seq_rows(s), :] = ours(2, s)[0] + SCALE * fn[
            seq_rows(s), pl.ds(mul(j * 256, 256), 256)
        ].astype(F32)

    def finish(s):
        for i in range(2, 6):
            x_copy(i, s).wait_recv()
        a = acc[seq_rows(s), :128] + (got(4, s) + got(3, s))
        b = acc[seq_rows(s), 128:] + (got(2, s) + got(5, s))
        acc[seq_rows(s), :128] = a
        acc[seq_rows(s), 128:] = b
        half, row = s // 2, s % 2 * 2
        total, square = a + b, a * a + b * b
        for i in range(2):
            r = slice(i * 128, i * 128 + 128)
            st2[0, half, row + i : row + i + 1, :] = jnp.sum(total[r].T, axis=0, keepdims=True)
            st2[0, half, row + i + 4 : row + i + 5, :] = jnp.sum(square[r].T, axis=0, keepdims=True)

    def normed(h, sums):
        for i in range(4):
            r = slice(h * 512 + i * 128, h * 512 + i * 128 + 128)
            mean = spread(sums[i : i + 1, :] * (1.0 / D))
            square = spread(sums[i + 4 : i + 5, :] * (1.0 / D))
            inv = lax.rsqrt(square - mean * mean + EPS)
            for q in range(2):
                cols = slice(q * 128, q * 128 + 128)
                out[r, cols] = ((acc[r, cols] - mean) * inv * gain2[:, cols]).astype(BF16)

    @pl.loop(0, 2)
    def _(s):
        theirs_of(0, s)
        theirs_of(1, s)

    @pl.loop(0, 2)
    def _(s):
        far_out(s)
        near_out(s)

    @pl.loop(3, 6)
    def _(i):
        tile(2, i)

    joined_out(0)
    @pl.loop(2, 4)
    def _(s):
        theirs_of(0, s)
        theirs_of(1, s)

    joined_out(1)
    @pl.loop(2, 4)
    def _(s):
        far_out(s)

    @pl.loop(2, 4)
    def _(s):
        near_out(s)

    @pl.loop(0, 4)
    def _(s):
        theirs_of(2, s)

    joined_out(2)
    joined_out(3)
    @pl.loop(0, 4)
    def _(s):
        own_out(s)

    for g in (g_gv, g_mo, g_in1, g_in2, g_wd, r_mo, r_so, s1):
        g.sent()
    for k in range(2):
        mix_copy(k).wait_send()
        fn_copy(k, mine).wait_send()
    for g in range(3):
        for s in range(4):
            dd_copy(g, s).wait_send()
    gain2 = g2[:, pl.ds(mul(j * 256, 256), 256)]
    finish(0)
    finish(1)
    s2[0].start()
    finish(2)
    finish(3)
    s2[1].start()
    normed(0, s2[0].total())
    for i in range(6):
        for s in range(4):
            x_copy(i, s).wait_send()
    last_sums = s2[1].total()
    normed(1, last_sums)
    for s in s2:
        s.sent()


def per_device(
    tokens, w_gate_side, w_value_side, spatial_gain, w_spatial, spatial_bias, w_mixer_out,
    first_gain, w_ff_gate, w_ff_up, conv_gate_taps, conv_up_taps, w_ff_down, second_gain,
):
    vmem = pl.BlockSpec(memory_space=pltpu.VMEM)
    hbm = pl.BlockSpec(memory_space=pl.ANY)
    V, DMA = pltpu.VMEM, pltpu.SemaphoreType.DMA
    return pl.pallas_call(
        kernel,
        out_shape=jax.ShapeDtypeStruct((ROWS, 256), BF16),
        in_specs=[hbm] * 14,
        out_specs=vmem,
        scratch_shapes=[
            V((ROWS, D), BF16),
            V((D, 128), BF16),
            V((D, 128), BF16),
            V((16, 512, 128), BF16),
            V((16, 768, 128), BF16),
            V((16, 768, 128), BF16),
            V((16, 768, 128), BF16),
            V((ROWS, 128), F32),
            V((ROWS, 128), F32),
            V((8, 16, 128), F32),
            V((8, 2, 8, 128), F32),
            V((16, 128), F32),
            V((4, ROWS, 128), BF16),
            V((8, 1536), F32),
            V((1, 128), F32),
            V((2, 128, 128), BF16),
            V((2, 128), F32),
            V((1, D), F32),
            V((3, 704), F32),
            V((3, 704), F32),
            V((1, D), F32),
            V((512, D), BF16),
            V((512, D), BF16),
            V((512, D), F32),
            V((512, D), F32),
            V((ROWS, D), BF16),
            V((ROWS, 768), BF16),
            V((4, ROWS, 256), BF16),
            V((4, ROWS, 256), BF16),
            V((6, ROWS, 128), BF16),
            V((6, ROWS, 128), BF16),
            V((2, ROWS, 128), F32),
            V((ROWS, 256), F32),
            DMA((14,)),
            DMA((5, 2, 16)),
            DMA((5, 2, 16)),
            DMA((2, 8)),
            DMA((2, 8)),
            DMA((3, 8)),
            DMA((3, 8)),
            DMA((4,)),
            DMA((4,)),
            DMA((3, 4)),
            DMA((3, 4)),
            DMA((6, 4)),
            DMA((6, 4)),
        ],
        compiler_params=pltpu.CompilerParams(
            collective_id=0, has_side_effects=True, vmem_limit_bytes=60 * 1024 * 1024
        ),
    )(
        tokens, w_gate_side, w_value_side, w_mixer_out, w_ff_gate.T, w_ff_up.T, w_ff_down,
        spatial_gain.reshape(1, 128), w_spatial, spatial_bias, first_gain.reshape(1, D),
        conv_gate_taps, conv_up_taps, second_gain.reshape(1, D),
    )


def solution(mesh):
    finer = Mesh(mesh.devices.reshape(4, 4, 4, 2), ("z", "y", "x", "c"))
    in_specs = (
        P(FS, None), P(FS, TP), P(FS, TP), P(TP), P(TP, None, None), P(TP, None), P(TP, FS), P(),
        P(FS, TP), P(FS, TP), P(None, TP), P(None, TP), P(TP, FS), P(),
    )
    return jax.shard_map(
        per_device, mesh=finer, in_specs=in_specs, out_specs=P(FS, TP), check_vma=False
    )
```
